128 devices in a mesh: kv: 16 (over z, y), tp: 8 (over x, core).
Axes of the slice: x: 4, y: 4, z: 4, core: 2. Of those that a mesh axis runs over, the one named last changes fastest.
Arguments:
- tokens: bfloat16 [256, 4096], P(None, ('kv', 'tp')), may hold values from -64 to 64
- mix_gain: float32 [4096], P('kv'), may hold values from 0.1 to 1.9
- w_query: bfloat16 [4096, 3072], P('kv', 'tp'), may hold values from -0.09375 to 0.09375
- w_key: bfloat16 [4096, 3072], P('kv', 'tp'), may hold values from -0.09375 to 0.09375
- w_value: bfloat16 [4096, 3072], P('kv', 'tp'), may hold values from -0.09375 to 0.09375
- w_gate: bfloat16 [4096, 3072], P('kv', 'tp'), may hold values from -0.09375 to 0.09375
- w_beta: bfloat16 [4096, 24], P('kv'), may hold values from -0.09375 to 0.09375
- w_decay: bfloat16 [4096, 24], P('kv'), may hold values from -0.09375 to 0.09375
- decay_rate: float32 [24], P('tp'), may hold values from 0.15 to 1.5
- out_gain: float32 [128], replicated, may hold values from 0.1 to 1.9
- state: float32 [256, 24, 128, 128], P('kv', 'tp'), may hold values from -0.6 to 0.6
- w_out: bfloat16 [3072, 4096], P('tp', 'kv'), may hold values from -0.109375 to 0.109375
- mlp_gain: float32 [4096], replicated, may hold values from 0.1 to 1.9
- w_up: bfloat16 [4096, 16384], P(None, ('kv', 'tp')), may hold values from -0.09375 to 0.09375
- w_down: bfloat16 [16384, 4096], P(('kv', 'tp')), may hold values from -0.1875 to 0.1875
Outputs:
- mixed: bfloat16 [256, 4096], P(None, ('kv', 'tp'))
- new_state: float32 [256, 24, 128, 128], P('kv', 'tp')
The draws below stay inside these ranges and needn't reach their ends.
All inputs are finite; a program needn't handle non-finite values.
Results may differ from the reference program's by a relative error of at most 0.0063.
Values may be sent and summed in bfloat16 or wider, within the bound.
A program may use at most 64 MiB of HBM per device.

```python
import math
import jax
import jax.numpy as jnp
from jax import lax

D = 4096
H = 24
HEAD = 128
FF = 16384
BATCH = 256


def draw_tokens(key, part):
    first, second, third = jax.random.split(jax.random.fold_in(key, 17), 3)
    position = jnp.arange(D, dtype=jnp.float32) / D
    column_scale = jnp.exp(jnp.log(6.0) * (position - 0.5)) * jax.random.uniform(second, (D,), jnp.float32, 0.6, 1.6)
    base = jnp.clip(jax.random.normal(first, (BATCH, D), jnp.float32), -4.0, 4.0)
    row_scale = jnp.exp(jax.random.uniform(third, (BATCH, 1), jnp.float32, jnp.log(0.4), jnp.log(4.0)))
    values = base * row_scale * column_scale[None, :]
    return values.astype(jnp.bfloat16)


def raised(entries, rng, source, target, parts, factor):
    owner, partner = [(jnp.arange(entries.shape[dim]) // (entries.shape[dim] // parts)).reshape([-1 if axis == dim else 1 for axis in range(entries.ndim)]) for dim in (source, target)]
    chosen = jax.random.permutation(rng, parts)[partner]
    strong = (owner == chosen) | (owner == (partner + parts // 2) % parts)
    return jnp.where(strong, factor * entries, entries)


def levels(own_key, extent, cuts, least, top_value):
    def one(dim, parts):
        steps = jax.random.uniform(jax.random.fold_in(jax.random.fold_in(own_key, 6), dim), (parts,), jnp.float32, least / len(cuts), top_value / len(cuts))
        return jnp.repeat(jnp.exp(steps), extent[dim] // parts).reshape((-1,) + (1,) * (len(extent) - dim - 1))

    level = one(*cuts[0])
    for cut in cuts[1:]:
        level = level * one(*cut)
    return level


def noise(own_key, extent, deviation, bound, cuts=(), kind=jnp.bfloat16):
    values = deviation * jax.random.normal(own_key, extent, jnp.float32)
    if cuts:
        values = values * levels(own_key, extent, cuts, -0.22, 0.18)
    return jnp.clip(values, -bound, bound).astype(kind)


def gaussian_with(rng, dims, deviation, limit, pieces, heavy, kind=jnp.bfloat16):
    values = deviation * jax.random.normal(rng, dims, jnp.float32)
    if pieces:
        values = values * levels(rng, dims, pieces, -0.22, 0.18)
    return jnp.clip(raised(values, jax.random.fold_in(rng, 3), *heavy), -limit, limit).astype(kind)


def setup_inputs(seed: int = 0) -> dict:
    key_of = jax.random.split(jax.random.key(seed), 16)
    return {
        "tokens": draw_tokens(jax.random.fold_in(key_of[15], 71), 0),
        "mix_gain": jnp.clip(1.0 + 0.18 * jax.random.normal(key_of[1], (D,), jnp.float32), 0.1, 1.9),
        "w_query": noise(key_of[2], (D, H * HEAD), D ** -0.5, 0.09375, ((0, 16), (1, 8))),
        "w_key": noise(key_of[3], (D, H * HEAD), D ** -0.5, 0.09375, ((0, 16), (1, 8))),
        "w_value": noise(key_of[4], (D, H * HEAD), D ** -0.5, 0.09375, ((0, 16), (1, 8))),
        "w_gate": noise(key_of[5], (D, H * HEAD), D ** -0.5, 0.09375, ((0, 16), (1, 8))),
        "w_beta": noise(key_of[6], (D, H), D ** -0.5, 0.09375, ((0, 16),)),
        "w_decay": noise(key_of[7], (D, H), D ** -0.5, 0.09375, ((0, 16),)),
        "decay_rate": jnp.clip(jnp.exp(math.log(1.5) - 2.3025851 * jax.random.uniform(key_of[8], (H,), jnp.float32) ** levels(key_of[8], (H,), ((0, 8),), -0.2, 0.2)), 0.15, 1.5),
        "out_gain": jnp.clip(1.0 + 0.18 * jax.random.normal(key_of[9], (HEAD,), jnp.float32), 0.1, 1.9),
        "state": noise(key_of[10], (BATCH, H, HEAD, HEAD), 0.1, 0.6, ((0, 16), (1, 8)), jnp.float32),
        "w_out": noise(key_of[11], (H * HEAD, D), (H * HEAD) ** -0.5, 0.109375, ((0, 8), (1, 16))),
        "mlp_gain": jnp.clip(1.0 + 0.18 * jax.random.normal(key_of[12], (D,), jnp.float32), 0.1, 1.9),
        "w_up": noise(key_of[13], (D, FF), D ** -0.5, 0.09375, ((1, 128),)),
        "w_down": gaussian_with(key_of[14], (FF, D), FF ** -0.5, 0.1875, ((0, 128),), (0, 1, 128, 5.5)),
    }


EPSILON = 1e-06

def head_norm(values):
    return values * lax.rsqrt(lax.optimization_barrier(jnp.sum(values * values, axis=-1, keepdims=True)) + EPSILON)

def per_head(inputs):
    old_state, decay, key, value, beta, query = inputs
    faded = old_state * decay[:, None, None]
    recalled = jnp.einsum('bkv,bk->bv', faded, key, precision=lax.Precision.HIGHEST)
    change = beta[:, None] * (value - recalled)
    updated = faded + key[:, :, None] * change[:, None, :]
    readout = jnp.einsum('bkv,bk->bv', updated, query, precision=lax.Precision.HIGHEST)
    return (updated, readout)

def reference(tokens, mix_gain, w_query, w_key, w_value, w_gate, w_beta, w_decay, decay_rate, out_gain, state, w_out, mlp_gain, w_up, w_down):
    tokens_f = tokens.astype(jnp.float32)
    row_scale = lax.rsqrt(lax.optimization_barrier(jnp.mean(tokens_f * tokens_f, axis=1, keepdims=True)) + EPSILON)
    normed = (tokens_f * mix_gain[None, :]).astype(jnp.bfloat16)

    def project(weight):
        return jnp.dot(normed, weight, preferred_element_type=jnp.float32) * row_scale
    query_raw = project(w_query).reshape(BATCH, H, HEAD)
    key_raw = project(w_key).reshape(BATCH, H, HEAD)
    value_raw = project(w_value).reshape(BATCH, H, HEAD)
    gate_raw = project(w_gate).reshape(BATCH, H, HEAD)
    beta_raw = project(w_beta)
    decay_raw = project(w_decay)
    query = head_norm(jax.nn.silu(query_raw)) * HEAD ** (-0.5)
    key = head_norm(jax.nn.silu(key_raw))
    value = jax.nn.silu(value_raw)
    beta = jax.nn.sigmoid(beta_raw)
    decay = jnp.exp(-decay_rate[None, :] * jax.nn.softplus(decay_raw))
    updated, readout = lax.map(per_head, (jnp.moveaxis(state, 1, 0), decay.T, jnp.moveaxis(key, 1, 0), jnp.moveaxis(value, 1, 0), beta.T, jnp.moveaxis(query, 1, 0)))
    new_state = jnp.moveaxis(updated, 0, 1)
    readout = jnp.moveaxis(readout, 0, 1)
    scaled = readout * lax.rsqrt(lax.optimization_barrier(jnp.mean(readout * readout, axis=-1, keepdims=True)) + EPSILON) * out_gain
    merged = (scaled * jax.nn.silu(gate_raw)).reshape(BATCH, H * HEAD).astype(jnp.bfloat16)
    residual = (tokens_f + jnp.dot(merged, w_out, preferred_element_type=jnp.float32)).astype(jnp.bfloat16)
    residual_f = residual.astype(jnp.float32)
    normed_mlp = (residual_f * lax.rsqrt(lax.optimization_barrier(jnp.mean(residual_f * residual_f, axis=1, keepdims=True)) + EPSILON) * mlp_gain[None, :]).astype(jnp.bfloat16)
    hidden = jnp.square(jax.nn.relu(jnp.dot(normed_mlp, w_up, preferred_element_type=jnp.float32))).astype(jnp.bfloat16)
    mixed = (residual_f + jnp.dot(hidden, w_down, preferred_element_type=jnp.float32)).astype(jnp.bfloat16)
    return (mixed, new_state)
```

```python
import functools
import math

import jax
import jax.numpy as jnp
from jax import lax
from jax.experimental import pallas as pl
from jax.experimental.pallas import tpu as pltpu
from jax.sharding import Mesh
from jax.sharding import PartitionSpec as P

EPSILON = 1e-06
MESH = pl.DeviceIdType.MESH
KV_TP = ("kv_0", "kv_1", "tp_0", "tp_1")
KV = ("kv_0", "kv_1")
TP = ("tp_0", "tp_1")
F32 = jnp.float32
BF16 = jnp.bfloat16


def silu(v):
    return v / (1.0 + jnp.exp(-v))


def layer_kernel(
    sizes,
    tok_ref,
    mix_gain_ref,
    wq_ref,
    wk_ref,
    wv_ref,
    wg_ref,
    wbeta_ref,
    wdecay_ref,
    rate_ref,
    out_gain_ref,
    state_ref,
    wout_ref,
    mlp_gain_ref,
    wup_ref,
    wdown_ref,
    mixed_ref,
    new_state_ref,
    col_t,
    w_proj,
    w_rates,
    w_out,
    w_up,
    w_down,
    st,
    col_n,
    send_b,
    recv_b,
    key_t,
    query_t,
    rows_s,
    readout_s,
    gate_s,
    merged,
    send_e,
    own_e,
    recv_e,
    res,
    res_t,
    hid,
    acc_up,
    send_d,
    recv_d,
    send_h,
    recv_h1a,
    recv_h1b,
    send_h2a,
    send_h2b,
    recv_h2a,
    recv_h2b,
    send_x,
    recv_x,
    local_sem,
    a_send,
    a_recv,
    b_send,
    b_recv,
    d_send,
    d_recv,
    e_send,
    e_recv,
    f1_send,
    f1_recv,
    fa_send,
    fb_send,
    fa_recv,
    fb_recv,
    fp_send,
    fp_recv,
    hd_send,
    hd_recv,
    h1a_send,
    h1b_send,
    h1a_recv,
    h1b_recv,
    h2_send,
    h2a_recv,
    h2b_recv,
    x_send,
    x_recv,
):
    nz, ny, nx, nc = sizes
    nkv, ntp = nz * ny, nx * nc
    z, y = lax.axis_index("kv_0"), lax.axis_index("kv_1")
    x, c = lax.axis_index("tp_0"), lax.axis_index("tp_1")
    kv, tp = z * ny + y, x * nc + c
    partner = {"tp_1": nc - 1 - c}

    dt, rows = tok_ref.shape
    dk = dt * ntp
    width = dk * nkv
    rb, heads, head = st.shape[0], st.shape[1], st.shape[2]
    proj = heads * head
    rt = rows // ntp
    rh = rows // nc
    rc = rh // 2

    def kv_dev(k):
        return {"kv_0": k // ny, "kv_1": lax.rem(k, ny)}

    def tp_dev(t):
        return {"tp_0": t // nc, "tp_1": lax.rem(t, nc)}

    def remote(src, dst, send_sem, recv_sem, dev):
        return pltpu.make_async_remote_copy(
            src_ref=src,
            dst_ref=dst,
            send_sem=send_sem,
            recv_sem=recv_sem,
            device_id=dev,
            device_id_type=MESH,
        )

    def loop(lo, hi, body):
        def wrapped(i, carry):
            body(i)
            return carry

        lax.fori_loop(lo, hi, wrapped, 0)

    def block(i, n):
        return pl.ds(pl.multiple_of(i * n, n), n)

    own_tok = col_t.at[block(tp, dt), :]
    tok_copy = pltpu.make_async_copy(tok_ref, own_tok, local_sem.at[0])
    tok_copy.start()
    proj_copies = [
        pltpu.make_async_copy(w, w_proj.at[i], local_sem.at[1 + i])
        for i, w in enumerate((wq_ref, wk_ref, wv_ref, wg_ref))
    ]
    for copy in proj_copies:
        copy.start()
    later_copies = [
        pltpu.make_async_copy(state_ref, st, local_sem.at[5]),
        pltpu.make_async_copy(wout_ref, w_out, local_sem.at[6]),
        pltpu.make_async_copy(wup_ref, w_up, local_sem.at[7]),
        pltpu.make_async_copy(wdown_ref, w_down, local_sem.at[8]),
    ]
    for copy in later_copies:
        copy.start()

    barrier = pltpu.get_barrier_semaphore()

    def greet_kv(d):
        k = lax.rem(kv + d, nkv)
        pl.semaphore_signal(barrier, inc=1, device_id=kv_dev(k), device_id_type=MESH)

    def greet_tp(d):
        t = lax.rem(tp + d, ntp)
        pl.semaphore_signal(barrier, inc=1, device_id=tp_dev(t), device_id_type=MESH)

    loop(1, nkv, greet_kv)
    loop(1, ntp, greet_tp)

    n_heads = wbeta_ref.shape[0]
    w_rates[...] = jnp.zeros_like(w_rates)
    w_rates[0:n_heads, :] = wbeta_ref[...]
    w_rates[32 : 32 + n_heads, :] = wdecay_ref[...]

    tok_copy.wait()
    pl.semaphore_wait(barrier, nkv - 1 + ntp - 1)

    def a_copy(d, src_tp, peer):
        blk = col_t.at[block(src_tp, dt), :]
        return remote(blk, blk, a_send.at[d], a_recv.at[src_tp], tp_dev(peer))

    loop(1, ntp, lambda d: a_copy(d, tp, lax.rem(tp + d, ntp)).start())

    def a_wait(d):
        src = lax.rem(tp + ntp - d, ntp)
        a_copy(d, src, src).wait_recv()

    loop(1, ntp, a_wait)

    cols = col_t[...].astype(F32).T
    col_n[...] = cols.astype(BF16)
    normed = (cols * mix_gain_ref[...]).astype(BF16)
    squares = jnp.sum(cols * cols, axis=1, keepdims=True)
    contract_last = (((1,), (1,)), ((), ()))
    rates_part = lax.dot_general(
        normed, w_rates[...], contract_last, preferred_element_type=F32
    )
    lane = lax.broadcasted_iota(jnp.int32, rates_part.shape, 1)
    rates_part = jnp.where(lane == 127, squares, rates_part)
    high = rates_part.astype(BF16)
    send_b[:, 4 * proj : 4 * proj + 128] = high
    send_b[:, 4 * proj + 128 :] = (rates_part - high.astype(F32)).astype(BF16)
    for i in range(4):
        proj_copies[i].wait()
        part = jnp.dot(normed, w_proj[i], preferred_element_type=F32)
        send_b[:, i * proj : (i + 1) * proj] = part.astype(BF16)

    def b_copy(d, dest_kv, src_kv, peer):
        return remote(
            send_b.at[block(dest_kv, rb), :],
            recv_b.at[src_kv],
            b_send.at[d],
            b_recv.at[src_kv],
            kv_dev(peer),
        )

    def b_start(d):
        peer = lax.rem(kv + d, nkv)
        b_copy(d, peer, kv, peer).start()

    loop(1, nkv, b_start)

    def b_add(d, acc):
        src = lax.rem(kv + nkv - d, nkv)
        b_copy(d, kv, src, src).wait_recv()
        return acc + recv_b[src].astype(F32)

    summed = lax.fori_loop(1, nkv, b_add, send_b[block(kv, rb), :].astype(F32))

    rates = summed[:, 4 * proj : 4 * proj + 128] + summed[:, 4 * proj + 128 :]
    lane_b = lax.broadcasted_iota(jnp.int32, rates.shape, 1)

    def pick(i):
        return jnp.sum(jnp.where(lane_b == i, rates, 0.0), axis=1, keepdims=True)

    row_scale = lax.rsqrt(pick(127) / width + EPSILON)
    repeat = 128 // rb
    for h in range(heads):
        at = slice(h * head, (h + 1) * head)
        beta_raw = pick(tp * heads + h) * row_scale
        decay_raw = pick(32 + tp * heads + h) * row_scale
        beta = 1.0 / (1.0 + jnp.exp(-beta_raw))
        softplus = jnp.maximum(decay_raw, 0.0) + jnp.log1p(jnp.exp(-jnp.abs(decay_raw)))
        decay = jnp.exp(-rate_ref[0, h] * softplus)
        query = silu(summed[:, 0 * proj : 1 * proj][:, at] * row_scale)
        query = query * lax.rsqrt(jnp.sum(query * query, axis=1, keepdims=True) + EPSILON)
        query = query * head ** (-0.5)
        key = silu(summed[:, 1 * proj : 2 * proj][:, at] * row_scale)
        key = key * lax.rsqrt(jnp.sum(key * key, axis=1, keepdims=True) + EPSILON)
        value = silu(summed[:, 2 * proj : 3 * proj][:, at] * row_scale)
        gate = summed[:, 3 * proj : 4 * proj][:, at] * row_scale
        key_t[h] = jnp.concatenate([key] * repeat, axis=0).T
        query_t[h] = jnp.concatenate([query] * repeat, axis=0).T
        shape = (rb, head)
        rows_s[0, h] = jnp.broadcast_to(decay, shape)
        rows_s[1, h] = jnp.broadcast_to(beta, shape)
        rows_s[2, h] = value
        rows_s[3, h] = jnp.broadcast_to(
            jnp.sum(key * query, axis=1, keepdims=True), shape
        )
        gate_s[:, at] = silu(gate)

    later_copies[0].wait()

    def delta(b):
        shift = lax.rem(128 - b, 128)
        for h in range(heads):
            state = st[b, h]
            key_b = pltpu.roll(key_t[h], shift, 1)[:, 0:1]
            query_b = pltpu.roll(query_t[h], shift, 1)[:, 0:1]
            decay = rows_s[0, h, pl.ds(b, 1), :]
            beta = rows_s[1, h, pl.ds(b, 1), :]
            value = rows_s[2, h, pl.ds(b, 1), :]
            key_query = rows_s[3, h, pl.ds(b, 1), :]
            recalled = decay * jnp.sum(state * key_b, axis=0, keepdims=True)
            change = beta * (value - recalled)
            old_read = decay * jnp.sum(state * query_b, axis=0, keepdims=True)
            readout_s[h, pl.ds(b, 1), :] = old_read + key_query * change
            st[b, h] = decay * state + key_b * change

    loop(0, rb, delta)
    state_out = pltpu.make_async_copy(st, new_state_ref, local_sem.at[9])
    state_out.start()

    own_rows = block(kv, rb)
    for h in range(heads):
        at = slice(h * head, (h + 1) * head)
        read = readout_s[h]
        scale = lax.rsqrt(jnp.sum(read * read, axis=1, keepdims=True) / head + EPSILON)
        merged[own_rows, at] = (read * scale * out_gain_ref[...] * gate_s[:, at]).astype(BF16)

    def d_copy(d, src_kv, peer):
        blk = merged.at[block(src_kv, rb), :]
        return remote(blk, blk, d_send.at[d], d_recv.at[src_kv], kv_dev(peer))

    loop(1, nkv, lambda d: d_copy(d, kv, lax.rem(kv + d, nkv)).start())

    def d_wait(d):
        src = lax.rem(kv + nkv - d, nkv)
        d_copy(d, src, src).wait_recv()

    later_copies[1].wait()
    loop(1, nkv, d_wait)

    part = jnp.dot(merged[...], w_out[...], preferred_element_type=F32)
    own_e[...] = part
    send_e[...] = part.astype(BF16)

    def e_copy(d, dest_tp, src_tp, peer):
        return remote(
            send_e.at[block(dest_tp, rt), :],
            recv_e.at[src_tp],
            e_send.at[d],
            e_recv.at[src_tp],
            tp_dev(peer),
        )

    def e_start(d):
        peer = lax.rem(tp + d, ntp)
        e_copy(d, peer, tp, peer).start()

    loop(1, ntp, e_start)

    def e_add(d, acc):
        src = lax.rem(tp + ntp - d, ntp)
        e_copy(d, tp, src, src).wait_recv()
        return acc + recv_e[src].astype(F32)

    my_rows = block(tp, rt)
    branch = lax.fori_loop(1, ntp, e_add, own_e[my_rows, :])
    res[kv, my_rows, :] = (col_n[my_rows, :].astype(F32) + branch).astype(BF16)

    def f1_copy(d, src_tp, peer):
        blk = res.at[kv, block(src_tp, rt), :]
        return remote(blk, blk, f1_send.at[d], f1_recv.at[src_tp], tp_dev(peer))

    loop(1, ntp, lambda d: f1_copy(d, tp, lax.rem(tp + d, ntp)).start())

    def f1_wait(d):
        src = lax.rem(tp + ntp - d, ntp)
        f1_copy(d, src, src).wait_recv()

    loop(1, ntp, f1_wait)

    rows_a = pl.ds(pl.multiple_of(c * rh, rc), rc)
    rows_b = pl.ds(pl.multiple_of(c * rh + rc, rc), rc)
    other = nc - 1 - c
    other_a = pl.ds(pl.multiple_of(other * rh, rc), rc)
    other_b = pl.ds(pl.multiple_of(other * rh + rc, rc), rc)

    def fa_copy(k, slot, dev):
        blk = res.at[k, rows_a, :]
        return remote(blk, blk, fa_send.at[slot], fa_recv.at[k], dev)

    def fb_copy(k, slot, dev):
        blk = res.at[k, rows_b, :]
        return remote(blk, blk, fb_send.at[slot], fb_recv.at[k], dev)

    def y_dev(d):
        return {"kv_1": lax.rem(y + d, ny)}

    def z_dev(d):
        return {"kv_0": lax.rem(z + d, nz)}

    def fp_copy(k, half, at):
        blk = res.at[k, at, :]
        return remote(blk, blk, fp_send.at[half, k], fp_recv.at[half, k], partner)

    for d in range(1, ny):
        fa_copy(kv, d - 1, y_dev(d)).start()
    for d in range(1, nz):
        fb_copy(kv, d - 1, z_dev(d)).start()
    a_base, b_base = ny - 1, nz - 1
    for d in range(1, nz):
        fa_copy(kv, a_base + d - 1, z_dev(d)).start()
    for d in range(1, ny):
        fb_copy(kv, b_base + d - 1, y_dev(d)).start()

    res_t[...] = res[kv].astype(F32).T

    for i in range(1, max(ny, nz)):
        if i < ny:
            k = z * ny + lax.rem(y + ny - i, ny)
            fa_copy(k, 0, partner).wait_recv()
            for d in range(1, nz):
                fa_copy(k, a_base + i * (nz - 1) + d - 1, z_dev(d)).start()
            fp_copy(k, 0, rows_a).start()
        if i < nz:
            k = lax.rem(z + nz - i, nz) * ny + y
            fb_copy(k, 0, partner).wait_recv()
            for d in range(1, ny):
                fb_copy(k, b_base + i * (ny - 1) + d - 1, y_dev(d)).start()
            fp_copy(k, 1, rows_b).start()

    def fa_late(i):
        zd, yd = 1 + lax.rem(i, nz - 1), i // (nz - 1)
        k = lax.rem(z + nz - zd, nz) * ny + lax.rem(y + ny - yd, ny)
        fa_copy(k, 0, partner).wait_recv()
        fp_copy(k, 0, rows_a).start()

    def fb_late(i):
        yd, zd = 1 + lax.rem(i, ny - 1), i // (ny - 1)
        k = lax.rem(z + nz - zd, nz) * ny + lax.rem(y + ny - yd, ny)
        fb_copy(k, 0, partner).wait_recv()
        fp_copy(k, 1, rows_b).start()

    loop(0, (nz - 1) * ny, fa_late)
    loop(0, (ny - 1) * nz, fb_late)

    def fp_wait(d):
        k = lax.rem(kv + d, nkv)
        fp_copy(k, 0, other_a).wait_recv()
        fp_copy(k, 1, other_b).wait_recv()

    loop(1, nkv, fp_wait)

    def square_sum(k, acc):
        blk = res[k].astype(F32)
        sq = blk * blk
        for i in range(dk // 128):
            acc = acc + sq[:, i * 128 : (i + 1) * 128]
        return acc

    total = lax.fori_loop(0, nkv, square_sum, jnp.zeros((rows, 128), F32))
    scale = lax.rsqrt(jnp.sum(total, axis=1, keepdims=True) / width + EPSILON)
    later_copies[2].wait()
    acc_up[...] = jnp.zeros_like(acc_up)

    def up(k):
        at = block(k, dk)
        blk = (res[k].astype(F32) * scale * mlp_gain_ref[:, at]).astype(BF16)
        acc_up[...] += jnp.dot(blk, w_up[at, :], preferred_element_type=F32)

    loop(0, nkv, up)
    relu = jnp.maximum(acc_up[...], 0.0)
    hid[...] = (relu * relu).astype(BF16)
    later_copies[3].wait()

    def hd_copy(k):
        return remote(send_d.at[k], recv_d.at[k], hd_send.at[k], hd_recv.at[k], partner)

    half_other = pl.ds(pl.multiple_of(other * rh, rh), rh)
    half_own = pl.ds(pl.multiple_of(c * rh, rh), rh)

    def down_other(i):
        k = lax.rem(kv + 1 + i, nkv)
        out = jnp.dot(hid[half_other, :], w_down[:, block(k, dk)], preferred_element_type=F32)
        send_d[k] = out.astype(BF16)
        hd_copy(k).start()

    loop(0, nkv, down_other)

    part_a, part_b = pl.ds(0, rc), pl.ds(rc, rc)

    def h1a_copy(k, src_z, dev):
        yk = lax.rem(k, ny)
        return remote(
            send_h.at[k, part_a, :],
            recv_h1a.at[src_z, yk],
            h1a_send.at[k],
            h1a_recv.at[src_z, yk],
            dev,
        )

    def h1b_copy(k, src_y, dev):
        zk = k // ny
        return remote(
            send_h.at[k, part_b, :],
            recv_h1b.at[src_y, zk],
            h1b_send.at[k],
            h1b_recv.at[src_y, zk],
            dev,
        )

    def down_own(i):
        k = lax.rem(kv + 1 + i, nkv)
        zk, yk = k // ny, lax.rem(k, ny)
        out = jnp.dot(hid[half_own, :], w_down[:, block(k, dk)], preferred_element_type=F32)
        hd_copy(k).wait_recv()
        send_h[k] = (out + recv_d[k].astype(F32)).astype(BF16)

        @pl.when(zk != z)
        def _():
            h1a_copy(k, z, {"kv_0": zk}).start()

        @pl.when(yk != y)
        def _():
            h1b_copy(k, y, {"kv_1": yk}).start()

    loop(0, nkv, down_own)

    def h1a_sum(yk):
        acc = send_h[z * ny + yk, 0:rc, :].astype(F32)
        for d in range(1, nz):
            src = lax.rem(z + nz - d, nz)
            h1a_copy(z * ny + yk, src, partner).wait_recv()
            acc = acc + recv_h1a[src, yk].astype(F32)
        return acc

    def h1b_sum(zk):
        acc = send_h[zk * ny + y, rc : 2 * rc, :].astype(F32)
        for d in range(1, ny):
            src = lax.rem(y + ny - d, ny)
            h1b_copy(zk * ny + y, src, partner).wait_recv()
            acc = acc + recv_h1b[src, zk].astype(F32)
        return acc

    def h2a_copy(d, yk, src_y, dev):
        return remote(
            send_h2a.at[yk], recv_h2a.at[src_y], h2_send.at[0, d], h2a_recv.at[src_y], dev
        )

    def h2b_copy(d, zk, src_z, dev):
        return remote(
            send_h2b.at[zk], recv_h2b.at[src_z], h2_send.at[1, d], h2b_recv.at[src_z], dev
        )

    for d in range(1, max(ny, nz)):
        if d < ny:
            yk = lax.rem(y + d, ny)
            send_h2a[yk] = h1a_sum(yk).astype(BF16)
            h2a_copy(d, yk, y, {"kv_1": yk}).start()
        if d < nz:
            zk = lax.rem(z + d, nz)
            send_h2b[zk] = h1b_sum(zk).astype(BF16)
            h2b_copy(d, zk, z, {"kv_0": zk}).start()
    sum_a = h1a_sum(y)
    sum_b = h1b_sum(z)
    for d in range(1, ny):
        src = lax.rem(y + ny - d, ny)
        h2a_copy(d, y, src, partner).wait_recv()
        sum_a = sum_a + recv_h2a[src].astype(F32)
    for d in range(1, nz):
        src = lax.rem(z + nz - d, nz)
        h2b_copy(d, z, src, partner).wait_recv()
        sum_b = sum_b + recv_h2b[src].astype(F32)

    own_sum = jnp.concatenate([sum_a, sum_b], axis=0).T.astype(BF16)
    send_x[...] = own_sum

    def x_copy(d, dest_tp, src_tp, peer):
        return remote(
            send_x.at[block(dest_tp, dt), :],
            recv_x.at[src_tp],
            x_send.at[d],
            x_recv.at[src_tp],
            tp_dev(peer),
        )

    def x_start(d):
        peer = lax.rem(tp + d, ntp)
        x_copy(d, peer, tp, peer).start()

    loop(1, ntp, x_start)
    recv_x[tp] = send_x[block(tp, dt), :]

    def x_wait(d):
        src = lax.rem(tp + ntp - d, ntp)
        x_copy(d, tp, src, src).wait_recv()

    loop(1, ntp, x_wait)
    for cc in range(nc):
        at = slice(cc * rh, (cc + 1) * rh)
        acc = res_t[block(tp, dt), at]
        branch = recv_x[cc].astype(F32)
        for xx in range(1, nx):
            branch = branch + recv_x[xx * nc + cc].astype(F32)
        mixed_ref[:, at] = (acc + branch).astype(BF16)

    def tp_sends(d):
        peer = lax.rem(tp + d, ntp)
        a_copy(d, tp, peer).wait_send()
        e_copy(d, peer, tp, peer).wait_send()
        f1_copy(d, tp, peer).wait_send()
        x_copy(d, peer, tp, peer).wait_send()

    loop(1, ntp, tp_sends)

    def kv_sends(d):
        peer = lax.rem(kv + d, nkv)
        b_copy(d, peer, kv, peer).wait_send()
        d_copy(d, kv, peer).wait_send()
        fp_copy(peer, 0, rows_a).wait_send()
        fp_copy(peer, 1, rows_b).wait_send()

    loop(1, nkv, kv_sends)
    loop(0, a_base + ny * (nz - 1), lambda i: fa_copy(kv, i, partner).wait_send())
    loop(0, b_base + nz * (ny - 1), lambda i: fb_copy(kv, i, partner).wait_send())

    def h_sends(k):
        zk, yk = k // ny, lax.rem(k, ny)
        hd_copy(k).wait_send()

        @pl.when(zk != z)
        def _():
            h1a_copy(k, z, {"kv_0": zk}).wait_send()

        @pl.when(yk != y)
        def _():
            h1b_copy(k, y, {"kv_1": yk}).wait_send()

    loop(0, nkv, h_sends)
    for d in range(1, ny):
        h2a_copy(d, lax.rem(y + d, ny), y, partner).wait_send()
    for d in range(1, nz):
        h2b_copy(d, lax.rem(z + d, nz), z, partner).wait_send()
    state_out.wait()


def local(
    sizes,
    tokens,
    mix_gain,
    w_query,
    w_key,
    w_value,
    w_gate,
    w_beta,
    w_decay,
    decay_rate,
    out_gain,
    state,
    w_out,
    mlp_gain,
    w_up,
    w_down,
):
    nz, ny, nx, nc = sizes
    nkv, ntp = nz * ny, nx * nc
    rows, dt = tokens.shape
    dk = dt * ntp
    rb, heads, head, _ = state.shape
    proj = heads * head
    sent = 4 * proj + 256
    ff = w_up.shape[1]
    rt, rh = rows // ntp, rows // nc
    rc = rh // 2
    vmem, dma = pltpu.VMEM, pltpu.SemaphoreType.DMA
    scratch = [
        vmem((dk, rows), BF16),
        vmem((4, dk, proj), BF16),
        vmem((128, dk), BF16),
        vmem(w_out.shape, BF16),
        vmem(w_up.shape, BF16),
        vmem(w_down.shape, BF16),
        vmem(state.shape, F32),
        vmem((rows, dk), BF16),
        vmem((rows, sent), BF16),
        vmem((nkv, rb, sent), BF16),
        vmem((heads, head, 128), F32),
        vmem((heads, head, 128), F32),
        vmem((4, heads, rb, head), F32),
        vmem((heads, rb, head), F32),
        vmem((rb, proj), F32),
        vmem((rows, proj), BF16),
        vmem((rows, dk), BF16),
        vmem((rows, dk), F32),
        vmem((ntp, rt, dk), BF16),
        vmem((nkv, rows, dk), BF16),
        vmem((dk, rows), F32),
        vmem((rows, ff), BF16),
        vmem((rows, ff), F32),
        vmem((nkv, rh, dk), BF16),
        vmem((nkv, rh, dk), BF16),
        vmem((nkv, rh, dk), BF16),
        vmem((nz, ny, rc, dk), BF16),
        vmem((ny, nz, rc, dk), BF16),
        vmem((ny, rc, dk), BF16),
        vmem((nz, rc, dk), BF16),
        vmem((ny, rc, dk), BF16),
        vmem((nz, rc, dk), BF16),
        vmem((dk, rh), BF16),
        vmem((ntp, dt, rh), BF16),
        dma((10,)),
        dma((ntp,)),
        dma((ntp,)),
        dma((nkv,)),
        dma((nkv,)),
        dma((nkv,)),
        dma((nkv,)),
        dma((ntp,)),
        dma((ntp,)),
        dma((ntp,)),
        dma((ntp,)),
        dma((ny - 1 + ny * (nz - 1),)),
        dma((nz - 1 + nz * (ny - 1),)),
        dma((nkv,)),
        dma((nkv,)),
        dma((2, nkv)),
        dma((2, nkv)),
        dma((nkv,)),
        dma((nkv,)),
        dma((nkv,)),
        dma((nkv,)),
        dma((nz, ny)),
        dma((ny, nz)),
        dma((2, max(ny, nz))),
        dma((ny,)),
        dma((nz,)),
        dma((ntp,)),
        dma((ntp,)),
    ]
    in_hbm = pl.BlockSpec(memory_space=pl.ANY)
    in_vmem = pl.BlockSpec(memory_space=pltpu.VMEM)
    in_smem = pl.BlockSpec(memory_space=pltpu.SMEM)
    mixed_t, new_state = pl.pallas_call(
        functools.partial(layer_kernel, sizes),
        out_shape=(
            jax.ShapeDtypeStruct((dt, rows), BF16),
            jax.ShapeDtypeStruct(state.shape, F32),
        ),
        in_specs=[
            in_hbm,
            in_vmem,
            in_hbm,
            in_hbm,
            in_hbm,
            in_hbm,
            in_vmem,
            in_vmem,
            in_smem,
            in_vmem,
            in_hbm,
            in_hbm,
            in_vmem,
            in_hbm,
            in_hbm,
        ],
        out_specs=(in_vmem, in_hbm),
        scratch_shapes=scratch,
        compiler_params=pltpu.CompilerParams(
            collective_id=0, has_side_effects=True, vmem_limit_bytes=67_000_000
        ),
        name="layer",
    )(
        tokens.T,
        mix_gain[None, :],
        w_query,
        w_key,
        w_value,
        w_gate,
        w_beta.T,
        w_decay.T,
        decay_rate[None, :],
        out_gain[None, :],
        state,
        w_out,
        mlp_gain[None, :],
        w_up,
        w_down,
    )
    return mixed_t.T, new_state


def solution(mesh):
    n = dict(mesh.shape)
    sizes = (n["kv"] // 4, 4, n["tp"] // 2, 2) if n["kv"] >= 8 else (2, n["kv"] // 2, n["tp"] // 2, 2)
    torus = Mesh(mesh.devices.reshape(sizes), KV_TP)
    in_specs = (
        P(None, KV_TP),
        P(KV),
        P(KV, TP),
        P(KV, TP),
        P(KV, TP),
        P(KV, TP),
        P(KV, None),
        P(KV, None),
        P(TP),
        P(),
        P(KV, TP, None, None),
        P(TP, KV),
        P(),
        P(None, KV_TP),
        P(KV_TP, None),
    )
    out_specs = (P(None, KV_TP), P(KV, TP, None, None))
    return jax.shard_map(
        functools.partial(local, sizes),
        mesh=torus,
        in_specs=in_specs,
        out_specs=out_specs,
        check_vma=False,
    )
```

```python
import functools
import math

import jax
import jax.numpy as jnp
from jax import lax
from jax.experimental import pallas as pl
from jax.experimental.pallas import tpu as pltpu
from jax.sharding import Mesh
from jax.sharding import PartitionSpec as P

EPSILON = 1e-06
MESH = pl.DeviceIdType.MESH
KV_TP = ("kv_0", "kv_1", "tp_0", "tp_1")
KV = ("kv_0", "kv_1")
TP = ("tp_0", "tp_1")
F32 = jnp.float32
BF16 = jnp.bfloat16


def silu(v):
    return v / (1.0 + jnp.exp(-v))


def layer_kernel(
    sizes,
    tok_ref,
    mix_gain_ref,
    wq_ref,
    wk_ref,
    wv_ref,
    wg_ref,
    wbeta_ref,
    wdecay_ref,
    rate_ref,
    out_gain_ref,
    state_ref,
    wout_ref,
    mlp_gain_ref,
    wup_ref,
    wdown_ref,
    mixed_ref,
    new_state_ref,
    col_t,
    w_proj,
    w_rates,
    w_beta,
    w_decay,
    mix_gain,
    out_gain,
    mlp_gain,
    rate,
    w_out,
    w_up,
    w_down,
    st,
    col_n,
    send_b,
    recv_b1a,
    recv_b1b,
    send_b2a,
    send_b2b,
    recv_b2a,
    recv_b2b,
    key_t,
    query_t,
    rows_s,
    merged,
    send_e,
    recv_e,
    recv_ex,
    res,
    res_t,
    hid,
    acc_up,
    total_sq,
    own_d,
    send_d,
    recv_d,
    send_h,
    recv_h1a,
    recv_h1b,
    send_h2a,
    send_h2b,
    recv_h2a,
    recv_h2b,
    send_x,
    recv_x,
    local_sem,
    a_send,
    a_recv,
    b1a_send,
    b1b_send,
    b1a_recv,
    b1b_recv,
    b2_send,
    b2a_recv,
    b2b_recv,
    d_send,
    d_recv,
    e_send,
    e_recv,
    ex_send,
    ex_recv,
    fa_send,
    fb_send,
    fa_recv,
    fb_recv,
    fp_send,
    fp_recv,
    hd_send,
    hd_recv,
    h1a_send,
    h1b_send,
    h1a_recv,
    h1b_recv,
    h2_send,
    h2a_recv,
    h2b_recv,
    x_send,
    x_recv,
):
    nz, ny, nx, nc = sizes
    nkv, ntp = nz * ny, nx * nc
    z, y = lax.axis_index("kv_0"), lax.axis_index("kv_1")
    x, c = lax.axis_index("tp_0"), lax.axis_index("tp_1")
    kv, tp = z * ny + y, x * nc + c
    partner = {"tp_1": nc - 1 - c}

    dt, rows = tok_ref.shape
    dk = dt * ntp
    width = dk * nkv
    rb, heads, head = st.shape[0], st.shape[1], st.shape[2]
    proj = heads * head
    rh = rows // nc
    rc = rh // 2
    cols_a = 2 * proj
    cols_b = 2 * proj + 128
    other = nc - 1 - c

    def kv_dev(k):
        return {"kv_0": k // ny, "kv_1": lax.rem(k, ny)}

    def tp_dev(t):
        return {"tp_0": t // nc, "tp_1": lax.rem(t, nc)}

    def remote(src, dst, send_sem, recv_sem, dev):
        return pltpu.make_async_remote_copy(
            src_ref=src,
            dst_ref=dst,
            send_sem=send_sem,
            recv_sem=recv_sem,
            device_id=dev,
            device_id_type=MESH,
        )

    def loop(lo, hi, body):
        def wrapped(i, carry):
            body(i)
            return carry

        lax.fori_loop(lo, hi, wrapped, 0)

    def block(i, n):
        return pl.ds(pl.multiple_of(i * n, n), n)

    own_tok = col_t.at[block(tp, dt), :]
    first = (
        (tok_ref, own_tok),
        (wbeta_ref, w_beta),
        (wdecay_ref, w_decay),
        (mix_gain_ref, mix_gain),
        (wq_ref, w_proj.at[0]),
        (wk_ref, w_proj.at[1]),
        (wv_ref, w_proj.at[2]),
        (wg_ref, w_proj.at[3]),
        (rate_ref, rate),
        (out_gain_ref, out_gain),
        (mlp_gain_ref, mlp_gain),
        (state_ref, st),
        (wout_ref, w_out),
        (wup_ref, w_up),
        (wdown_ref, w_down),
    )
    copies = [
        pltpu.make_async_copy(src, dst, local_sem.at[i]) for i, (src, dst) in enumerate(first)
    ]
    for copy in copies:
        copy.start()

    barrier = pltpu.get_barrier_semaphore()

    def greet(dev):
        pl.semaphore_signal(barrier, inc=1, device_id=dev, device_id_type=MESH)

    def greet_tp(d):
        greet(tp_dev(lax.rem(tp + d, ntp)))

    loop(1, ntp, greet_tp)
    for d in range(1, ny):
        greet({"kv_1": lax.rem(y + d, ny)})
    for d in range(1, nz):
        greet({"kv_0": lax.rem(z + d, nz)})

    n_heads = wbeta_ref.shape[0]
    copies[1].wait()
    copies[2].wait()
    w_rates[...] = jnp.zeros_like(w_rates)
    w_rates[0:n_heads, :] = w_beta[...]
    w_rates[32 : 32 + n_heads, :] = w_decay[...]

    copies[0].wait()
    copies[3].wait()
    pl.semaphore_wait(barrier, ntp - 1 + ny - 1 + nz - 1)

    def a_copy(d, src_tp, peer):
        blk = col_t.at[block(src_tp, dt), :]
        return remote(blk, blk, a_send.at[d], a_recv.at[src_tp], tp_dev(peer))

    loop(1, ntp, lambda d: a_copy(d, tp, lax.rem(tp + d, ntp)).start())

    def a_wait(d):
        src = lax.rem(tp + ntp - d, ntp)
        a_copy(d, src, src).wait_recv()

    loop(1, ntp, a_wait)

    cols = col_t[...].astype(F32).T
    col_n[...] = cols.astype(BF16)
    normed = (cols * mix_gain[...]).astype(BF16)
    squares = jnp.sum(cols * cols, axis=1, keepdims=True)

    def project(i):
        copies[4 + i].wait()
        return jnp.dot(normed, w_proj[i], preferred_element_type=F32).astype(BF16)

    def b1a_copy(k, src_z, dev):
        yk = lax.rem(k, ny)
        return remote(
            send_b.at[block(k, rb), pl.ds(0, cols_a)],
            recv_b1a.at[src_z, yk],
            b1a_send.at[k],
            b1a_recv.at[src_z, yk],
            dev,
        )

    def b1b_copy(k, src_y, dev):
        zk = k // ny
        return remote(
            send_b.at[block(k, rb), pl.ds(cols_a, cols_b)],
            recv_b1b.at[src_y, zk],
            b1b_send.at[k],
            b1b_recv.at[src_y, zk],
            dev,
        )

    for i in range(2):
        send_b[:, i * proj : (i + 1) * proj] = project(i)

    def b1a_start(i):
        yk, zk = lax.rem(y + 1 + i // (nz - 1), ny), lax.rem(z + 1 + lax.rem(i, nz - 1), nz)
        b1a_copy(zk * ny + yk, z, {"kv_0": zk}).start()

    loop(0, ny * (nz - 1), b1a_start)

    contract_last = (((1,), (1,)), ((), ()))
    rates_part = lax.dot_general(
        normed, w_rates[...], contract_last, preferred_element_type=F32
    )
    lane = lax.broadcasted_iota(jnp.int32, rates_part.shape, 1)
    rates_part = jnp.where(lane == 63, squares, rates_part)
    high = rates_part.astype(BF16).astype(F32)
    low = pltpu.roll(rates_part - high, 64, 1)
    send_b[:, 4 * proj :] = jnp.where(lane < 64, high, low).astype(BF16)
    for i in range(2, 4):
        send_b[:, i * proj : (i + 1) * proj] = project(i)

    def b1b_start(i):
        zk, yk = lax.rem(z + 1 + i // (ny - 1), nz), lax.rem(y + 1 + lax.rem(i, ny - 1), ny)
        b1b_copy(zk * ny + yk, y, {"kv_1": yk}).start()

    loop(0, nz * (ny - 1), b1b_start)

    def b1a_sum(yk):
        k = z * ny + yk
        acc = send_b[block(k, rb), 0:cols_a].astype(F32)
        for d in range(1, nz):
            src = lax.rem(z + nz - d, nz)
            b1a_copy(k, src, partner).wait_recv()
            acc = acc + recv_b1a[src, yk].astype(F32)
        return acc

    def b1b_sum(zk):
        k = zk * ny + y
        acc = send_b[block(k, rb), cols_a : cols_a + cols_b].astype(F32)
        for d in range(1, ny):
            src = lax.rem(y + ny - d, ny)
            b1b_copy(k, src, partner).wait_recv()
            acc = acc + recv_b1b[src, zk].astype(F32)
        return acc

    def b2a_copy(d, yk, src_y, dev):
        return remote(
            send_b2a.at[yk], recv_b2a.at[src_y], b2_send.at[0, d], b2a_recv.at[src_y], dev
        )

    def b2b_copy(d, zk, src_z, dev):
        return remote(
            send_b2b.at[zk], recv_b2b.at[src_z], b2_send.at[1, d], b2b_recv.at[src_z], dev
        )

    for d in range(1, max(ny, nz)):
        if d < ny:
            yk = lax.rem(y + d, ny)
            send_b2a[yk] = b1a_sum(yk).astype(BF16)
            b2a_copy(d, yk, y, {"kv_1": yk}).start()
        if d < nz:
            zk = lax.rem(z + d, nz)
            send_b2b[zk] = b1b_sum(zk).astype(BF16)
            b2b_copy(d, zk, z, {"kv_0": zk}).start()
    sum_a = b1a_sum(y)
    sum_b = b1b_sum(z)

    for d in range(1, nz):
        src = lax.rem(z + nz - d, nz)
        b2b_copy(d, z, src, partner).wait_recv()
        sum_b = sum_b + recv_b2b[src].astype(F32)
    for d in range(1, ny):
        src = lax.rem(y + ny - d, ny)
        b2a_copy(d, y, src, partner).wait_recv()
        sum_a = sum_a + recv_b2a[src].astype(F32)

    rates = sum_b[:, 2 * proj :]
    rates = rates + pltpu.roll(rates, 64, 1)
    lane_b = lax.broadcasted_iota(jnp.int32, rates.shape, 1)

    def pick(i):
        return jnp.sum(jnp.where(lane_b == i, rates, 0.0), axis=1, keepdims=True)

    for i in range(8, 12):
        copies[i].wait()
    row_scale = lax.rsqrt(pick(63) / width + EPSILON)
    repeat = 128 // rb
    group = 4
    gates = []
    for h in range(heads):
        at = slice(h * head, (h + 1) * head)
        beta_raw = pick(tp * heads + h) * row_scale
        decay_raw = pick(32 + tp * heads + h) * row_scale
        beta = 1.0 / (1.0 + jnp.exp(-beta_raw))
        softplus = jnp.maximum(decay_raw, 0.0) + jnp.log1p(jnp.exp(-jnp.abs(decay_raw)))
        decay = jnp.exp(-rate[0:1, h : h + 1] * softplus)
        query = silu(sum_a[:, :proj][:, at] * row_scale)
        query = query * lax.rsqrt(jnp.sum(query * query, axis=1, keepdims=True) + EPSILON)
        query = query * head ** (-0.5)
        key = silu(sum_a[:, proj:][:, at] * row_scale)
        key = key * lax.rsqrt(jnp.sum(key * key, axis=1, keepdims=True) + EPSILON)
        key_tr = jnp.concatenate([key] * repeat, axis=0).T
        query_tr = jnp.concatenate([query] * repeat, axis=0).T
        for g in range(rb // group):
            key_t[g, h] = pltpu.roll(key_tr, (128 - g * group) % 128, 1) if g else key_tr
            query_t[g, h] = pltpu.roll(query_tr, (128 - g * group) % 128, 1) if g else query_tr
        shape = (rb, head)
        rows_s[0, h] = jnp.broadcast_to(decay, shape)
        rows_s[1, h] = jnp.broadcast_to(beta, shape)
        rows_s[2, h] = silu(sum_b[:, :proj][:, at] * row_scale)
        rows_s[3, h] = jnp.broadcast_to(
            jnp.sum(key * query, axis=1, keepdims=True), shape
        )
        gates.append(silu(sum_b[:, proj : 2 * proj][:, at] * row_scale))

    def read_group(g):
        for i in range(group):
            b = g * group + i
            for h in range(heads):
                state = st[b, h]
                rows_s[4, h, pl.ds(b, 1), :] = jnp.sum(
                    state * key_t[g, h, :, i : i + 1], axis=0, keepdims=True
                )
                rows_s[5, h, pl.ds(b, 1), :] = jnp.sum(
                    state * query_t[g, h, :, i : i + 1], axis=0, keepdims=True
                )

    loop(0, rb // group, read_group)

    own_rows = block(kv, rb)
    for h in range(heads):
        at = slice(h * head, (h + 1) * head)
        decay = rows_s[0, h]
        change = rows_s[1, h] * (rows_s[2, h] - decay * rows_s[4, h])
        read = decay * rows_s[5, h] + rows_s[3, h] * change
        rows_s[4, h] = change
        scale = lax.rsqrt(jnp.sum(read * read, axis=1, keepdims=True) / head + EPSILON)
        merged[own_rows, at] = (read * scale * out_gain[...] * gates[h]).astype(BF16)

    def d_copy(d, src_kv, peer):
        blk = merged.at[block(src_kv, rb), :]
        return remote(blk, blk, d_send.at[d], d_recv.at[src_kv], kv_dev(peer))

    loop(1, nkv, lambda d: d_copy(d, kv, lax.rem(kv + d, nkv)).start())

    def d_wait(d):
        src = lax.rem(kv + nkv - d, nkv)
        d_copy(d, src, src).wait_recv()

    def write_group(g):
        for i in range(group):
            b = g * group + i
            for h in range(heads):
                new_state_ref[b, h] = (
                    rows_s[0, h, pl.ds(b, 1), :] * st[b, h]
                    + key_t[g, h, :, i : i + 1] * rows_s[4, h, pl.ds(b, 1), :]
                )

    loop(0, rb // group, write_group)
    copies[12].wait()
    loop(1, nkv, d_wait)

    half_other = pl.ds(pl.multiple_of(other * rh, rh), rh)
    half_own = pl.ds(pl.multiple_of(c * rh, rh), rh)
    e_copy = remote(send_e, recv_e, e_send, e_recv, partner)
    send_e[...] = jnp.dot(
        merged[half_other, :], w_out[...], preferred_element_type=F32
    ).astype(BF16)
    e_copy.start()
    part = jnp.dot(merged[half_own, :], w_out[...], preferred_element_type=F32)
    e_copy.wait_recv()
    recv_ex[x] = (part + recv_e[...].astype(F32)).astype(BF16)

    def ex_copy(d, src_x, dev):
        blk = recv_ex.at[src_x]
        return remote(blk, blk, ex_send.at[d], ex_recv.at[src_x], dev)

    for d in range(1, nx):
        ex_copy(d, x, {"tp_0": lax.rem(x + d, nx)}).start()
    for d in range(1, nx):
        ex_copy(d, lax.rem(x + nx - d, nx), partner).wait_recv()
    branch = recv_ex[0].astype(F32)
    for i in range(1, nx):
        branch = branch + recv_ex[i].astype(F32)
    res[kv, half_own, :] = (col_n[half_own, :].astype(F32) + branch).astype(BF16)

    rows_a = pl.ds(pl.multiple_of(c * rh, rc), rc)
    rows_b = pl.ds(pl.multiple_of(c * rh + rc, rc), rc)
    other_a = pl.ds(pl.multiple_of(other * rh, rc), rc)
    other_b = pl.ds(pl.multiple_of(other * rh + rc, rc), rc)

    def fa_copy(k, slot, dev):
        blk = res.at[k, rows_a, :]
        return remote(blk, blk, fa_send.at[slot], fa_recv.at[k], dev)

    def fb_copy(k, slot, dev):
        blk = res.at[k, rows_b, :]
        return remote(blk, blk, fb_send.at[slot], fb_recv.at[k], dev)

    def y_dev(d):
        return {"kv_1": lax.rem(y + d, ny)}

    def z_dev(d):
        return {"kv_0": lax.rem(z + d, nz)}

    def fp_copy(k, half, at):
        blk = res.at[k, at, :]
        return remote(blk, blk, fp_send.at[half, k], fp_recv.at[half, k], partner)

    for d in range(1, ny):
        fa_copy(kv, d - 1, y_dev(d)).start()
    for d in range(1, nz):
        fb_copy(kv, d - 1, z_dev(d)).start()
    a_base, b_base = ny - 1, nz - 1
    for d in range(1, nz):
        fa_copy(kv, a_base + d - 1, z_dev(d)).start()
    for d in range(1, ny):
        fb_copy(kv, b_base + d - 1, y_dev(d)).start()

    fp_copy(kv, 0, rows_a).start()
    fp_copy(kv, 1, rows_b).start()

    for i in range(1, max(ny, nz)):
        if i < ny:
            k = z * ny + lax.rem(y + ny - i, ny)
            fa_copy(k, 0, partner).wait_recv()
            for d in range(1, nz):
                fa_copy(k, a_base + i * (nz - 1) + d - 1, z_dev(d)).start()
            fp_copy(k, 0, rows_a).start()
        if i < nz:
            k = lax.rem(z + nz - i, nz) * ny + y
            fb_copy(k, 0, partner).wait_recv()
            for d in range(1, ny):
                fb_copy(k, b_base + i * (ny - 1) + d - 1, y_dev(d)).start()
            fp_copy(k, 1, rows_b).start()

    n_late = max((nz - 1) * ny, (ny - 1) * nz)

    def late(i):
        zd, yd = 1 + lax.rem(i, nz - 1), i // (nz - 1)
        k = lax.rem(z + nz - zd, nz) * ny + lax.rem(y + ny - yd, ny)
        fa_copy(k, 0, partner).wait_recv()
        fp_copy(k, 0, rows_a).start()
        yd, zd = 1 + lax.rem(i, ny - 1), i // (ny - 1)
        k = lax.rem(z + nz - zd, nz) * ny + lax.rem(y + ny - yd, ny)
        fb_copy(k, 0, partner).wait_recv()
        fp_copy(k, 1, rows_b).start()

    def up(j):
        k = lax.rem(z + nz - j // ny, nz) * ny + lax.rem(y + ny - lax.rem(j, ny), ny)
        fp_copy(k, 0, other_a).wait_recv()
        fp_copy(k, 1, other_b).wait_recv()
        at = block(k, dk)
        blk = res[k].astype(F32)
        sq = blk * blk
        total = total_sq[...]
        for i in range(dk // 128):
            total = total + sq[:, i * 128 : (i + 1) * 128]
        total_sq[...] = total
        acc_up[...] += jnp.dot(
            (blk * mlp_gain[:, at]).astype(BF16), w_up[at, :], preferred_element_type=F32
        )

    lag = 0
    for j in range(1, nkv):
        zd, yd = j // ny, j % ny
        ready = max(yd * (nz - 1) + zd - 1 if zd else 0, zd * (ny - 1) + yd - 1 if yd else 0)
        lag = max(lag, ready - (j - 1))

    acc_up[...] = jnp.zeros_like(acc_up)
    total_sq[...] = jnp.zeros_like(total_sq)
    copies[13].wait()
    up(0)
    res_t[...] = res[kv].astype(F32).T
    loop(0, lag, late)

    def late_and_up(i):
        late(i)
        up(i - lag + 1)

    loop(lag, n_late, late_and_up)

    loop(n_late - lag + 1, nkv, up)

    copies[14].wait()
    scale = lax.rsqrt(jnp.sum(total_sq[...], axis=1, keepdims=True) / width + EPSILON)
    relu = jnp.maximum(acc_up[...] * scale, 0.0)
    acc_up[...] = relu * relu
    hid[0:rh, :] = acc_up[half_other, :].astype(BF16)
    hid[rh:, :] = acc_up[half_own, :].astype(BF16)

    def hd_copy(k):
        return remote(send_d.at[k], recv_d.at[k], hd_send.at[k], hd_recv.at[k], partner)

    def down(i):
        k = lax.rem(kv + 1 + i, nkv)
        out = jnp.dot(hid[...], w_down[:, block(k, dk)], preferred_element_type=F32)
        send_d[k] = out[:rh].astype(BF16)
        hd_copy(k).start()
        own_d[k] = out[rh:]

    part_a, part_b = pl.ds(0, rc), pl.ds(rc, rc)

    def h1a_copy(k, src_z, dev):
        yk = lax.rem(k, ny)
        return remote(
            send_h.at[k, part_a, :],
            recv_h1a.at[src_z, yk],
            h1a_send.at[k],
            h1a_recv.at[src_z, yk],
            dev,
        )

    def h1b_copy(k, src_y, dev):
        zk = k // ny
        return remote(
            send_h.at[k, part_b, :],
            recv_h1b.at[src_y, zk],
            h1b_send.at[k],
            h1b_recv.at[src_y, zk],
            dev,
        )

    def joined(i):
        k = lax.rem(kv + 1 + i, nkv)
        zk, yk = k // ny, lax.rem(k, ny)
        hd_copy(k).wait_recv()
        send_h[k] = (own_d[k] + recv_d[k].astype(F32)).astype(BF16)

        @pl.when(zk != z)
        def _():
            h1a_copy(k, z, {"kv_0": zk}).start()

        @pl.when(yk != y)
        def _():
            h1b_copy(k, y, {"kv_1": yk}).start()

    behind = min(6, nkv - 1)
    loop(0, behind, down)

    def down_and_joined(i):
        down(i)
        joined(i - behind)

    loop(behind, nkv, down_and_joined)
    loop(nkv - behind, nkv, joined)

    def h1a_sum(yk):
        acc = send_h[z * ny + yk, 0:rc, :].astype(F32)
        for d in range(1, nz):
            src = lax.rem(z + nz - d, nz)
            h1a_copy(z * ny + yk, src, partner).wait_recv()
            acc = acc + recv_h1a[src, yk].astype(F32)
        return acc

    def h1b_sum(zk):
        acc = send_h[zk * ny + y, rc : 2 * rc, :].astype(F32)
        for d in range(1, ny):
            src = lax.rem(y + ny - d, ny)
            h1b_copy(zk * ny + y, src, partner).wait_recv()
            acc = acc + recv_h1b[src, zk].astype(F32)
        return acc

    def h2a_copy(d, yk, src_y, dev):
        return remote(
            send_h2a.at[yk], recv_h2a.at[src_y], h2_send.at[0, d], h2a_recv.at[src_y], dev
        )

    def h2b_copy(d, zk, src_z, dev):
        return remote(
            send_h2b.at[zk], recv_h2b.at[src_z], h2_send.at[1, d], h2b_recv.at[src_z], dev
        )

    for d in range(1, max(ny, nz)):
        if d < ny:
            yk = lax.rem(y + d, ny)
            send_h2a[yk] = h1a_sum(yk).astype(BF16)
            h2a_copy(d, yk, y, {"kv_1": yk}).start()
        if d < nz:
            zk = lax.rem(z + d, nz)
            send_h2b[zk] = h1b_sum(zk).astype(BF16)
            h2b_copy(d, zk, z, {"kv_0": zk}).start()
    sum_a = h1a_sum(y)
    sum_b = h1b_sum(z)
    for d in range(1, ny):
        src = lax.rem(y + ny - d, ny)
        h2a_copy(d, y, src, partner).wait_recv()
        sum_a = sum_a + recv_h2a[src].astype(F32)
    for d in range(1, nz):
        src = lax.rem(z + nz - d, nz)
        h2b_copy(d, z, src, partner).wait_recv()
        sum_b = sum_b + recv_h2b[src].astype(F32)

    own_sum = jnp.concatenate([sum_a, sum_b], axis=0).T.astype(BF16)
    send_x[...] = own_sum

    def x_copy(d, dest_tp, src_tp, peer):
        return remote(
            send_x.at[block(dest_tp, dt), :],
            recv_x.at[src_tp],
            x_send.at[d],
            x_recv.at[src_tp],
            tp_dev(peer),
        )

    def x_start(d):
        peer = lax.rem(tp + d, ntp)
        x_copy(d, peer, tp, peer).start()

    loop(1, ntp, x_start)
    recv_x[tp] = send_x[block(tp, dt), :]

    def x_wait(d):
        src = lax.rem(tp + ntp - d, ntp)
        x_copy(d, tp, src, src).wait_recv()

    loop(1, ntp, x_wait)
    for cc in range(nc):
        at = slice(cc * rh, (cc + 1) * rh)
        acc = res_t[block(tp, dt), at]
        branch = recv_x[cc].astype(F32)
        for xx in range(1, nx):
            branch = branch + recv_x[xx * nc + cc].astype(F32)
        mixed_ref[:, at] = (acc + branch).astype(BF16)

    def tp_sends(d):
        peer = lax.rem(tp + d, ntp)
        a_copy(d, tp, peer).wait_send()
        x_copy(d, peer, tp, peer).wait_send()

    loop(1, ntp, tp_sends)

    def kv_sends(d):
        peer = lax.rem(kv + d, nkv)
        d_copy(d, kv, peer).wait_send()

    loop(1, nkv, kv_sends)
    e_copy.wait_send()
    for d in range(1, nx):
        ex_copy(d, x, partner).wait_send()
    loop(0, a_base + ny * (nz - 1), lambda i: fa_copy(kv, i, partner).wait_send())
    loop(0, b_base + nz * (ny - 1), lambda i: fb_copy(kv, i, partner).wait_send())

    def h_sends(k):
        zk, yk = k // ny, lax.rem(k, ny)
        fp_copy(k, 0, rows_a).wait_send()
        fp_copy(k, 1, rows_b).wait_send()
        hd_copy(k).wait_send()

        @pl.when(zk != z)
        def _():
            b1a_copy(k, z, {"kv_0": zk}).wait_send()
            h1a_copy(k, z, {"kv_0": zk}).wait_send()

        @pl.when(yk != y)
        def _():
            b1b_copy(k, y, {"kv_1": yk}).wait_send()
            h1b_copy(k, y, {"kv_1": yk}).wait_send()

    loop(0, nkv, h_sends)
    for d in range(1, ny):
        b2a_copy(d, lax.rem(y + d, ny), y, partner).wait_send()
        h2a_copy(d, lax.rem(y + d, ny), y, partner).wait_send()
    for d in range(1, nz):
        b2b_copy(d, lax.rem(z + d, nz), z, partner).wait_send()
        h2b_copy(d, lax.rem(z + d, nz), z, partner).wait_send()


def local(
    sizes,
    tokens,
    mix_gain,
    w_query,
    w_key,
    w_value,
    w_gate,
    w_beta,
    w_decay,
    decay_rate,
    out_gain,
    state,
    w_out,
    mlp_gain,
    w_up,
    w_down,
):
    nz, ny, nx, nc = sizes
    nkv, ntp = nz * ny, nx * nc
    rows, dt = tokens.shape
    dk = dt * ntp
    rb, heads, head, _ = state.shape
    proj = heads * head
    sent = 4 * proj + 128
    cols_a, cols_b = 2 * proj, 2 * proj + 128
    n_heads = w_beta.shape[1]
    ff = w_up.shape[1]
    rh = rows // nc
    rc = rh // 2
    vmem, dma = pltpu.VMEM, pltpu.SemaphoreType.DMA
    scratch = [
        vmem((dk, rows), BF16),
        vmem((4, dk, proj), BF16),
        vmem((128, dk), BF16),
        vmem((n_heads, dk), BF16),
        vmem((n_heads, dk), BF16),
        vmem((1, dk), F32),
        vmem((1, head), F32),
        vmem((1, dk * nkv), F32),
        vmem((1, heads), F32),
        vmem(w_out.shape, BF16),
        vmem(w_up.shape, BF16),
        vmem(w_down.shape, BF16),
        vmem(state.shape, F32),
        vmem((rows, dk), BF16),
        vmem((rows, sent), BF16),
        vmem((nz, ny, rb, cols_a), BF16),
        vmem((ny, nz, rb, cols_b), BF16),
        vmem((ny, rb, cols_a), BF16),
        vmem((nz, rb, cols_b), BF16),
        vmem((ny, rb, cols_a), BF16),
        vmem((nz, rb, cols_b), BF16),
        vmem((rb // 4, heads, head, 128), F32),
        vmem((rb // 4, heads, head, 128), F32),
        vmem((6, heads, rb, head), F32),
        vmem((rows, proj), BF16),
        vmem((rh, dk), BF16),
        vmem((rh, dk), BF16),
        vmem((nx, rh, dk), BF16),
        vmem((nkv, rows, dk), BF16),
        vmem((dk, rows), F32),
        vmem((rows, ff), BF16),
        vmem((rows, ff), F32),
        vmem((rows, 128), F32),
        vmem((nkv, rh, dk), F32),
        vmem((nkv, rh, dk), BF16),
        vmem((nkv, rh, dk), BF16),
        vmem((nkv, rh, dk), BF16),
        vmem((nz, ny, rc, dk), BF16),
        vmem((ny, nz, rc, dk), BF16),
        vmem((ny, rc, dk), BF16),
        vmem((nz, rc, dk), BF16),
        vmem((ny, rc, dk), BF16),
        vmem((nz, rc, dk), BF16),
        vmem((dk, rh), BF16),
        vmem((ntp, dt, rh), BF16),
        dma((15,)),
        dma((ntp,)),
        dma((ntp,)),
        dma((nkv,)),
        dma((nkv,)),
        dma((nz, ny)),
        dma((ny, nz)),
        dma((2, max(ny, nz))),
        dma((ny,)),
        dma((nz,)),
        dma((nkv,)),
        dma((nkv,)),
        dma(()),
        dma(()),
        dma((nx,)),
        dma((nx,)),
        dma((ny - 1 + ny * (nz - 1),)),
        dma((nz - 1 + nz * (ny - 1),)),
        dma((nkv,)),
        dma((nkv,)),
        dma((2, nkv)),
        dma((2, nkv)),
        dma((nkv,)),
        dma((nkv,)),
        dma((nkv,)),
        dma((nkv,)),
        dma((nz, ny)),
        dma((ny, nz)),
        dma((2, max(ny, nz))),
        dma((ny,)),
        dma((nz,)),
        dma((ntp,)),
        dma((ntp,)),
    ]
    in_hbm = pl.BlockSpec(memory_space=pl.ANY)
    in_vmem = pl.BlockSpec(memory_space=pltpu.VMEM)
    mixed_t, new_state = pl.pallas_call(
        functools.partial(layer_kernel, sizes),
        out_shape=(
            pltpu.VMEM((dt, rows), BF16),
            pltpu.VMEM(state.shape, F32),
        ),
        in_specs=[in_hbm] * 15,
        out_specs=(in_vmem, in_vmem),
        scratch_shapes=scratch,
        compiler_params=pltpu.CompilerParams(
            collective_id=0, has_side_effects=True, vmem_limit_bytes=63_500_000
        ),
        name="layer",
    )(
        tokens.T,
        mix_gain[None, :],
        w_query,
        w_key,
        w_value,
        w_gate,
        w_beta.T,
        w_decay.T,
        decay_rate[None, :],
        out_gain[None, :],
        state,
        w_out,
        mlp_gain[None, :],
        w_up,
        w_down,
    )
    return mixed_t.T, new_state


def solution(mesh):
    n = dict(mesh.shape)
    sizes = (n["kv"] // 4, 4, n["tp"] // 2, 2) if n["kv"] >= 8 else (2, n["kv"] // 2, n["tp"] // 2, 2)
    torus = Mesh(mesh.devices.reshape(sizes), KV_TP)
    in_specs = (
        P(None, KV_TP),
        P(KV),
        P(KV, TP),
        P(KV, TP),
        P(KV, TP),
        P(KV, TP),
        P(KV, None),
        P(KV, None),
        P(TP),
        P(),
        P(KV, TP, None, None),
        P(TP, KV),
        P(),
        P(None, KV_TP),
        P(KV_TP, None),
    )
    out_specs = (P(None, KV_TP), P(KV, TP, None, None))
    return jax.shard_map(
        functools.partial(local, sizes),
        mesh=torus,
        in_specs=in_specs,
        out_specs=out_specs,
        check_vma=False,
    )
```

```python
import functools
import math

import jax
import jax.numpy as jnp
from jax import lax
from jax.experimental import pallas as pl
from jax.experimental.pallas import tpu as pltpu
from jax.sharding import Mesh
from jax.sharding import PartitionSpec as P

EPSILON = 1e-06
MESH = pl.DeviceIdType.MESH
KV_TP = ("kv_0", "kv_1", "tp_0", "tp_1")
KV = ("kv_0", "kv_1")
TP = ("tp_0", "tp_1")
F32 = jnp.float32
BF16 = jnp.bfloat16


def silu(v):
    return v / (1.0 + jnp.exp(-v))


def layer_kernel(
    sizes,
    tok_ref,
    mix_gain_ref,
    wq_ref,
    wk_ref,
    wv_ref,
    wg_ref,
    wbeta_ref,
    wdecay_ref,
    rate_ref,
    out_gain_ref,
    state_ref,
    wout_ref,
    mlp_gain_ref,
    wup_ref,
    wdown_ref,
    mixed_ref,
    new_state_ref,
    col_t,
    w_proj,
    w_rates,
    w_beta,
    w_decay,
    mix_gain,
    out_gain,
    mlp_gain,
    rate,
    w_out,
    w_up,
    w_down,
    st,
    col_n,
    send_b,
    recv_b1a,
    recv_b1b,
    send_b2a,
    send_b2b,
    recv_b2a,
    recv_b2b,
    key_t,
    query_t,
    rows_s,
    merged,
    send_e,
    recv_e,
    recv_ex,
    res,
    res_t,
    recv_r,
    hid,
    acc_up,
    total_sq,
    send_h,
    recv_h1a,
    recv_h1b,
    send_h2a,
    send_h2b,
    recv_h2a,
    recv_h2b,
    send_x,
    recv_x,
    local_sem,
    a_send,
    a_recv,
    b1a_send,
    b1b_send,
    b1a_recv,
    b1b_recv,
    b2_send,
    b2a_recv,
    b2b_recv,
    d_send,
    d_recv,
    e_send,
    e_recv,
    ex_send,
    ex_recv,
    fa_send,
    fb_send,
    fa_recv,
    fb_recv,
    r_send,
    r_recv,
    swap_send,
    swap_recv,
    h1a_send,
    h1b_send,
    h1a_recv,
    h1b_recv,
    h2_send,
    h2a_recv,
    h2b_recv,
    x_send,
    x_recv,
):
    nz, ny, nx, nc = sizes
    nkv, ntp = nz * ny, nx * nc
    z, y = lax.axis_index("kv_0"), lax.axis_index("kv_1")
    x, c = lax.axis_index("tp_0"), lax.axis_index("tp_1")
    kv, tp = z * ny + y, x * nc + c
    partner = {"tp_1": nc - 1 - c}

    dt, rows = tok_ref.shape
    ff = wup_ref.shape[1]
    dk = dt * ntp
    width = dk * nkv
    rb, heads, head = st.shape[0], st.shape[1], st.shape[2]
    proj = heads * head
    rh = rows // nc
    rc = rh // 2
    cols_a = 2 * proj
    cols_b = 2 * proj + 128
    other = nc - 1 - c

    def kv_dev(k):
        return {"kv_0": k // ny, "kv_1": lax.rem(k, ny)}

    def tp_dev(t):
        return {"tp_0": t // nc, "tp_1": lax.rem(t, nc)}

    def remote(src, dst, send_sem, recv_sem, dev):
        return pltpu.make_async_remote_copy(
            src_ref=src,
            dst_ref=dst,
            send_sem=send_sem,
            recv_sem=recv_sem,
            device_id=dev,
            device_id_type=MESH,
        )

    def loop(lo, hi, body):
        def wrapped(i, carry):
            body(i)
            return carry

        lax.fori_loop(lo, hi, wrapped, 0)

    def block(i, n):
        return pl.ds(pl.multiple_of(i * n, n), n)

    own_tok = col_t.at[block(tp, dt), :]
    first = (
        (tok_ref, own_tok),
        (wbeta_ref, w_beta),
        (wdecay_ref, w_decay),
        (mix_gain_ref, mix_gain),
        (wq_ref, w_proj.at[0]),
        (wk_ref, w_proj.at[1]),
        (wv_ref, w_proj.at[2]),
        (wg_ref, w_proj.at[3]),
        (rate_ref, rate),
        (out_gain_ref, out_gain),
        (mlp_gain_ref, mlp_gain),
        (state_ref, st),
        (wout_ref, w_out),
        (wup_ref, w_up.at[:, pl.ds(0, ff)]),
        (wdown_ref, w_down.at[pl.ds(0, ff), :]),
    )
    copies = [
        pltpu.make_async_copy(src, dst, local_sem.at[i]) for i, (src, dst) in enumerate(first)
    ]
    for copy in copies:
        copy.start()

    barrier = pltpu.get_barrier_semaphore()

    def greet(dev):
        pl.semaphore_signal(barrier, inc=1, device_id=dev, device_id_type=MESH)

    def greet_tp(d):
        greet(tp_dev(lax.rem(tp + d, ntp)))

    loop(1, ntp, greet_tp)
    for d in range(1, ny):
        greet({"kv_1": lax.rem(y + d, ny)})
    for d in range(1, nz):
        greet({"kv_0": lax.rem(z + d, nz)})

    n_heads = wbeta_ref.shape[0]
    copies[1].wait()
    copies[2].wait()
    w_rates[...] = jnp.zeros_like(w_rates)
    w_rates[0:n_heads, :] = w_beta[...]
    w_rates[32 : 32 + n_heads, :] = w_decay[...]

    copies[0].wait()
    copies[3].wait()
    pl.semaphore_wait(barrier, ntp - 1 + ny - 1 + nz - 1)

    def a_copy(d, src_tp, peer):
        blk = col_t.at[block(src_tp, dt), :]
        return remote(blk, blk, a_send.at[d], a_recv.at[src_tp], tp_dev(peer))

    loop(1, ntp, lambda d: a_copy(d, tp, lax.rem(tp + d, ntp)).start())

    def a_wait(d):
        src = lax.rem(tp + ntp - d, ntp)
        a_copy(d, src, src).wait_recv()

    loop(1, ntp, a_wait)

    cols = col_t[...].astype(F32).T
    col_n[...] = cols.astype(BF16)
    normed = (cols * mix_gain[...]).astype(BF16)
    squares = jnp.sum(cols * cols, axis=1, keepdims=True)

    def project(i):
        copies[4 + i].wait()
        return jnp.dot(normed, w_proj[i], preferred_element_type=F32).astype(BF16)

    def b1a_copy(k, src_z, dev):
        yk = lax.rem(k, ny)
        return remote(
            send_b.at[block(k, rb), pl.ds(0, cols_a)],
            recv_b1a.at[src_z, yk],
            b1a_send.at[k],
            b1a_recv.at[src_z, yk],
            dev,
        )

    def b1b_copy(k, src_y, dev):
        zk = k // ny
        return remote(
            send_b.at[block(k, rb), pl.ds(cols_a, cols_b)],
            recv_b1b.at[src_y, zk],
            b1b_send.at[k],
            b1b_recv.at[src_y, zk],
            dev,
        )

    for i in range(2):
        send_b[:, i * proj : (i + 1) * proj] = project(i)

    def b1a_start(i):
        yk, zk = lax.rem(y + 1 + i // (nz - 1), ny), lax.rem(z + 1 + lax.rem(i, nz - 1), nz)
        b1a_copy(zk * ny + yk, z, {"kv_0": zk}).start()

    loop(0, ny * (nz - 1), b1a_start)

    contract_last = (((1,), (1,)), ((), ()))
    rates_part = lax.dot_general(
        normed, w_rates[...], contract_last, preferred_element_type=F32
    )
    lane = lax.broadcasted_iota(jnp.int32, rates_part.shape, 1)
    rates_part = jnp.where(lane == 63, squares, rates_part)
    high = rates_part.astype(BF16).astype(F32)
    low = pltpu.roll(rates_part - high, 64, 1)
    send_b[:, 4 * proj :] = jnp.where(lane < 64, high, low).astype(BF16)
    for i in range(2, 4):
        send_b[:, i * proj : (i + 1) * proj] = project(i)

    def b1b_start(i):
        zk, yk = lax.rem(z + 1 + i // (ny - 1), nz), lax.rem(y + 1 + lax.rem(i, ny - 1), ny)
        b1b_copy(zk * ny + yk, y, {"kv_1": yk}).start()

    loop(0, nz * (ny - 1), b1b_start)

    def b1a_sum(yk):
        k = z * ny + yk
        acc = send_b[block(k, rb), 0:cols_a].astype(F32)
        for d in range(1, nz):
            src = lax.rem(z + nz - d, nz)
            b1a_copy(k, src, partner).wait_recv()
            acc = acc + recv_b1a[src, yk].astype(F32)
        return acc

    def b1b_sum(zk):
        k = zk * ny + y
        acc = send_b[block(k, rb), cols_a : cols_a + cols_b].astype(F32)
        for d in range(1, ny):
            src = lax.rem(y + ny - d, ny)
            b1b_copy(k, src, partner).wait_recv()
            acc = acc + recv_b1b[src, zk].astype(F32)
        return acc

    def b2a_copy(d, yk, src_y, dev):
        return remote(
            send_b2a.at[yk], recv_b2a.at[src_y], b2_send.at[0, d], b2a_recv.at[src_y], dev
        )

    def b2b_copy(d, zk, src_z, dev):
        return remote(
            send_b2b.at[zk], recv_b2b.at[src_z], b2_send.at[1, d], b2b_recv.at[src_z], dev
        )

    for d in range(1, max(ny, nz)):
        if d < ny:
            yk = lax.rem(y + d, ny)
            send_b2a[yk] = b1a_sum(yk).astype(BF16)
            b2a_copy(d, yk, y, {"kv_1": yk}).start()
        if d < nz:
            zk = lax.rem(z + d, nz)
            send_b2b[zk] = b1b_sum(zk).astype(BF16)
            b2b_copy(d, zk, z, {"kv_0": zk}).start()
    sum_a = b1a_sum(y)
    sum_b = b1b_sum(z)

    for d in range(1, nz):
        src = lax.rem(z + nz - d, nz)
        b2b_copy(d, z, src, partner).wait_recv()
        sum_b = sum_b + recv_b2b[src].astype(F32)
    for d in range(1, ny):
        src = lax.rem(y + ny - d, ny)
        b2a_copy(d, y, src, partner).wait_recv()
        sum_a = sum_a + recv_b2a[src].astype(F32)

    swaps = [
        remote(
            w_up.at[:, pl.ds(0, ff)],
            w_up.at[:, pl.ds(ff, ff)],
            swap_send.at[0],
            swap_recv.at[0],
            partner,
        ),
        remote(
            w_down.at[pl.ds(0, ff), :],
            w_down.at[pl.ds(ff, ff), :],
            swap_send.at[1],
            swap_recv.at[1],
            partner,
        ),
    ]
    for i in range(2):
        copies[13 + i].wait()
        swaps[i].start()

    rates = sum_b[:, 2 * proj :]
    rates = rates + pltpu.roll(rates, 64, 1)
    lane_b = lax.broadcasted_iota(jnp.int32, rates.shape, 1)

    def pick(i):
        return jnp.sum(jnp.where(lane_b == i, rates, 0.0), axis=1, keepdims=True)

    for i in range(8, 12):
        copies[i].wait()
    row_scale = lax.rsqrt(pick(63) / width + EPSILON)
    repeat = 128 // rb
    group = 4
    gates = []
    for h in range(heads):
        at = slice(h * head, (h + 1) * head)
        beta_raw = pick(tp * heads + h) * row_scale
        decay_raw = pick(32 + tp * heads + h) * row_scale
        beta = 1.0 / (1.0 + jnp.exp(-beta_raw))
        softplus = jnp.maximum(decay_raw, 0.0) + jnp.log1p(jnp.exp(-jnp.abs(decay_raw)))
        decay = jnp.exp(-rate[0:1, h : h + 1] * softplus)
        query = silu(sum_a[:, :proj][:, at] * row_scale)
        query = query * lax.rsqrt(jnp.sum(query * query, axis=1, keepdims=True) + EPSILON)
        query = query * head ** (-0.5)
        key = silu(sum_a[:, proj:][:, at] * row_scale)
        key = key * lax.rsqrt(jnp.sum(key * key, axis=1, keepdims=True) + EPSILON)
        key_tr = jnp.concatenate([key] * repeat, axis=0).T
        query_tr = jnp.concatenate([query] * repeat, axis=0).T
        for g in range(rb // group):
            key_t[g, h] = pltpu.roll(key_tr, (128 - g * group) % 128, 1) if g else key_tr
            query_t[g, h] = pltpu.roll(query_tr, (128 - g * group) % 128, 1) if g else query_tr
        shape = (rb, head)
        rows_s[0, h] = jnp.broadcast_to(decay, shape)
        rows_s[1, h] = jnp.broadcast_to(beta, shape)
        rows_s[2, h] = silu(sum_b[:, :proj][:, at] * row_scale)
        rows_s[3, h] = jnp.broadcast_to(
            jnp.sum(key * query, axis=1, keepdims=True), shape
        )
        gates.append(silu(sum_b[:, proj : 2 * proj][:, at] * row_scale))

    def read_group(g):
        for i in range(group):
            b = g * group + i
            for h in range(heads):
                state = st[b, h]
                rows_s[4, h, pl.ds(b, 1), :] = jnp.sum(
                    state * key_t[g, h, :, i : i + 1], axis=0, keepdims=True
                )
                rows_s[5, h, pl.ds(b, 1), :] = jnp.sum(
                    state * query_t[g, h, :, i : i + 1], axis=0, keepdims=True
                )

    loop(0, rb // group, read_group)

    own_rows = block(kv, rb)
    for h in range(heads):
        at = slice(h * head, (h + 1) * head)
        decay = rows_s[0, h]
        change = rows_s[1, h] * (rows_s[2, h] - decay * rows_s[4, h])
        read = decay * rows_s[5, h] + rows_s[3, h] * change
        rows_s[4, h] = change
        scale = lax.rsqrt(jnp.sum(read * read, axis=1, keepdims=True) / head + EPSILON)
        merged[own_rows, at] = (read * scale * out_gain[...] * gates[h]).astype(BF16)

    def d_copy(d, src_kv, peer):
        blk = merged.at[block(src_kv, rb), :]
        return remote(blk, blk, d_send.at[d], d_recv.at[src_kv], kv_dev(peer))

    loop(1, nkv, lambda d: d_copy(d, kv, lax.rem(kv + d, nkv)).start())

    def d_wait(d):
        src = lax.rem(kv + nkv - d, nkv)
        d_copy(d, src, src).wait_recv()

    def write_group(g):
        for i in range(group):
            b = g * group + i
            for h in range(heads):
                new_state_ref[b, h] = (
                    rows_s[0, h, pl.ds(b, 1), :] * st[b, h]
                    + key_t[g, h, :, i : i + 1] * rows_s[4, h, pl.ds(b, 1), :]
                )

    loop(0, rb // group, write_group)
    copies[12].wait()

    def a_b_sends(k):
        zk, yk = k // ny, lax.rem(k, ny)

        @pl.when(zk != z)
        def _():
            b1a_copy(k, z, {"kv_0": zk}).wait_send()

        @pl.when(yk != y)
        def _():
            b1b_copy(k, y, {"kv_1": yk}).wait_send()

    loop(0, nkv, a_b_sends)
    loop(1, ntp, lambda d: a_copy(d, tp, lax.rem(tp + d, ntp)).wait_send())
    for d in range(1, ny):
        b2a_copy(d, lax.rem(y + d, ny), y, partner).wait_send()
    for d in range(1, nz):
        b2b_copy(d, lax.rem(z + d, nz), z, partner).wait_send()
    loop(1, nkv, d_wait)

    half_other = pl.ds(pl.multiple_of(other * rh, rh), rh)
    half_own = pl.ds(pl.multiple_of(c * rh, rh), rh)
    e_copy = remote(send_e, recv_e, e_send, e_recv, partner)
    send_e[...] = jnp.dot(
        merged[half_other, :], w_out[...], preferred_element_type=F32
    ).astype(BF16)
    e_copy.start()
    part = jnp.dot(merged[half_own, :], w_out[...], preferred_element_type=F32)
    e_copy.wait_recv()
    recv_ex[x] = (part + recv_e[...].astype(F32)).astype(BF16)

    def ex_copy(d, src_x, dev):
        blk = recv_ex.at[src_x]
        return remote(blk, blk, ex_send.at[d], ex_recv.at[src_x], dev)

    for d in range(1, nx):
        ex_copy(d, x, {"tp_0": lax.rem(x + d, nx)}).start()
    for d in range(1, nx):
        ex_copy(d, lax.rem(x + nx - d, nx), partner).wait_recv()
    branch = recv_ex[0].astype(F32)
    for i in range(1, nx):
        branch = branch + recv_ex[i].astype(F32)
    res[kv] = (col_n[half_own, :].astype(F32) + branch).astype(BF16)

    rows_a, rows_b = pl.ds(0, rc), pl.ds(rc, rc)

    def fa_copy(k, slot, dev):
        blk = res.at[k, rows_a, :]
        return remote(blk, blk, fa_send.at[slot], fa_recv.at[k], dev)

    def fb_copy(k, slot, dev):
        blk = res.at[k, rows_b, :]
        return remote(blk, blk, fb_send.at[slot], fb_recv.at[k], dev)

    def y_dev(d):
        return {"kv_1": lax.rem(y + d, ny)}

    def z_dev(d):
        return {"kv_0": lax.rem(z + d, nz)}

    for d in range(1, ny):
        fa_copy(kv, d - 1, y_dev(d)).start()
    for d in range(1, nz):
        fb_copy(kv, d - 1, z_dev(d)).start()
    a_base, b_base = ny - 1, nz - 1
    for d in range(1, nz):
        fa_copy(kv, a_base + d - 1, z_dev(d)).start()
    for d in range(1, ny):
        fb_copy(kv, b_base + d - 1, y_dev(d)).start()


    res_t[...] = res[kv].astype(F32).T.astype(BF16)
    r_copy = remote(
        res_t.at[block(x * nc + other, dt), :], recv_r, r_send, r_recv, partner
    )
    r_copy.start()

    def up(j):
        k = lax.rem(z + nz - j // ny, nz) * ny + lax.rem(y + ny - lax.rem(j, ny), ny)
        at = block(k, dk)
        blk = res[k].astype(F32)
        sq = blk * blk
        total = total_sq[...]
        for i in range(dk // 128):
            total = total + sq[:, i * 128 : (i + 1) * 128]
        total_sq[...] = total
        acc_up[...] += jnp.dot(
            (blk * mlp_gain[:, at]).astype(BF16), w_up[at, :], preferred_element_type=F32
        )

    acc_up[...] = jnp.zeros_like(acc_up)
    total_sq[...] = jnp.zeros_like(total_sq)
    for swap in swaps:
        swap.wait_recv()
    up(0)
    loop(1, nkv, lambda d: d_copy(d, kv, lax.rem(kv + d, nkv)).wait_send())
    e_copy.wait_send()
    for d in range(1, nx):
        ex_copy(d, x, partner).wait_send()

    for i in range(1, max(ny, nz)):
        if i < ny:
            k = z * ny + lax.rem(y + ny - i, ny)
            fa_copy(k, 0, partner).wait_recv()
            for d in range(1, nz):
                fa_copy(k, a_base + i * (nz - 1) + d - 1, z_dev(d)).start()
        if i < nz:
            k = lax.rem(z + nz - i, nz) * ny + y
            fb_copy(k, 0, partner).wait_recv()
            for d in range(1, ny):
                fb_copy(k, b_base + i * (ny - 1) + d - 1, y_dev(d)).start()

    n_late = max((nz - 1) * ny, (ny - 1) * nz)

    def late(i):
        zd, yd = 1 + lax.rem(i, nz - 1), i // (nz - 1)
        k = lax.rem(z + nz - zd, nz) * ny + lax.rem(y + ny - yd, ny)
        fa_copy(k, 0, partner).wait_recv()
        yd, zd = 1 + lax.rem(i, ny - 1), i // (ny - 1)
        k = lax.rem(z + nz - zd, nz) * ny + lax.rem(y + ny - yd, ny)
        fb_copy(k, 0, partner).wait_recv()

    lag = 0
    for j in range(1, nkv):
        zd, yd = j // ny, j % ny
        ready = max(yd * (nz - 1) + zd - 1 if zd else 0, zd * (ny - 1) + yd - 1 if yd else 0)
        lag = max(lag, ready - (j - 1))

    loop(0, lag, late)

    def late_and_up(i):
        late(i)
        up(i - lag + 1)

    loop(lag, n_late, late_and_up)

    loop(n_late - lag + 1, nkv, up)

    scale = lax.rsqrt(jnp.sum(total_sq[...], axis=1, keepdims=True) / width + EPSILON)
    relu = jnp.maximum(acc_up[...] * scale, 0.0)
    hid[...] = (relu * relu).astype(BF16)

    part_a, part_b = pl.ds(0, rc), pl.ds(rc, rc)

    def h1a_copy(k, src_z, dev):
        yk = lax.rem(k, ny)
        return remote(
            send_h.at[k, part_a, :],
            recv_h1a.at[src_z, yk],
            h1a_send.at[k],
            h1a_recv.at[src_z, yk],
            dev,
        )

    def h1b_copy(k, src_y, dev):
        zk = k // ny
        return remote(
            send_h.at[k, part_b, :],
            recv_h1b.at[src_y, zk],
            h1b_send.at[k],
            h1b_recv.at[src_y, zk],
            dev,
        )

    def down(i):
        k = lax.rem(kv + 1 + i, nkv)
        zk, yk = k // ny, lax.rem(k, ny)
        out = jnp.dot(hid[...], w_down[:, block(k, dk)], preferred_element_type=F32)
        send_h[k] = out.astype(BF16)

        @pl.when(zk != z)
        def _():
            h1a_copy(k, z, {"kv_0": zk}).start()

        @pl.when(yk != y)
        def _():
            h1b_copy(k, y, {"kv_1": yk}).start()

    loop(0, nkv, down)
    loop(0, a_base + ny * (nz - 1), lambda i: fa_copy(kv, i, partner).wait_send())
    loop(0, b_base + nz * (ny - 1), lambda i: fb_copy(kv, i, partner).wait_send())
    for swap in swaps:
        swap.wait_send()
    r_copy.wait_send()

    def h1a_sum(yk):
        acc = send_h[z * ny + yk, 0:rc, :].astype(F32)
        for d in range(1, nz):
            src = lax.rem(z + nz - d, nz)
            h1a_copy(z * ny + yk, src, partner).wait_recv()
            acc = acc + recv_h1a[src, yk].astype(F32)
        return acc

    def h1b_sum(zk):
        acc = send_h[zk * ny + y, rc : 2 * rc, :].astype(F32)
        for d in range(1, ny):
            src = lax.rem(y + ny - d, ny)
            h1b_copy(zk * ny + y, src, partner).wait_recv()
            acc = acc + recv_h1b[src, zk].astype(F32)
        return acc

    def h2a_copy(d, yk, src_y, dev):
        return remote(
            send_h2a.at[yk], recv_h2a.at[src_y], h2_send.at[0, d], h2a_recv.at[src_y], dev
        )

    def h2b_copy(d, zk, src_z, dev):
        return remote(
            send_h2b.at[zk], recv_h2b.at[src_z], h2_send.at[1, d], h2b_recv.at[src_z], dev
        )

    for d in range(1, max(ny, nz)):
        if d < ny:
            yk = lax.rem(y + d, ny)
            send_h2a[yk] = h1a_sum(yk).astype(BF16)
            h2a_copy(d, yk, y, {"kv_1": yk}).start()
        if d < nz:
            zk = lax.rem(z + d, nz)
            send_h2b[zk] = h1b_sum(zk).astype(BF16)
            h2b_copy(d, zk, z, {"kv_0": zk}).start()
    sum_a = h1a_sum(y)
    sum_b = h1b_sum(z)
    for d in range(1, ny):
        src = lax.rem(y + ny - d, ny)
        h2a_copy(d, y, src, partner).wait_recv()
        sum_a = sum_a + recv_h2a[src].astype(F32)
    for d in range(1, nz):
        src = lax.rem(z + nz - d, nz)
        h2b_copy(d, z, src, partner).wait_recv()
        sum_b = sum_b + recv_h2b[src].astype(F32)

    own_sum = jnp.concatenate([sum_a, sum_b], axis=0).T.astype(BF16)
    send_x[...] = own_sum

    def x_copy(d, dest_tp, src_tp, peer):
        return remote(
            send_x.at[block(dest_tp, dt), :],
            recv_x.at[src_tp],
            x_send.at[d],
            x_recv.at[src_tp],
            tp_dev(peer),
        )

    def x_start(d):
        peer = lax.rem(tp + d, ntp)
        x_copy(d, peer, tp, peer).start()

    loop(1, ntp, x_start)
    recv_x[tp] = send_x[block(tp, dt), :]

    def x_wait(d):
        src = lax.rem(tp + ntp - d, ntp)
        x_copy(d, tp, src, src).wait_recv()

    loop(1, ntp, x_wait)
    r_copy.wait_recv()

    def finish(core, residual):
        total = residual.astype(F32) + recv_x[core].astype(F32)
        for xx in range(1, nx):
            total = total + recv_x[xx * nc + core].astype(F32)
        mixed_ref[:, block(core, rh)] = total.astype(BF16)

    finish(c, res_t[block(tp, dt), :])
    finish(other, recv_r[...])

    def tp_sends(d):
        peer = lax.rem(tp + d, ntp)
        x_copy(d, peer, tp, peer).wait_send()

    loop(1, ntp, tp_sends)

    def h_sends(k):
        zk, yk = k // ny, lax.rem(k, ny)

        @pl.when(zk != z)
        def _():
            h1a_copy(k, z, {"kv_0": zk}).wait_send()

        @pl.when(yk != y)
        def _():
            h1b_copy(k, y, {"kv_1": yk}).wait_send()

    loop(0, nkv, h_sends)
    for d in range(1, ny):
        h2a_copy(d, lax.rem(y + d, ny), y, partner).wait_send()
    for d in range(1, nz):
        h2b_copy(d, lax.rem(z + d, nz), z, partner).wait_send()


def local(
    sizes,
    tokens,
    mix_gain,
    w_query,
    w_key,
    w_value,
    w_gate,
    w_beta,
    w_decay,
    decay_rate,
    out_gain,
    state,
    w_out,
    mlp_gain,
    w_up,
    w_down,
):
    nz, ny, nx, nc = sizes
    nkv, ntp = nz * ny, nx * nc
    rows, dt = tokens.shape
    dk = dt * ntp
    rb, heads, head, _ = state.shape
    proj = heads * head
    sent = 4 * proj + 128
    cols_a, cols_b = 2 * proj, 2 * proj + 128
    n_heads = w_beta.shape[1]
    ff = w_up.shape[1]
    rh = rows // nc
    rc = rh // 2
    vmem, dma = pltpu.VMEM, pltpu.SemaphoreType.DMA
    scratch = [
        vmem((dk, rows), BF16),
        vmem((4, dk, proj), BF16),
        vmem((128, dk), BF16),
        vmem((n_heads, dk), BF16),
        vmem((n_heads, dk), BF16),
        vmem((1, dk), F32),
        vmem((1, head), F32),
        vmem((1, dk * nkv), F32),
        vmem((1, heads), F32),
        vmem(w_out.shape, BF16),
        vmem((w_up.shape[0], 2 * ff), BF16),
        vmem((2 * ff, w_down.shape[1]), BF16),
        vmem(state.shape, F32),
        vmem((rows, dk), BF16),
        vmem((rows, sent), BF16),
        vmem((nz, ny, rb, cols_a), BF16),
        vmem((ny, nz, rb, cols_b), BF16),
        vmem((ny, rb, cols_a), BF16),
        vmem((nz, rb, cols_b), BF16),
        vmem((ny, rb, cols_a), BF16),
        vmem((nz, rb, cols_b), BF16),
        vmem((rb // 4, heads, head, 128), F32),
        vmem((rb // 4, heads, head, 128), F32),
        vmem((6, heads, rb, head), F32),
        vmem((rows, proj), BF16),
        vmem((rh, dk), BF16),
        vmem((rh, dk), BF16),
        vmem((nx, rh, dk), BF16),
        vmem((nkv, rh, dk), BF16),
        vmem((dk, rh), BF16),
        vmem((dt, rh), BF16),
        vmem((rh, 2 * ff), BF16),
        vmem((rh, 2 * ff), F32),
        vmem((rh, 128), F32),
        vmem((nkv, rh, dk), BF16),
        vmem((nz, ny, rc, dk), BF16),
        vmem((ny, nz, rc, dk), BF16),
        vmem((ny, rc, dk), BF16),
        vmem((nz, rc, dk), BF16),
        vmem((ny, rc, dk), BF16),
        vmem((nz, rc, dk), BF16),
        vmem((dk, rh), BF16),
        vmem((ntp, dt, rh), BF16),
        dma((15,)),
        dma((ntp,)),
        dma((ntp,)),
        dma((nkv,)),
        dma((nkv,)),
        dma((nz, ny)),
        dma((ny, nz)),
        dma((2, max(ny, nz))),
        dma((ny,)),
        dma((nz,)),
        dma((nkv,)),
        dma((nkv,)),
        dma(()),
        dma(()),
        dma((nx,)),
        dma((nx,)),
        dma((ny - 1 + ny * (nz - 1),)),
        dma((nz - 1 + nz * (ny - 1),)),
        dma((nkv,)),
        dma((nkv,)),
        dma(()),
        dma(()),
        dma((2,)),
        dma((2,)),
        dma((nkv,)),
        dma((nkv,)),
        dma((nz, ny)),
        dma((ny, nz)),
        dma((2, max(ny, nz))),
        dma((ny,)),
        dma((nz,)),
        dma((ntp,)),
        dma((ntp,)),
    ]
    in_hbm = pl.BlockSpec(memory_space=pl.ANY)
    in_vmem = pl.BlockSpec(memory_space=pltpu.VMEM)
    mixed_t, new_state = pl.pallas_call(
        functools.partial(layer_kernel, sizes),
        out_shape=(
            pltpu.VMEM((dt, rows), BF16),
            pltpu.VMEM(state.shape, F32),
        ),
        in_specs=[in_hbm] * 15,
        out_specs=(in_vmem, in_vmem),
        scratch_shapes=scratch,
        compiler_params=pltpu.CompilerParams(
            collective_id=0, has_side_effects=True, vmem_limit_bytes=63_500_000
        ),
        name="layer",
    )(
        tokens.T,
        mix_gain[None, :],
        w_query,
        w_key,
        w_value,
        w_gate,
        w_beta.T,
        w_decay.T,
        decay_rate[None, :],
        out_gain[None, :],
        state,
        w_out,
        mlp_gain[None, :],
        w_up,
        w_down,
    )
    return mixed_t.T, new_state


def solution(mesh):
    n = dict(mesh.shape)
    sizes = (n["kv"] // 4, 4, n["tp"] // 2, 2) if n["kv"] >= 8 else (2, n["kv"] // 2, n["tp"] // 2, 2)
    torus = Mesh(mesh.devices.reshape(sizes), KV_TP)
    in_specs = (
        P(None, KV_TP),
        P(KV),
        P(KV, TP),
        P(KV, TP),
        P(KV, TP),
        P(KV, TP),
        P(KV, None),
        P(KV, None),
        P(TP),
        P(),
        P(KV, TP, None, None),
        P(TP, KV),
        P(),
        P(None, KV_TP),
        P(KV_TP, None),
    )
    out_specs = (P(None, KV_TP), P(KV, TP, None, None))
    return jax.shard_map(
        functools.partial(local, sizes),
        mesh=torus,
        in_specs=in_specs,
        out_specs=out_specs,
        check_vma=False,
    )
```

```python
import functools

import jax
import jax.numpy as jnp
from jax import lax
from jax.experimental import pallas as pl
from jax.experimental.pallas import tpu as pltpu
from jax.sharding import Mesh
from jax.sharding import PartitionSpec as P

EPSILON = 1e-06
MESH = pl.DeviceIdType.MESH
KV_TP = ("kv_0", "kv_1", "tp_0", "tp_1")
KV = ("kv_0", "kv_1")
TP = ("tp_0", "tp_1")
F32 = jnp.float32
BF16 = jnp.bfloat16


def silu(v):
    return v / (1.0 + jnp.exp(-v))


def layer_kernel(
    sizes,
    tok_ref,
    mix_gain_ref,
    wq_ref,
    wk_ref,
    wv_ref,
    wg_ref,
    wbeta_ref,
    wdecay_ref,
    rate_ref,
    out_gain_ref,
    state_ref,
    wout_ref,
    mlp_gain_ref,
    wup_ref,
    wdown_ref,
    mixed_ref,
    new_state_ref,
    col_t,
    w_proj,
    w_rates,
    w_beta,
    w_decay,
    mix_gain,
    out_gain,
    mlp_gain,
    rate,
    w_out,
    w_up,
    w_down,
    st,
    col_n,
    send_b,
    recv_b1a,
    recv_b1b,
    send_b2a,
    send_b2b,
    recv_b2a,
    recv_b2b,
    key_t,
    query_t,
    rows_s,
    merged,
    send_e,
    recv_e,
    recv_ex,
    res,
    res_t,
    recv_r,
    hid,
    acc_up,
    total_sq,
    send_h,
    recv_h1a,
    recv_h1b,
    send_h2a,
    send_h2b,
    recv_h2a,
    recv_h2b,
    send_x,
    recv_x,
    local_sem,
    a_send,
    a_recv,
    b1a_send,
    b1b_send,
    b1a_recv,
    b1b_recv,
    b2_send,
    b2_recv,
    d_send,
    d_recv,
    e_send,
    e_recv,
    ex_send,
    ex_recv,
    fa_send,
    fb_send,
    fa_recv,
    fb_recv,
    r_send,
    r_recv,
    swap_send,
    swap_recv,
    h1a_send,
    h1b_send,
    h1a_recv,
    h1b_recv,
    h2_send,
    h2_recv,
    x_send,
    x_recv,
):
    nz, ny, nx, nc = sizes
    nkv, ntp = nz * ny, nx * nc
    z, y = lax.axis_index("kv_0"), lax.axis_index("kv_1")
    x, c = lax.axis_index("tp_0"), lax.axis_index("tp_1")
    kv, tp = z * ny + y, x * nc + c
    partner = {"tp_1": nc - 1 - c}

    dt, rows = tok_ref.shape
    ff = wup_ref.shape[1]
    dk = dt * ntp
    width = dk * nkv
    rb, heads, head = st.shape[0], st.shape[1], st.shape[2]
    proj = heads * head
    rh = rows // nc
    rc = rh // 2
    cols_a = 2 * proj
    cols_b = 2 * proj + 128
    other = nc - 1 - c

    def kv_dev(k):
        return {"kv_0": k // ny, "kv_1": lax.rem(k, ny)}

    def tp_dev(t):
        return {"tp_0": t // nc, "tp_1": lax.rem(t, nc)}

    def remote(src, dst, send_sem, recv_sem, dev):
        return pltpu.make_async_remote_copy(
            src_ref=src,
            dst_ref=dst,
            send_sem=send_sem,
            recv_sem=recv_sem,
            device_id=dev,
            device_id_type=MESH,
        )

    def all_received(ref, send_sem, recv_sem):
        remote(ref, ref, send_sem, recv_sem, partner).wait_recv()

    def all_sent(ref, send_sem, recv_sem):
        remote(ref, ref, send_sem, recv_sem, partner).wait_send()

    def loop(lo, hi, body):
        def wrapped(i, carry):
            body(i)
            return carry

        lax.fori_loop(lo, hi, wrapped, 0)

    def ring(n):
        return sorted(range(1, n), key=lambda d: (-min(d, n - d), d))

    def block(i, n):
        return pl.ds(pl.multiple_of(i * n, n), n)

    own_tok = col_t.at[block(tp, dt), :]
    first = (
        (tok_ref, own_tok),
        (wbeta_ref, w_beta),
        (wdecay_ref, w_decay),
        (mix_gain_ref, mix_gain),
        (rate_ref, rate),
        (out_gain_ref, out_gain),
        (mlp_gain_ref, mlp_gain),
        (state_ref, st),
        (wout_ref, w_out),
        (wup_ref, w_up.at[:, pl.ds(0, ff)]),
        (wdown_ref, w_down.at[pl.ds(0, ff), :]),
    )
    copies = [
        pltpu.make_async_copy(src, dst, local_sem.at[i]) for i, (src, dst) in enumerate(first)
    ]
    for copy in copies[:4]:
        copy.start()
    for i, w in enumerate((wq_ref, wk_ref, wv_ref, wg_ref)):
        pltpu.make_async_copy(w, w_proj.at[i], local_sem.at[11]).start()
    for copy in copies[4:]:
        copy.start()

    barrier = pltpu.get_barrier_semaphore()

    def greet(dev):
        pl.semaphore_signal(barrier, inc=1, device_id=dev, device_id_type=MESH)

    def greet_tp(d):
        greet(tp_dev(lax.rem(tp + d, ntp)))

    loop(1, ntp, greet_tp)
    for d in range(1, ny):
        greet({"kv_1": lax.rem(y + d, ny)})
    for d in range(1, nz):
        greet({"kv_0": lax.rem(z + d, nz)})

    n_heads = wbeta_ref.shape[0]
    copies[1].wait()
    copies[2].wait()
    w_rates[...] = jnp.zeros_like(w_rates)
    w_rates[0:n_heads, :] = w_beta[...]
    w_rates[32 : 32 + n_heads, :] = w_decay[...]

    copies[0].wait()
    copies[3].wait()
    pl.semaphore_wait(barrier, ntp - 1 + ny - 1 + nz - 1)

    def tp_peers():
        near = [(0, 1)] if nc == 2 else []
        return [(dx, dc) for dx in ring(nx) for dc in range(nc)] + near

    def tp_peer(dx, dc):
        return lax.rem(x + dx, nx) * nc + lax.rem(c + dc, nc)

    for dx, dc in tp_peers():
        remote(own_tok, own_tok, a_send, a_recv, tp_dev(tp_peer(dx, dc))).start()

    a_all = col_t.at[pl.ds(0, (ntp - 1) * dt), :]
    all_received(a_all, a_send, a_recv)

    cols = col_t[...].astype(F32).T
    col_n[...] = cols.astype(BF16)
    normed = (cols * mix_gain[...]).astype(BF16)
    squares = jnp.sum(cols * cols, axis=1, keepdims=True)

    pltpu.make_async_copy(w_proj, w_proj, local_sem.at[11]).wait()

    def project(i):
        return jnp.dot(normed, w_proj[i], preferred_element_type=F32).astype(BF16)

    def b1a_copy(dz, yk):
        zk = lax.rem(z + dz, nz)
        return remote(
            send_b.at[block(zk * ny + yk, rb), pl.ds(0, cols_a)],
            recv_b1a.at[yk, dz - 1],
            b1a_send,
            b1a_recv.at[yk],
            {"kv_0": zk},
        )

    def b1b_copy(dy, zk):
        yk = lax.rem(y + dy, ny)
        return remote(
            send_b.at[block(zk * ny + yk, rb), pl.ds(cols_a, cols_b)],
            recv_b1b.at[zk, dy - 1],
            b1b_send,
            b1b_recv.at[zk],
            {"kv_1": yk},
        )

    for i in range(2):
        send_b[:, i * proj : (i + 1) * proj] = project(i)

    for dy in [*ring(ny), 0]:
        for dz in ring(nz):
            b1a_copy(dz, lax.rem(y + dy, ny)).start()

    contract_last = (((1,), (1,)), ((), ()))
    rates_part = lax.dot_general(
        normed, w_rates[...], contract_last, preferred_element_type=F32
    )
    lane = lax.broadcasted_iota(jnp.int32, rates_part.shape, 1)
    rates_part = jnp.where(lane == 63, squares, rates_part)
    high = rates_part.astype(BF16).astype(F32)
    low = pltpu.roll(rates_part - high, 64, 1)
    send_b[:, 4 * proj :] = jnp.where(lane < 64, high, low).astype(BF16)
    for i in range(2, 4):
        send_b[:, i * proj : (i + 1) * proj] = project(i)

    for dz in [*ring(nz), 0]:
        for dy in ring(ny):
            b1b_copy(dy, lax.rem(z + dz, nz)).start()

    def b1a_sum(yk):
        acc = send_b[block(z * ny + yk, rb), 0:cols_a].astype(F32)
        all_received(recv_b1a.at[yk], b1a_send, b1a_recv.at[yk])
        for i in range(nz - 1):
            acc = acc + recv_b1a[yk, i].astype(F32)
        return acc

    def b1b_sum(zk):
        acc = send_b[block(zk * ny + y, rb), cols_a : cols_a + cols_b].astype(F32)
        all_received(recv_b1b.at[zk], b1b_send, b1b_recv.at[zk])
        for i in range(ny - 1):
            acc = acc + recv_b1b[zk, i].astype(F32)
        return acc

    def b2a_copy(d):
        blk = send_b2a.at[d - 1]
        dev = {"kv_1": lax.rem(y + d, ny)}
        return remote(blk, recv_b2a.at[d - 1], b2_send.at[0], b2_recv.at[0], dev)

    def b2b_copy(d):
        blk = send_b2b.at[d - 1]
        dev = {"kv_0": lax.rem(z + d, nz)}
        return remote(blk, recv_b2b.at[d - 1], b2_send.at[1], b2_recv.at[1], dev)

    for i in range(max(ny, nz) - 1):
        if i < ny - 1:
            d = ring(ny)[i]
            send_b2a[d - 1] = b1a_sum(lax.rem(y + d, ny)).astype(BF16)
            b2a_copy(d).start()
        if i < nz - 1:
            d = ring(nz)[i]
            send_b2b[d - 1] = b1b_sum(lax.rem(z + d, nz)).astype(BF16)
            b2b_copy(d).start()
    sum_a = b1a_sum(y)
    sum_b = b1b_sum(z)

    all_received(recv_b2b, b2_send.at[1], b2_recv.at[1])
    for i in range(nz - 1):
        sum_b = sum_b + recv_b2b[i].astype(F32)
    all_received(recv_b2a, b2_send.at[0], b2_recv.at[0])
    for i in range(ny - 1):
        sum_a = sum_a + recv_b2a[i].astype(F32)

    swaps = [
        remote(
            w_up.at[:, pl.ds(0, ff)],
            w_up.at[:, pl.ds(ff, ff)],
            swap_send.at[0],
            swap_recv.at[0],
            partner,
        ),
        remote(
            w_down.at[pl.ds(0, ff), :],
            w_down.at[pl.ds(ff, ff), :],
            swap_send.at[1],
            swap_recv.at[1],
            partner,
        ),
    ]
    for i in range(2):
        copies[9 + i].wait()
        swaps[i].start()

    rates = sum_b[:, 2 * proj :]
    rates = rates + pltpu.roll(rates, 64, 1)
    lane_b = lax.broadcasted_iota(jnp.int32, rates.shape, 1)

    def pick(i):
        return jnp.sum(jnp.where(lane_b == i, rates, 0.0), axis=1, keepdims=True)

    for i in range(4, 8):
        copies[i].wait()
    row_scale = lax.rsqrt(pick(63) / width + EPSILON)
    repeat = 128 // rb
    group = 4
    gates = []
    for h in range(heads):
        at = slice(h * head, (h + 1) * head)
        beta_raw = pick(tp * heads + h) * row_scale
        decay_raw = pick(32 + tp * heads + h) * row_scale
        beta = 1.0 / (1.0 + jnp.exp(-beta_raw))
        softplus = jnp.maximum(decay_raw, 0.0) + jnp.log1p(jnp.exp(-jnp.abs(decay_raw)))
        decay = jnp.exp(-rate[0:1, h : h + 1] * softplus)
        query = silu(sum_a[:, :proj][:, at] * row_scale)
        query = query * lax.rsqrt(jnp.sum(query * query, axis=1, keepdims=True) + EPSILON)
        query = query * head ** (-0.5)
        key = silu(sum_a[:, proj:][:, at] * row_scale)
        key = key * lax.rsqrt(jnp.sum(key * key, axis=1, keepdims=True) + EPSILON)
        key_tr = jnp.concatenate([key] * repeat, axis=0).T
        query_tr = jnp.concatenate([query] * repeat, axis=0).T
        for g in range(rb // group):
            key_t[g, h] = pltpu.roll(key_tr, (128 - g * group) % 128, 1) if g else key_tr
            query_t[g, h] = pltpu.roll(query_tr, (128 - g * group) % 128, 1) if g else query_tr
        shape = (rb, head)
        rows_s[0, h] = jnp.broadcast_to(decay, shape)
        rows_s[1, h] = jnp.broadcast_to(beta, shape)
        rows_s[2, h] = silu(sum_b[:, :proj][:, at] * row_scale)
        rows_s[3, h] = jnp.broadcast_to(
            jnp.sum(key * query, axis=1, keepdims=True), shape
        )
        gates.append(silu(sum_b[:, proj : 2 * proj][:, at] * row_scale))

    def read_group(g):
        for i in range(group):
            b = g * group + i
            for h in range(heads):
                state = st[b, h]
                rows_s[4, h, pl.ds(b, 1), :] = jnp.sum(
                    state * key_t[g, h, :, i : i + 1], axis=0, keepdims=True
                )
                rows_s[5, h, pl.ds(b, 1), :] = jnp.sum(
                    state * query_t[g, h, :, i : i + 1], axis=0, keepdims=True
                )

    loop(0, rb // group, read_group)

    own_rows = block(kv, rb)
    for h in range(heads):
        at = slice(h * head, (h + 1) * head)
        decay = rows_s[0, h]
        change = rows_s[1, h] * (rows_s[2, h] - decay * rows_s[4, h])
        read = decay * rows_s[5, h] + rows_s[3, h] * change
        rows_s[4, h] = change
        scale = lax.rsqrt(jnp.sum(read * read, axis=1, keepdims=True) / head + EPSILON)
        merged[own_rows, at] = (read * scale * out_gain[...] * gates[h]).astype(BF16)

    d_own = merged.at[own_rows, :]
    d_all = merged.at[pl.ds(0, (nkv - 1) * rb), :]

    def hops(d):
        dz, dy = d // ny, d % ny
        return min(dz, nz - dz) + min(dy, ny - dy)

    def kv_peer(d):
        return lax.rem(z + d // ny, nz) * ny + lax.rem(y + d % ny, ny)

    for d in sorted(range(1, nkv), key=lambda d: -hops(d)):
        remote(d_own, d_own, d_send, d_recv, kv_dev(kv_peer(d))).start()

    def write_group(g):
        for i in range(group):
            b = g * group + i
            for h in range(heads):
                st[b, h] = (
                    rows_s[0, h, pl.ds(b, 1), :] * st[b, h]
                    + key_t[g, h, :, i : i + 1] * rows_s[4, h, pl.ds(b, 1), :]
                )

    loop(0, rb // group, write_group)
    state_out = pltpu.make_async_copy(st, new_state_ref, local_sem.at[12])
    state_out.start()
    copies[8].wait()

    all_sent(a_all, a_send, a_recv)
    all_sent(recv_b1a, b1a_send, b1a_recv.at[0])
    all_sent(recv_b1b, b1b_send, b1b_recv.at[0])
    all_sent(recv_b2a, b2_send.at[0], b2_recv.at[0])
    all_sent(recv_b2b, b2_send.at[1], b2_recv.at[1])
    all_received(d_all, d_send, d_recv)

    half_other = pl.ds(pl.multiple_of(other * rh, rh), rh)
    half_own = pl.ds(pl.multiple_of(c * rh, rh), rh)
    e_copy = remote(send_e, recv_e, e_send, e_recv, partner)
    send_e[...] = jnp.dot(
        merged[half_other, :], w_out[...], preferred_element_type=F32
    ).astype(BF16)
    e_copy.start()
    part = jnp.dot(merged[half_own, :], w_out[...], preferred_element_type=F32)
    e_copy.wait_recv()
    recv_ex[x] = (part + recv_e[...].astype(F32)).astype(BF16)

    def ex_copy(half, dev):
        blk = recv_ex.at[x, pl.ds(half * rc, rc), :]
        return remote(blk, blk, ex_send.at[half], ex_recv.at[half], dev)

    def ex_all(half):
        return recv_ex.at[pl.ds(0, nx - 1), pl.ds(half * rc, rc), :]

    for half in range(2):
        for d in ring(nx):
            ex_copy(half, {"tp_0": lax.rem(x + d, nx)}).start()

    def residual(half):
        all_received(ex_all(half), ex_send.at[half], ex_recv.at[half])
        at = slice(half * rc, (half + 1) * rc)
        branch = recv_ex[0, at].astype(F32)
        for i in range(1, nx):
            branch = branch + recv_ex[i, at].astype(F32)
        tok = col_n[pl.ds(pl.multiple_of(c * rh + half * rc, rc), rc), :]
        res[kv, at] = (tok.astype(F32) + branch).astype(BF16)

    rows_a, rows_b = pl.ds(0, rc), pl.ds(rc, rc)

    def fa_copy(k, dev):
        blk = res.at[k, rows_a, :]
        return remote(blk, blk, fa_send, fa_recv.at[k], dev)

    def fb_copy(k, dev):
        blk = res.at[k, rows_b, :]
        return remote(blk, blk, fb_send, fb_recv.at[k], dev)

    def y_dev(d):
        return {"kv_1": lax.rem(y + d, ny)}

    def z_dev(d):
        return {"kv_0": lax.rem(z + d, nz)}

    residual(0)
    for d in ring(ny):
        fa_copy(kv, y_dev(d)).start()
    for d in ring(nz):
        fa_copy(kv, z_dev(d)).start()
    residual(1)
    for d in ring(nz):
        fb_copy(kv, z_dev(d)).start()
    for d in ring(ny):
        fb_copy(kv, y_dev(d)).start()

    res_t[...] = res[kv].astype(F32).T.astype(BF16)
    r_copy = remote(
        res_t.at[block(x * nc + other, dt), :], recv_r, r_send, r_recv, partner
    )
    r_copy.start()

    def up(*blocks):
        total, acc = total_sq[...], acc_up[...]
        for j in blocks:
            k = lax.rem(z + nz - j // ny, nz) * ny + lax.rem(y + ny - lax.rem(j, ny), ny)
            at = block(k, dk)
            blk = res[k].astype(F32)
            sq = blk * blk
            for i in range(dk // 128):
                total = total + sq[:, i * 128 : (i + 1) * 128]
            acc = acc + jnp.dot(
                (blk * mlp_gain[:, at]).astype(BF16), w_up[at, :], preferred_element_type=F32
            )
        total_sq[...], acc_up[...] = total, acc

    acc_up[...] = jnp.zeros_like(acc_up)
    total_sq[...] = jnp.zeros_like(total_sq)
    for swap in swaps:
        swap.wait_recv()
    up(0)
    all_sent(d_all, d_send, d_recv)
    e_copy.wait_send()
    for half in range(2):
        all_sent(ex_all(half), ex_send.at[half], ex_recv.at[half])

    for i in range(1, max(ny, nz)):
        if i < ny:
            k = z * ny + lax.rem(y + ny - i, ny)
            fa_copy(k, partner).wait_recv()
            for d in ring(nz):
                fa_copy(k, z_dev(d)).start()
        if i < nz:
            k = lax.rem(z + nz - i, nz) * ny + y
            fb_copy(k, partner).wait_recv()
            for d in ring(ny):
                fb_copy(k, y_dev(d)).start()

    n_late = max((nz - 1) * ny, (ny - 1) * nz)

    def late(i):
        zd, yd = 1 + lax.rem(i, nz - 1), i // (nz - 1)
        k = lax.rem(z + nz - zd, nz) * ny + lax.rem(y + ny - yd, ny)
        fa_copy(k, partner).wait_recv()
        yd, zd = 1 + lax.rem(i, ny - 1), i // (ny - 1)
        k = lax.rem(z + nz - zd, nz) * ny + lax.rem(y + ny - yd, ny)
        fb_copy(k, partner).wait_recv()

    lag = 0
    for j in range(1, nkv):
        zd, yd = j // ny, j % ny
        ready = max(yd * (nz - 1) + zd - 1 if zd else 0, zd * (ny - 1) + yd - 1 if yd else 0)
        lag = max(lag, ready - (j - 1))

    loop(0, lag, late)

    def late_and_up(i):
        late(i)
        up(i - lag + 1)

    loop(lag, n_late, late_and_up)

    up(*range(n_late - lag + 1, nkv))

    scale = lax.rsqrt(jnp.sum(total_sq[...], axis=1, keepdims=True) / width + EPSILON)
    relu = jnp.maximum(acc_up[...] * scale, 0.0)
    hid[...] = (relu * relu).astype(BF16)

    part_a, part_b = pl.ds(0, rc), pl.ds(rc, rc)

    def h1a_copy(dz, k):
        return remote(
            send_h.at[k, part_a, :],
            recv_h1a.at[lax.rem(k, ny), dz - 1],
            h1a_send,
            h1a_recv.at[lax.rem(k, ny)],
            {"kv_0": k // ny},
        )

    def h1b_copy(dy, k):
        return remote(
            send_h.at[k, part_b, :],
            recv_h1b.at[k // ny, dy - 1],
            h1b_send,
            h1b_recv.at[k // ny],
            {"kv_1": lax.rem(k, ny)},
        )

    def down(dz, dy):
        zk, yk = lax.rem(z + dz, nz), lax.rem(y + dy, ny)
        k = zk * ny + yk
        out = jnp.dot(hid[...], w_down[:, block(k, dk)], preferred_element_type=F32)
        send_h[k] = out.astype(BF16)
        if dz:
            h1a_copy(dz, k).start()
        if dy:
            h1b_copy(dy, k).start()

    z_order, y_order = [*ring(nz), 0], [*ring(ny), 0]
    for s in range(max(nz, ny)):
        shell = [(i, s) for i in range(s, nz)] + [(s, i) for i in range(s + 1, ny)]
        for i, j in shell:
            if i < nz and j < ny:
                down(z_order[i], y_order[j])
    all_sent(res.at[pl.ds(0, nkv - 1), rows_a, :], fa_send, fa_recv.at[0])
    all_sent(res.at[pl.ds(0, nkv - 1), rows_b, :], fb_send, fb_recv.at[0])
    for swap in swaps:
        swap.wait_send()
    r_copy.wait_send()

    def h1a_sum(yk):
        acc = send_h[z * ny + yk, 0:rc, :].astype(F32)
        all_received(recv_h1a.at[yk], h1a_send, h1a_recv.at[yk])
        for i in range(nz - 1):
            acc = acc + recv_h1a[yk, i].astype(F32)
        return acc

    def h1b_sum(zk):
        acc = send_h[zk * ny + y, rc : 2 * rc, :].astype(F32)
        all_received(recv_h1b.at[zk], h1b_send, h1b_recv.at[zk])
        for i in range(ny - 1):
            acc = acc + recv_h1b[zk, i].astype(F32)
        return acc

    def h2a_copy(d):
        blk = send_h2a.at[d - 1]
        dev = {"kv_1": lax.rem(y + d, ny)}
        return remote(blk, recv_h2a.at[d - 1], h2_send.at[0], h2_recv.at[0], dev)

    def h2b_copy(d):
        blk = send_h2b.at[d - 1]
        dev = {"kv_0": lax.rem(z + d, nz)}
        return remote(blk, recv_h2b.at[d - 1], h2_send.at[1], h2_recv.at[1], dev)

    for i in range(max(ny, nz) - 1):
        if i < ny - 1:
            d = ring(ny)[i]
            send_h2a[d - 1] = h1a_sum(lax.rem(y + d, ny)).astype(BF16)
            h2a_copy(d).start()
        if i < nz - 1:
            d = ring(nz)[i]
            send_h2b[d - 1] = h1b_sum(lax.rem(z + d, nz)).astype(BF16)
            h2b_copy(d).start()
    sum_a = h1a_sum(y)
    sum_b = h1b_sum(z)
    all_received(recv_h2a, h2_send.at[0], h2_recv.at[0])
    for i in range(ny - 1):
        sum_a = sum_a + recv_h2a[i].astype(F32)
    all_received(recv_h2b, h2_send.at[1], h2_recv.at[1])
    for i in range(nz - 1):
        sum_b = sum_b + recv_h2b[i].astype(F32)

    own_sum = jnp.concatenate([sum_a, sum_b], axis=0).T.astype(BF16)
    send_x[...] = own_sum

    def x_copy(peer):
        blk = send_x.at[block(peer, dt), :]
        return remote(blk, recv_x.at[tp], x_send, x_recv, tp_dev(peer))

    x_all = recv_x.at[pl.ds(0, ntp - 1)]
    for dx, dc in tp_peers():
        x_copy(tp_peer(dx, dc)).start()
    recv_x[tp] = send_x[block(tp, dt), :]

    all_received(x_all, x_send, x_recv)
    r_copy.wait_recv()

    def finish(core, residual):
        total = residual.astype(F32) + recv_x[core].astype(F32)
        for xx in range(1, nx):
            total = total + recv_x[xx * nc + core].astype(F32)
        mixed_ref[:, block(core, rh)] = total.astype(BF16)

    finish(c, res_t[block(tp, dt), :])
    finish(other, recv_r[...])

    all_sent(x_all, x_send, x_recv)
    all_sent(recv_h1a, h1a_send, h1a_recv.at[0])
    all_sent(recv_h1b, h1b_send, h1b_recv.at[0])
    all_sent(recv_h2a, h2_send.at[0], h2_recv.at[0])
    all_sent(recv_h2b, h2_send.at[1], h2_recv.at[1])
    state_out.wait()


def local(
    sizes,
    tokens,
    mix_gain,
    w_query,
    w_key,
    w_value,
    w_gate,
    w_beta,
    w_decay,
    decay_rate,
    out_gain,
    state,
    w_out,
    mlp_gain,
    w_up,
    w_down,
):
    nz, ny, nx, nc = sizes
    nkv, ntp = nz * ny, nx * nc
    rows, dt = tokens.shape
    dk = dt * ntp
    rb, heads, head, _ = state.shape
    proj = heads * head
    sent = 4 * proj + 128
    cols_a, cols_b = 2 * proj, 2 * proj + 128
    n_heads = w_beta.shape[1]
    ff = w_up.shape[1]
    rh = rows // nc
    rc = rh // 2
    vmem, dma = pltpu.VMEM, pltpu.SemaphoreType.DMA
    scratch = [
        vmem((dk, rows), BF16),
        vmem((4, dk, proj), BF16),
        vmem((128, dk), BF16),
        vmem((n_heads, dk), BF16),
        vmem((n_heads, dk), BF16),
        vmem((1, dk), F32),
        vmem((1, head), F32),
        vmem((1, dk * nkv), F32),
        vmem((1, heads), F32),
        vmem(w_out.shape, BF16),
        vmem((w_up.shape[0], 2 * ff), BF16),
        vmem((2 * ff, w_down.shape[1]), BF16),
        vmem(state.shape, F32),
        vmem((rows, dk), BF16),
        vmem((rows, sent), BF16),
        vmem((ny, nz - 1, rb, cols_a), BF16),
        vmem((nz, ny - 1, rb, cols_b), BF16),
        vmem((ny - 1, rb, cols_a), BF16),
        vmem((nz - 1, rb, cols_b), BF16),
        vmem((ny - 1, rb, cols_a), BF16),
        vmem((nz - 1, rb, cols_b), BF16),
        vmem((rb // 4, heads, head, 128), F32),
        vmem((rb // 4, heads, head, 128), F32),
        vmem((6, heads, rb, head), F32),
        vmem((rows, proj), BF16),
        vmem((rh, dk), BF16),
        vmem((rh, dk), BF16),
        vmem((nx, rh, dk), BF16),
        vmem((nkv, rh, dk), BF16),
        vmem((dk, rh), BF16),
        vmem((dt, rh), BF16),
        vmem((rh, 2 * ff), BF16),
        vmem((rh, 2 * ff), F32),
        vmem((rh, 128), F32),
        vmem((nkv, rh, dk), BF16),
        vmem((ny, nz - 1, rc, dk), BF16),
        vmem((nz, ny - 1, rc, dk), BF16),
        vmem((ny - 1, rc, dk), BF16),
        vmem((nz - 1, rc, dk), BF16),
        vmem((ny - 1, rc, dk), BF16),
        vmem((nz - 1, rc, dk), BF16),
        vmem((dk, rh), BF16),
        vmem((ntp, dt, rh), BF16),
        dma((13,)),
        dma(()),
        dma(()),
        dma(()),
        dma(()),
        dma((ny,)),
        dma((nz,)),
        dma((2,)),
        dma((2,)),
        dma(()),
        dma(()),
        dma(()),
        dma(()),
        dma((2,)),
        dma((2,)),
        dma(()),
        dma(()),
        dma((nkv,)),
        dma((nkv,)),
        dma(()),
        dma(()),
        dma((2,)),
        dma((2,)),
        dma(()),
        dma(()),
        dma((ny,)),
        dma((nz,)),
        dma((2,)),
        dma((2,)),
        dma(()),
        dma(()),
    ]
    in_hbm = pl.BlockSpec(memory_space=pl.ANY)
    in_vmem = pl.BlockSpec(memory_space=pltpu.VMEM)
    mixed_t, new_state = pl.pallas_call(
        functools.partial(layer_kernel, sizes),
        out_shape=(
            pltpu.VMEM((dt, rows), BF16),
            pltpu.VMEM(state.shape, F32),
        ),
        in_specs=[in_hbm] * 15,
        out_specs=(in_vmem, in_hbm),
        scratch_shapes=scratch,
        compiler_params=pltpu.CompilerParams(
            collective_id=0, has_side_effects=True, vmem_limit_bytes=63_500_000
        ),
        name="layer",
    )(
        tokens.T,
        mix_gain[None, :],
        w_query,
        w_key,
        w_value,
        w_gate,
        w_beta.T,
        w_decay.T,
        decay_rate[None, :],
        out_gain[None, :],
        state,
        w_out,
        mlp_gain[None, :],
        w_up,
        w_down,
    )
    return mixed_t.T, new_state


def solution(mesh):
    n = dict(mesh.shape)
    sizes = (n["kv"] // 4, 4, n["tp"] // 2, 2) if n["kv"] >= 8 else (2, n["kv"] // 2, n["tp"] // 2, 2)
    torus = Mesh(mesh.devices.reshape(sizes), KV_TP)
    in_specs = (
        P(None, KV_TP),
        P(KV),
        P(KV, TP),
        P(KV, TP),
        P(KV, TP),
        P(KV, TP),
        P(KV, None),
        P(KV, None),
        P(TP),
        P(),
        P(KV, TP, None, None),
        P(TP, KV),
        P(),
        P(None, KV_TP),
        P(KV_TP, None),
    )
    out_specs = (P(None, KV_TP), P(KV, TP, None, None))
    return jax.shard_map(
        functools.partial(local, sizes),
        mesh=torus,
        in_specs=in_specs,
        out_specs=out_specs,
        check_vma=False,
    )
```

```python
import functools

import jax
import jax.numpy as jnp
from jax import lax
from jax.experimental import pallas as pl
from jax.experimental.pallas import tpu as pltpu
from jax.sharding import Mesh
from jax.sharding import PartitionSpec as P

EPSILON = 1e-06
MESH = pl.DeviceIdType.MESH
KV_TP = ("kv_0", "kv_1", "tp_0", "tp_1")
KV = ("kv_0", "kv_1")
TP = ("tp_0", "tp_1")
F32 = jnp.float32
BF16 = jnp.bfloat16


def silu(v):
    return v / (1.0 + jnp.exp(-v))


def layer_kernel(
    sizes,
    tok_ref,
    mix_gain_ref,
    wq_ref,
    wk_ref,
    wv_ref,
    wg_ref,
    wbeta_ref,
    wdecay_ref,
    rate_ref,
    out_gain_ref,
    state_ref,
    wout_ref,
    mlp_gain_ref,
    wup_ref,
    wdown_ref,
    mixed_ref,
    new_state_ref,
    col_t,
    w_proj,
    w_rates,
    w_beta,
    w_decay,
    mix_gain,
    out_gain,
    mlp_gain,
    rate,
    w_out,
    w_up,
    w_down,
    st,
    col_n,
    send_b,
    recv_b1,
    send_b2,
    recv_b2,
    key_t,
    query_t,
    rows_s,
    mine,
    merged,
    recv_ex,
    res,
    res_t,
    recv_r,
    hid,
    acc_up,
    total_sq,
    send_h,
    recv_h1a,
    recv_h1b,
    send_h2a,
    send_h2b,
    recv_h2a,
    recv_h2b,
    send_x,
    recv_x,
    local_sem,
    a_send,
    a_recv,
    b1_send,
    b1_recv,
    b2_send,
    b2_recv,
    d_send,
    d_recv,
    ex_send,
    ex_recv,
    fa_send,
    fb_send,
    fa_recv,
    fb_recv,
    r_send,
    r_recv,
    swap_send,
    swap_recv,
    h1a_send,
    h1b_send,
    h1a_recv,
    h1b_recv,
    h2_send,
    h2_recv,
    x_send,
    x_recv,
):
    nz, ny, nx, nc = sizes
    nkv, ntp = nz * ny, nx * nc
    z, y = lax.axis_index("kv_0"), lax.axis_index("kv_1")
    x, c = lax.axis_index("tp_0"), lax.axis_index("tp_1")
    kv, tp = z * ny + y, x * nc + c
    partner = {"tp_1": nc - 1 - c}

    dt, rows = tok_ref.shape
    ff = wup_ref.shape[1]
    dk = dt * ntp
    width = dk * nkv
    rb, heads, head = st.shape[0], st.shape[1], st.shape[2]
    proj = heads * head
    rh = rows // nc
    rc = rh // 2
    other = nc - 1 - c

    def kv_dev(k):
        return {"kv_0": k // ny, "kv_1": lax.rem(k, ny)}

    def tp_dev(t):
        return {"tp_0": t // nc, "tp_1": lax.rem(t, nc)}

    def remote(src, dst, send_sem, recv_sem, dev):
        return pltpu.make_async_remote_copy(
            src_ref=src,
            dst_ref=dst,
            send_sem=send_sem,
            recv_sem=recv_sem,
            device_id=dev,
            device_id_type=MESH,
        )

    def all_received(ref, send_sem, recv_sem):
        remote(ref, ref, send_sem, recv_sem, partner).wait_recv()

    def all_sent(ref, send_sem, recv_sem):
        remote(ref, ref, send_sem, recv_sem, partner).wait_send()

    def loop(lo, hi, body):
        def wrapped(i, carry):
            body(i)
            return carry

        lax.fori_loop(lo, hi, wrapped, 0)

    def ring(n):
        return sorted(range(1, n), key=lambda d: (-min(d, n - d), d))

    def block(i, n):
        return pl.ds(pl.multiple_of(i * n, n), n)

    own_tok = col_t.at[block(tp, dt), :]
    first = (
        (tok_ref, own_tok),
        (wbeta_ref, w_beta),
        (wdecay_ref, w_decay),
        (mix_gain_ref, mix_gain),
        (rate_ref, rate),
        (out_gain_ref, out_gain),
        (mlp_gain_ref, mlp_gain),
        (state_ref, st),
        (wout_ref, w_out.at[block(c, proj), :]),
        (wup_ref, w_up.at[:, pl.ds(0, ff)]),
        (wdown_ref, w_down.at[pl.ds(0, ff), :]),
    )
    copies = [
        pltpu.make_async_copy(src, dst, local_sem.at[i]) for i, (src, dst) in enumerate(first)
    ]
    for copy in copies[:4]:
        copy.start()
    for i, w in enumerate((wq_ref, wk_ref, wv_ref, wg_ref)):
        pltpu.make_async_copy(w, w_proj.at[i], local_sem.at[11]).start()
    for copy in copies[4:]:
        copy.start()

    barrier = pltpu.get_barrier_semaphore()

    def greet(dev):
        pl.semaphore_signal(barrier, inc=1, device_id=dev, device_id_type=MESH)

    def greet_tp(d):
        greet(tp_dev(lax.rem(tp + d, ntp)))

    loop(1, ntp, greet_tp)
    for d in range(1, ny):
        greet({"kv_1": lax.rem(y + d, ny)})
    for d in range(1, nz):
        greet({"kv_0": lax.rem(z + d, nz)})

    n_heads = wbeta_ref.shape[0]
    copies[1].wait()
    copies[2].wait()
    w_rates[...] = jnp.zeros_like(w_rates)
    w_rates[0:n_heads, :] = w_beta[...]
    w_rates[32 : 32 + n_heads, :] = w_decay[...]

    copies[0].wait()
    copies[3].wait()
    pl.semaphore_wait(barrier, ntp - 1 + ny - 1 + nz - 1)

    def tp_peers():
        near = [(0, 1)] if nc == 2 else []
        return [(dx, dc) for dx in ring(nx) for dc in range(nc)] + near

    def tp_peer(dx, dc):
        return lax.rem(x + dx, nx) * nc + lax.rem(c + dc, nc)

    for dx, dc in tp_peers():
        remote(own_tok, own_tok, a_send, a_recv, tp_dev(tp_peer(dx, dc))).start()

    a_all = col_t.at[pl.ds(0, (ntp - 1) * dt), :]
    all_received(a_all, a_send, a_recv)

    cols = col_t[...].astype(F32).T
    col_n[...] = cols.astype(BF16)
    normed = (cols * mix_gain[...]).astype(BF16)
    squares = jnp.sum(cols * cols, axis=1, keepdims=True)

    pltpu.make_async_copy(w_proj, w_proj, local_sem.at[11]).wait()

    def project(i):
        return jnp.dot(normed, w_proj[i], preferred_element_type=F32).astype(BF16)

    class Reduction:
        def __init__(self, i, column, columns, z_first):
            self.i, self.z_first = i, z_first
            self.n1, self.n2 = (nz, ny) if z_first else (ny, nz)
            self.at = pl.ds(column, columns)
            self.recv1, self.send2, self.recv2 = recv_b1[i], send_b2[i], recv_b2[i]

        def place(self, first, second):
            dz, dy = (first, second) if self.z_first else (second, first)
            return lax.rem(z + dz, nz), lax.rem(y + dy, ny)

        def rows(self, first, second):
            zk, yk = self.place(first, second)
            return send_b.at[block(zk * ny + yk, rb), self.at]

        def start(self):
            for second in [*ring(self.n2), 0]:
                for first in ring(self.n1):
                    zk, yk = self.place(first, second)
                    line, dev = (yk, {"kv_0": zk}) if self.z_first else (zk, {"kv_1": yk})
                    remote(
                        self.rows(first, second),
                        self.recv1.at[line, first - 1],
                        b1_send.at[self.i],
                        b1_recv.at[self.i, line],
                        dev,
                    ).start()

        def first_sum(self, second):
            zk, yk = self.place(0, second)
            line = yk if self.z_first else zk
            acc = self.rows(0, second)[...].astype(F32)
            all_received(self.recv1.at[line], b1_send.at[self.i], b1_recv.at[self.i, line])
            for k in range(self.n1 - 1):
                acc = acc + self.recv1[line, k].astype(F32)
            return acc

        def pass_on(self, second):
            zk, yk = self.place(0, second)
            dev = {"kv_1": yk} if self.z_first else {"kv_0": zk}
            blk = self.send2.at[second - 1]
            blk[...] = self.first_sum(second).astype(BF16)
            remote(
                blk, self.recv2.at[second - 1], b2_send.at[self.i], b2_recv.at[self.i], dev
            ).start()

        def second_sum(self, acc):
            all_received(self.recv2, b2_send.at[self.i], b2_recv.at[self.i])
            for k in range(self.n2 - 1):
                acc = acc + self.recv2[k].astype(F32)
            return acc

        def sent(self):
            all_sent(self.recv1, b1_send.at[self.i], b1_recv.at[self.i, 0])
            all_sent(self.recv2, b2_send.at[self.i], b2_recv.at[self.i])

    q_end, k_end = proj + 128, 2 * proj + 128
    for_query = Reduction(0, 0, q_end, True)
    for_key = Reduction(1, q_end, proj, False)
    for_value = Reduction(2, k_end, proj, True)
    for_gate = Reduction(3, k_end + proj, proj, False)

    send_b[:, q_end:k_end] = project(1)
    for_key.start()
    contract_last = (((1,), (1,)), ((), ()))
    rates_part = lax.dot_general(
        normed, w_rates[...], contract_last, preferred_element_type=F32
    )
    lane = lax.broadcasted_iota(jnp.int32, rates_part.shape, 1)
    rates_part = jnp.where(lane == 63, squares, rates_part)
    high = rates_part.astype(BF16).astype(F32)
    low = pltpu.roll(rates_part - high, 64, 1)
    send_b[:, proj:q_end] = jnp.where(lane < 64, high, low).astype(BF16)
    send_b[:, :proj] = project(0)
    for_query.start()
    send_b[:, k_end : k_end + proj] = project(2)
    for_value.start()
    send_b[:, k_end + proj :] = project(3)
    for_gate.start()

    def pass_on_both(by_z, by_y):
        for i in range(max(ny, nz) - 1):
            if i < nz - 1:
                by_y.pass_on(ring(nz)[i])
            if i < ny - 1:
                by_z.pass_on(ring(ny)[i])
        return by_z.first_sum(0), by_y.first_sum(0)

    query_sum, key_sum = pass_on_both(for_query, for_key)

    value_sum, gate_sum = pass_on_both(for_value, for_gate)

    key_sum = for_key.second_sum(key_sum)
    query_sum = for_query.second_sum(query_sum)

    swaps = [
        remote(
            w_out.at[block(c, proj), :],
            w_out.at[block(c, proj), :],
            swap_send.at[0],
            swap_recv.at[0],
            partner,
        ),
        remote(
            w_up.at[:, pl.ds(0, ff)],
            w_up.at[:, pl.ds(ff, ff)],
            swap_send.at[1],
            swap_recv.at[1],
            partner,
        ),
        remote(
            w_down.at[pl.ds(0, ff), :],
            w_down.at[pl.ds(ff, ff), :],
            swap_send.at[2],
            swap_recv.at[2],
            partner,
        ),
    ]
    for i in range(3):
        copies[8 + i].wait()
        swaps[i].start()

    rates = query_sum[:, proj:]
    rates = rates + pltpu.roll(rates, 64, 1)
    lane_b = lax.broadcasted_iota(jnp.int32, rates.shape, 1)

    def pick(i):
        return jnp.sum(jnp.where(lane_b == i, rates, 0.0), axis=1, keepdims=True)

    for i in range(4, 8):
        copies[i].wait()
    row_scale = lax.rsqrt(pick(63) / width + EPSILON)
    repeat = 128 // rb
    group = 4
    for h in range(heads):
        at = slice(h * head, (h + 1) * head)
        beta_raw = pick(tp * heads + h) * row_scale
        decay_raw = pick(32 + tp * heads + h) * row_scale
        beta = 1.0 / (1.0 + jnp.exp(-beta_raw))
        softplus = jnp.maximum(decay_raw, 0.0) + jnp.log1p(jnp.exp(-jnp.abs(decay_raw)))
        decay = jnp.exp(-rate[0:1, h : h + 1] * softplus)
        query = silu(query_sum[:, at] * row_scale)
        query = query * lax.rsqrt(jnp.sum(query * query, axis=1, keepdims=True) + EPSILON)
        query = query * head ** (-0.5)
        key = silu(key_sum[:, at] * row_scale)
        key = key * lax.rsqrt(jnp.sum(key * key, axis=1, keepdims=True) + EPSILON)
        key_tr = jnp.concatenate([key] * repeat, axis=0).T
        query_tr = jnp.concatenate([query] * repeat, axis=0).T
        for g in range(rb // group):
            key_t[g, h] = pltpu.roll(key_tr, (128 - g * group) % 128, 1) if g else key_tr
            query_t[g, h] = pltpu.roll(query_tr, (128 - g * group) % 128, 1) if g else query_tr
        shape = (rb, head)
        rows_s[0, h] = jnp.broadcast_to(decay, shape)
        rows_s[1, h] = jnp.broadcast_to(beta, shape)
        rows_s[2, h] = jnp.broadcast_to(
            jnp.sum(key * query, axis=1, keepdims=True), shape
        )

    def read_group(g):
        for i in range(group):
            b = g * group + i
            for h in range(heads):
                state = st[b, h]
                rows_s[3, h, pl.ds(b, 1), :] = jnp.sum(
                    state * key_t[g, h, :, i : i + 1], axis=0, keepdims=True
                )
                rows_s[4, h, pl.ds(b, 1), :] = jnp.sum(
                    state * query_t[g, h, :, i : i + 1], axis=0, keepdims=True
                )

    loop(0, rb // group, read_group)

    value_sum = for_value.second_sum(value_sum)
    gate_sum = for_gate.second_sum(gate_sum)
    for h in range(heads):
        at = slice(h * head, (h + 1) * head)
        decay = rows_s[0, h]
        value = silu(value_sum[:, at] * row_scale)
        change = rows_s[1, h] * (value - decay * rows_s[3, h])
        read = decay * rows_s[4, h] + rows_s[2, h] * change
        rows_s[3, h] = change
        scale = lax.rsqrt(jnp.sum(read * read, axis=1, keepdims=True) / head + EPSILON)
        gate = silu(gate_sum[:, at] * row_scale)
        mine[:, at] = (read * scale * out_gain[...] * gate).astype(BF16)

    per_half = nkv // nc
    home = kv // per_half
    my_rows = block(lax.rem(kv, per_half), rb)
    slot = merged.at[my_rows, block(c, proj)]

    def d_bytes(n):
        return send_b.at[pl.ds(0, n * rb), pl.ds(0, proj)]

    def hops(d):
        dz, dy = d // ny, d % ny
        return min(dz, nz - dz) + min(dy, ny - dy)

    def kv_peer(d):
        return lax.rem(z + d // ny, nz) * ny + lax.rem(y + d % ny, ny)

    for d in sorted(range(1, nkv), key=lambda d: -hops(d)):
        dev = {**kv_dev(kv_peer(d)), "tp_1": home}
        remote(mine, slot, d_send, d_recv, dev).start()

    @pl.when(home != c)
    def _():
        remote(mine, slot, d_send, d_recv, {"tp_1": home}).start()

    @pl.when(home == c)
    def _():
        merged[my_rows, block(c, proj)] = mine[...]

    def write_group(g):
        for i in range(group):
            b = g * group + i
            for h in range(heads):
                st[b, h] = (
                    rows_s[0, h, pl.ds(b, 1), :] * st[b, h]
                    + key_t[g, h, :, i : i + 1] * rows_s[3, h, pl.ds(b, 1), :]
                )

    loop(0, rb // group, write_group)
    state_out = pltpu.make_async_copy(st, new_state_ref, local_sem.at[12])
    state_out.start()
    all_sent(a_all, a_send, a_recv)
    for reduction in (for_query, for_key, for_value, for_gate):
        reduction.sent()

    @pl.when(home == c)
    def _():
        all_received(d_bytes(nkv - 1), d_send, d_recv)

    @pl.when(home != c)
    def _():
        all_received(d_bytes(nkv), d_send, d_recv)

    swaps[0].wait_recv()

    def ex_copy(half, dev):
        blk = recv_ex.at[x, pl.ds(half * rc, rc), :]
        return remote(blk, blk, ex_send.at[half], ex_recv.at[half], dev)

    def ex_all(half):
        return recv_ex.at[pl.ds(0, nx - 1), pl.ds(half * rc, rc), :]

    for half in range(2):
        at = slice(half * rc, (half + 1) * rc)
        part = jnp.dot(merged[at, :], w_out[...], preferred_element_type=F32)
        recv_ex[x, at] = part.astype(BF16)
        for d in ring(nx):
            ex_copy(half, {"tp_0": lax.rem(x + d, nx)}).start()

    def residual(half):
        all_received(ex_all(half), ex_send.at[half], ex_recv.at[half])
        at = slice(half * rc, (half + 1) * rc)
        branch = recv_ex[0, at].astype(F32)
        for i in range(1, nx):
            branch = branch + recv_ex[i, at].astype(F32)
        tok = col_n[pl.ds(pl.multiple_of(c * rh + half * rc, rc), rc), :]
        res[kv, at] = (tok.astype(F32) + branch).astype(BF16)

    rows_a, rows_b = pl.ds(0, rc), pl.ds(rc, rc)

    def fa_copy(k, dev):
        blk = res.at[k, rows_a, :]
        return remote(blk, blk, fa_send, fa_recv.at[k], dev)

    def fb_copy(k, dev):
        blk = res.at[k, rows_b, :]
        return remote(blk, blk, fb_send, fb_recv.at[k], dev)

    def y_dev(d):
        return {"kv_1": lax.rem(y + d, ny)}

    def z_dev(d):
        return {"kv_0": lax.rem(z + d, nz)}

    residual(0)
    for d in ring(ny):
        fa_copy(kv, y_dev(d)).start()
    for d in ring(nz):
        fa_copy(kv, z_dev(d)).start()
    residual(1)
    for d in ring(nz):
        fb_copy(kv, z_dev(d)).start()
    for d in ring(ny):
        fb_copy(kv, y_dev(d)).start()

    res_t[...] = res[kv].astype(F32).T.astype(BF16)
    r_copy = remote(
        res_t.at[block(x * nc + other, dt), :], recv_r, r_send, r_recv, partner
    )
    r_copy.start()

    def up(*blocks):
        total, acc = total_sq[...], acc_up[...]
        for j in blocks:
            k = lax.rem(z + nz - j // ny, nz) * ny + lax.rem(y + ny - lax.rem(j, ny), ny)
            at = block(k, dk)
            blk = res[k].astype(F32)
            sq = blk * blk
            for i in range(dk // 128):
                total = total + sq[:, i * 128 : (i + 1) * 128]
            acc = acc + jnp.dot(
                (blk * mlp_gain[:, at]).astype(BF16), w_up[at, :], preferred_element_type=F32
            )
        total_sq[...], acc_up[...] = total, acc

    acc_up[...] = jnp.zeros_like(acc_up)
    total_sq[...] = jnp.zeros_like(total_sq)
    for swap in swaps[1:]:
        swap.wait_recv()
    up(0)

    @pl.when(home == c)
    def _():
        all_sent(d_bytes(nkv - 1), d_send, d_recv)

    @pl.when(home != c)
    def _():
        all_sent(d_bytes(nkv), d_send, d_recv)

    for half in range(2):
        all_sent(ex_all(half), ex_send.at[half], ex_recv.at[half])

    for i in range(1, max(ny, nz)):
        if i < ny:
            k = z * ny + lax.rem(y + ny - i, ny)
            fa_copy(k, partner).wait_recv()
            for d in ring(nz):
                fa_copy(k, z_dev(d)).start()
        if i < nz:
            k = lax.rem(z + nz - i, nz) * ny + y
            fb_copy(k, partner).wait_recv()
            for d in ring(ny):
                fb_copy(k, y_dev(d)).start()

    n_late = max((nz - 1) * ny, (ny - 1) * nz)

    def late(i):
        zd, yd = 1 + lax.rem(i, nz - 1), i // (nz - 1)
        k = lax.rem(z + nz - zd, nz) * ny + lax.rem(y + ny - yd, ny)
        fa_copy(k, partner).wait_recv()
        yd, zd = 1 + lax.rem(i, ny - 1), i // (ny - 1)
        k = lax.rem(z + nz - zd, nz) * ny + lax.rem(y + ny - yd, ny)
        fb_copy(k, partner).wait_recv()

    lag = 0
    for j in range(1, nkv):
        zd, yd = j // ny, j % ny
        ready = max(yd * (nz - 1) + zd - 1 if zd else 0, zd * (ny - 1) + yd - 1 if yd else 0)
        lag = max(lag, ready - (j - 1))

    loop(0, lag, late)

    def late_and_up(i):
        late(i)
        up(i - lag + 1)

    loop(lag, n_late, late_and_up)

    up(*range(n_late - lag + 1, nkv))

    scale = lax.rsqrt(jnp.sum(total_sq[...], axis=1, keepdims=True) / width + EPSILON)
    relu = jnp.maximum(acc_up[...] * scale, 0.0)
    hid[...] = (relu * relu).astype(BF16)

    part_a, part_b = pl.ds(0, rc), pl.ds(rc, rc)

    def h1a_copy(dz, k):
        return remote(
            send_h.at[k, part_a, :],
            recv_h1a.at[lax.rem(k, ny), dz - 1],
            h1a_send,
            h1a_recv.at[lax.rem(k, ny)],
            {"kv_0": k // ny},
        )

    def h1b_copy(dy, k):
        return remote(
            send_h.at[k, part_b, :],
            recv_h1b.at[k // ny, dy - 1],
            h1b_send,
            h1b_recv.at[k // ny],
            {"kv_1": lax.rem(k, ny)},
        )

    def down(dz, dy):
        zk, yk = lax.rem(z + dz, nz), lax.rem(y + dy, ny)
        k = zk * ny + yk
        out = jnp.dot(hid[...], w_down[:, block(k, dk)], preferred_element_type=F32)
        send_h[k] = out.astype(BF16)
        if dz:
            h1a_copy(dz, k).start()
        if dy:
            h1b_copy(dy, k).start()

    z_order, y_order = [*ring(nz), 0], [*ring(ny), 0]
    for s in range(max(nz, ny)):
        shell = [(i, s) for i in range(s, nz)] + [(s, i) for i in range(s + 1, ny)]
        for i, j in shell:
            if i < nz and j < ny:
                down(z_order[i], y_order[j])
    all_sent(res.at[pl.ds(0, nkv - 1), rows_a, :], fa_send, fa_recv.at[0])
    all_sent(res.at[pl.ds(0, nkv - 1), rows_b, :], fb_send, fb_recv.at[0])
    for swap in swaps:
        swap.wait_send()
    r_copy.wait_send()

    def h1a_sum(yk):
        acc = send_h[z * ny + yk, 0:rc, :].astype(F32)
        all_received(recv_h1a.at[yk], h1a_send, h1a_recv.at[yk])
        for i in range(nz - 1):
            acc = acc + recv_h1a[yk, i].astype(F32)
        return acc

    def h1b_sum(zk):
        acc = send_h[zk * ny + y, rc : 2 * rc, :].astype(F32)
        all_received(recv_h1b.at[zk], h1b_send, h1b_recv.at[zk])
        for i in range(ny - 1):
            acc = acc + recv_h1b[zk, i].astype(F32)
        return acc

    def h2a_copy(d):
        blk = send_h2a.at[d - 1]
        dev = {"kv_1": lax.rem(y + d, ny)}
        return remote(blk, recv_h2a.at[d - 1], h2_send.at[0], h2_recv.at[0], dev)

    def h2b_copy(d):
        blk = send_h2b.at[d - 1]
        dev = {"kv_0": lax.rem(z + d, nz)}
        return remote(blk, recv_h2b.at[d - 1], h2_send.at[1], h2_recv.at[1], dev)

    for i in range(max(ny, nz) - 1):
        if i < ny - 1:
            d = ring(ny)[i]
            send_h2a[d - 1] = h1a_sum(lax.rem(y + d, ny)).astype(BF16)
            h2a_copy(d).start()
        if i < nz - 1:
            d = ring(nz)[i]
            send_h2b[d - 1] = h1b_sum(lax.rem(z + d, nz)).astype(BF16)
            h2b_copy(d).start()
    sum_a = h1a_sum(y)
    sum_b = h1b_sum(z)
    all_received(recv_h2a, h2_send.at[0], h2_recv.at[0])
    for i in range(ny - 1):
        sum_a = sum_a + recv_h2a[i].astype(F32)
    all_received(recv_h2b, h2_send.at[1], h2_recv.at[1])
    for i in range(nz - 1):
        sum_b = sum_b + recv_h2b[i].astype(F32)

    own_sum = jnp.concatenate([sum_a, sum_b], axis=0).T.astype(BF16)
    send_x[...] = own_sum

    def x_copy(peer):
        blk = send_x.at[block(peer, dt), :]
        return remote(blk, recv_x.at[tp], x_send, x_recv, tp_dev(peer))

    x_all = recv_x.at[pl.ds(0, ntp - 1)]
    for dx, dc in tp_peers():
        x_copy(tp_peer(dx, dc)).start()
    recv_x[tp] = send_x[block(tp, dt), :]

    all_received(x_all, x_send, x_recv)
    r_copy.wait_recv()

    def finish(core, residual):
        total = residual.astype(F32) + recv_x[core].astype(F32)
        for xx in range(1, nx):
            total = total + recv_x[xx * nc + core].astype(F32)
        mixed_ref[:, block(core, rh)] = total.astype(BF16)

    finish(c, res_t[block(tp, dt), :])
    finish(other, recv_r[...])

    all_sent(x_all, x_send, x_recv)
    all_sent(recv_h1a, h1a_send, h1a_recv.at[0])
    all_sent(recv_h1b, h1b_send, h1b_recv.at[0])
    all_sent(recv_h2a, h2_send.at[0], h2_recv.at[0])
    all_sent(recv_h2b, h2_send.at[1], h2_recv.at[1])
    state_out.wait()


def local(
    sizes,
    tokens,
    mix_gain,
    w_query,
    w_key,
    w_value,
    w_gate,
    w_beta,
    w_decay,
    decay_rate,
    out_gain,
    state,
    w_out,
    mlp_gain,
    w_up,
    w_down,
):
    nz, ny, nx, nc = sizes
    nkv, ntp = nz * ny, nx * nc
    rows, dt = tokens.shape
    dk = dt * ntp
    rb, heads, head, _ = state.shape
    proj = heads * head
    sent = 4 * proj + 128
    reductions = ((proj + 128, True), (proj, False), (proj, True), (proj, False))
    first = [(ny, nz) if by_z else (nz, ny) for _, by_z in reductions]
    widths = [w for w, _ in reductions]
    n_heads = w_beta.shape[1]
    ff = w_up.shape[1]
    rh = rows // nc
    rc = rh // 2
    vmem, dma = pltpu.VMEM, pltpu.SemaphoreType.DMA
    scratch = [
        vmem((dk, rows), BF16),
        vmem((4, dk, proj), BF16),
        vmem((128, dk), BF16),
        vmem((n_heads, dk), BF16),
        vmem((n_heads, dk), BF16),
        vmem((1, dk), F32),
        vmem((1, head), F32),
        vmem((1, dk * nkv), F32),
        vmem((1, heads), F32),
        vmem((nc * proj, dk), BF16),
        vmem((w_up.shape[0], 2 * ff), BF16),
        vmem((2 * ff, w_down.shape[1]), BF16),
        vmem(state.shape, F32),
        vmem((rows, dk), BF16),
        vmem((rows, sent), BF16),
        [vmem((n2, n1 - 1, rb, w), BF16) for (n2, n1), w in zip(first, widths)],
        [vmem((n2 - 1, rb, w), BF16) for (n2, n1), w in zip(first, widths)],
        [vmem((n2 - 1, rb, w), BF16) for (n2, n1), w in zip(first, widths)],
        vmem((rb // 4, heads, head, 128), F32),
        vmem((rb // 4, heads, head, 128), F32),
        vmem((5, heads, rb, head), F32),
        vmem((rb, proj), BF16),
        vmem((rh, nc * proj), BF16),
        vmem((nx, rh, dk), BF16),
        vmem((nkv, rh, dk), BF16),
        vmem((dk, rh), BF16),
        vmem((dt, rh), BF16),
        vmem((rh, 2 * ff), BF16),
        vmem((rh, 2 * ff), F32),
        vmem((rh, 128), F32),
        vmem((nkv, rh, dk), BF16),
        vmem((ny, nz - 1, rc, dk), BF16),
        vmem((nz, ny - 1, rc, dk), BF16),
        vmem((ny - 1, rc, dk), BF16),
        vmem((nz - 1, rc, dk), BF16),
        vmem((ny - 1, rc, dk), BF16),
        vmem((nz - 1, rc, dk), BF16),
        vmem((dk, rh), BF16),
        vmem((ntp, dt, rh), BF16),
        dma((13,)),
        dma(()),
        dma(()),
        dma((4,)),
        dma((4, max(ny, nz))),
        dma((4,)),
        dma((4,)),
        dma(()),
        dma(()),
        dma((2,)),
        dma((2,)),
        dma(()),
        dma(()),
        dma((nkv,)),
        dma((nkv,)),
        dma(()),
        dma(()),
        dma((3,)),
        dma((3,)),
        dma(()),
        dma(()),
        dma((ny,)),
        dma((nz,)),
        dma((2,)),
        dma((2,)),
        dma(()),
        dma(()),
    ]
    in_hbm = pl.BlockSpec(memory_space=pl.ANY)
    in_vmem = pl.BlockSpec(memory_space=pltpu.VMEM)
    mixed_t, new_state = pl.pallas_call(
        functools.partial(layer_kernel, sizes),
        out_shape=(
            pltpu.VMEM((dt, rows), BF16),
            pltpu.VMEM(state.shape, F32),
        ),
        in_specs=[in_hbm] * 15,
        out_specs=(in_vmem, in_hbm),
        scratch_shapes=scratch,
        compiler_params=pltpu.CompilerParams(
            collective_id=0, has_side_effects=True, vmem_limit_bytes=63_500_000
        ),
        name="layer",
    )(
        tokens.T,
        mix_gain[None, :],
        w_query,
        w_key,
        w_value,
        w_gate,
        w_beta.T,
        w_decay.T,
        decay_rate[None, :],
        out_gain[None, :],
        state,
        w_out,
        mlp_gain[None, :],
        w_up,
        w_down,
    )
    return mixed_t.T, new_state


def solution(mesh):
    n = dict(mesh.shape)
    sizes = (n["kv"] // 4, 4, n["tp"] // 2, 2) if n["kv"] >= 8 else (2, n["kv"] // 2, n["tp"] // 2, 2)
    torus = Mesh(mesh.devices.reshape(sizes), KV_TP)
    in_specs = (
        P(None, KV_TP),
        P(KV),
        P(KV, TP),
        P(KV, TP),
        P(KV, TP),
        P(KV, TP),
        P(KV, None),
        P(KV, None),
        P(TP),
        P(),
        P(KV, TP, None, None),
        P(TP, KV),
        P(),
        P(None, KV_TP),
        P(KV_TP, None),
    )
    out_specs = (P(None, KV_TP), P(KV, TP, None, None))
    return jax.shard_map(
        functools.partial(local, sizes),
        mesh=torus,
        in_specs=in_specs,
        out_specs=out_specs,
        check_vma=False,
    )
```

```python
import functools

import jax
import jax.numpy as jnp
from jax import lax
from jax.experimental import pallas as pl
from jax.experimental.pallas import tpu as pltpu
from jax.sharding import Mesh
from jax.sharding import PartitionSpec as P

EPSILON = 1e-06
MESH = pl.DeviceIdType.MESH
KV_TP = ("kv_0", "kv_1", "tp_0", "tp_1")
KV = ("kv_0", "kv_1")
TP = ("tp_0", "tp_1")
F32 = jnp.float32
BF16 = jnp.bfloat16


def silu(v):
    return v / (1.0 + jnp.exp(-v))


def layer_kernel(
    sizes,
    tok_ref,
    mix_gain_ref,
    wq_ref,
    wk_ref,
    wv_ref,
    wg_ref,
    wbeta_ref,
    wdecay_ref,
    rate_ref,
    out_gain_ref,
    state_ref,
    wout_ref,
    mlp_gain_ref,
    wup_ref,
    wdown_ref,
    mixed_ref,
    new_state_ref,
    col_t,
    w_proj,
    w_rates,
    w_beta,
    w_decay,
    mix_gain,
    out_gain,
    mlp_gain,
    rate,
    w_out,
    w_up,
    w_down,
    st,
    col_n,
    send_b,
    recv_b1,
    send_b2,
    recv_b2,
    key_t,
    query_t,
    rows_s,
    mine,
    merged,
    recv_ex,
    res,
    res_t,
    recv_r,
    hid,
    acc_up,
    total_sq,
    send_h,
    recv_h1a,
    recv_h1b,
    send_xa,
    send_xb,
    recv_x,
    bytes_x,
    local_sem,
    a_send,
    a_recv,
    b1_send,
    b1_recv,
    b2_send,
    b2_recv,
    d_send,
    d_recv,
    ex_send,
    ex_recv,
    fa_send,
    fb_send,
    fa_recv,
    fb_recv,
    r_send,
    r_recv,
    swap_send,
    swap_recv,
    h1a_send,
    h1b_send,
    h1a_recv,
    h1b_recv,
    x_send,
    x_recv,
):
    nz, ny, nx, nc = sizes
    nkv, ntp = nz * ny, nx * nc
    z, y = lax.axis_index("kv_0"), lax.axis_index("kv_1")
    x, c = lax.axis_index("tp_0"), lax.axis_index("tp_1")
    kv, tp = z * ny + y, x * nc + c
    partner = {"tp_1": nc - 1 - c}

    dt, rows = tok_ref.shape
    ff = wup_ref.shape[1]
    dk = dt * ntp
    width = dk * nkv
    rb, heads, head = st.shape[0], st.shape[1], st.shape[2]
    proj = heads * head
    rh = rows // nc
    rc = rh // 2
    other = nc - 1 - c

    def kv_dev(k):
        return {"kv_0": k // ny, "kv_1": lax.rem(k, ny)}

    def tp_dev(t):
        return {"tp_0": t // nc, "tp_1": lax.rem(t, nc)}

    def remote(src, dst, send_sem, recv_sem, dev):
        return pltpu.make_async_remote_copy(
            src_ref=src,
            dst_ref=dst,
            send_sem=send_sem,
            recv_sem=recv_sem,
            device_id=dev,
            device_id_type=MESH,
        )

    def all_received(ref, send_sem, recv_sem):
        remote(ref, ref, send_sem, recv_sem, partner).wait_recv()

    def all_sent(ref, send_sem, recv_sem):
        remote(ref, ref, send_sem, recv_sem, partner).wait_send()

    def loop(lo, hi, body):
        def wrapped(i, carry):
            body(i)
            return carry

        lax.fori_loop(lo, hi, wrapped, 0)

    def ring(n):
        return sorted(range(1, n), key=lambda d: (-min(d, n - d), d))

    def block(i, n):
        return pl.ds(pl.multiple_of(i * n, n), n)

    own_tok = col_t.at[block(tp, dt), :]
    first = (
        (tok_ref, own_tok),
        (wbeta_ref, w_beta),
        (wdecay_ref, w_decay),
        (mix_gain_ref, mix_gain),
        (rate_ref, rate),
        (out_gain_ref, out_gain),
        (mlp_gain_ref, mlp_gain),
        (state_ref, st),
        (wout_ref, w_out.at[block(c, proj), :]),
        (wup_ref, w_up.at[:, pl.ds(0, ff)]),
        (wdown_ref, w_down.at[pl.ds(0, ff), :]),
    )
    copies = [
        pltpu.make_async_copy(src, dst, local_sem.at[i]) for i, (src, dst) in enumerate(first)
    ]
    for copy in copies[:4]:
        copy.start()
    for i, w in enumerate((wq_ref, wk_ref, wv_ref, wg_ref)):
        pltpu.make_async_copy(w, w_proj.at[i], local_sem.at[11]).start()
    for copy in copies[4:]:
        copy.start()

    barrier = pltpu.get_barrier_semaphore()

    def greet(dev):
        pl.semaphore_signal(barrier, inc=1, device_id=dev, device_id_type=MESH)

    def greet_tp(d):
        greet(tp_dev(lax.rem(tp + d, ntp)))

    loop(1, ntp, greet_tp)
    for d in range(1, ny):
        greet({"kv_1": lax.rem(y + d, ny)})
    for d in range(1, nz):
        greet({"kv_0": lax.rem(z + d, nz)})

    n_heads = wbeta_ref.shape[0]
    copies[1].wait()
    copies[2].wait()
    w_rates[...] = jnp.zeros_like(w_rates)
    w_rates[0:n_heads, :] = w_beta[...]
    w_rates[32 : 32 + n_heads, :] = w_decay[...]

    copies[0].wait()
    copies[3].wait()
    pl.semaphore_wait(barrier, ntp - 1 + ny - 1 + nz - 1)

    def tp_peers():
        near = [(0, 1)] if nc == 2 else []
        return [(dx, dc) for dx in ring(nx) for dc in range(nc)] + near

    def tp_peer(dx, dc):
        return lax.rem(x + dx, nx) * nc + lax.rem(c + dc, nc)

    for dx, dc in tp_peers():
        remote(own_tok, own_tok, a_send, a_recv, tp_dev(tp_peer(dx, dc))).start()

    a_all = col_t.at[pl.ds(0, (ntp - 1) * dt), :]
    all_received(a_all, a_send, a_recv)

    cols = col_t[...].astype(F32).T
    col_n[...] = cols.astype(BF16)
    normed = (cols * mix_gain[...]).astype(BF16)
    squares = jnp.sum(cols * cols, axis=1, keepdims=True)

    pltpu.make_async_copy(w_proj, w_proj, local_sem.at[11]).wait()

    def project(i):
        return jnp.dot(normed, w_proj[i], preferred_element_type=F32).astype(BF16)

    class Reduction:
        def __init__(self, i, column, columns, z_first):
            self.i, self.z_first = i, z_first
            self.n1, self.n2 = (nz, ny) if z_first else (ny, nz)
            self.at = pl.ds(column, columns)
            self.recv1, self.send2, self.recv2 = recv_b1[i], send_b2[i], recv_b2[i]

        def place(self, first, second):
            dz, dy = (first, second) if self.z_first else (second, first)
            return lax.rem(z + dz, nz), lax.rem(y + dy, ny)

        def rows(self, first, second):
            zk, yk = self.place(first, second)
            return send_b.at[block(zk * ny + yk, rb), self.at]

        def start(self):
            for second in [*ring(self.n2), 0]:
                for first in ring(self.n1):
                    zk, yk = self.place(first, second)
                    line, dev = (yk, {"kv_0": zk}) if self.z_first else (zk, {"kv_1": yk})
                    remote(
                        self.rows(first, second),
                        self.recv1.at[line, first - 1],
                        b1_send.at[self.i],
                        b1_recv.at[self.i, line],
                        dev,
                    ).start()

        def first_sum(self, second):
            zk, yk = self.place(0, second)
            line = yk if self.z_first else zk
            acc = self.rows(0, second)[...].astype(F32)
            all_received(self.recv1.at[line], b1_send.at[self.i], b1_recv.at[self.i, line])
            for k in range(self.n1 - 1):
                acc = acc + self.recv1[line, k].astype(F32)
            return acc

        def pass_on(self, second):
            zk, yk = self.place(0, second)
            dev = {"kv_1": yk} if self.z_first else {"kv_0": zk}
            blk = self.send2.at[second - 1]
            blk[...] = self.first_sum(second).astype(BF16)
            remote(
                blk, self.recv2.at[second - 1], b2_send.at[self.i], b2_recv.at[self.i], dev
            ).start()

        def second_sum(self, acc):
            all_received(self.recv2, b2_send.at[self.i], b2_recv.at[self.i])
            for k in range(self.n2 - 1):
                acc = acc + self.recv2[k].astype(F32)
            return acc

        def sent(self):
            all_sent(self.recv1, b1_send.at[self.i], b1_recv.at[self.i, 0])
            all_sent(self.recv2, b2_send.at[self.i], b2_recv.at[self.i])

    q_end, k_end = proj + 128, 2 * proj + 128
    for_query = Reduction(0, 0, q_end, True)
    for_key = Reduction(1, q_end, proj, False)
    for_value = Reduction(2, k_end, proj, True)
    for_gate = Reduction(3, k_end + proj, proj, False)

    send_b[:, q_end:k_end] = project(1)
    for_key.start()
    contract_last = (((1,), (1,)), ((), ()))
    rates_part = lax.dot_general(
        normed, w_rates[...], contract_last, preferred_element_type=F32
    )
    lane = lax.broadcasted_iota(jnp.int32, rates_part.shape, 1)
    rates_part = jnp.where(lane == 63, squares, rates_part)
    high = rates_part.astype(BF16).astype(F32)
    low = pltpu.roll(rates_part - high, 64, 1)
    send_b[:, proj:q_end] = jnp.where(lane < 64, high, low).astype(BF16)
    send_b[:, :proj] = project(0)
    for_query.start()
    send_b[:, k_end : k_end + proj] = project(2)
    for_value.start()
    send_b[:, k_end + proj :] = project(3)
    for_gate.start()

    def pass_on_both(by_z, by_y):
        for i in range(max(ny, nz) - 1):
            if i < nz - 1:
                by_y.pass_on(ring(nz)[i])
            if i < ny - 1:
                by_z.pass_on(ring(ny)[i])
        return by_z.first_sum(0), by_y.first_sum(0)

    query_sum, key_sum = pass_on_both(for_query, for_key)

    value_sum, gate_sum = pass_on_both(for_value, for_gate)

    key_sum = for_key.second_sum(key_sum)
    query_sum = for_query.second_sum(query_sum)

    swaps = [
        remote(
            w_out.at[block(c, proj), :],
            w_out.at[block(c, proj), :],
            swap_send.at[0],
            swap_recv.at[0],
            partner,
        ),
        remote(
            w_up.at[:, pl.ds(0, ff)],
            w_up.at[:, pl.ds(ff, ff)],
            swap_send.at[1],
            swap_recv.at[1],
            partner,
        ),
        remote(
            w_down.at[pl.ds(0, ff), :],
            w_down.at[pl.ds(ff, ff), :],
            swap_send.at[2],
            swap_recv.at[2],
            partner,
        ),
    ]
    for i in range(3):
        copies[8 + i].wait()
        swaps[i].start()

    rates = query_sum[:, proj:]
    rates = rates + pltpu.roll(rates, 64, 1)
    lane_b = lax.broadcasted_iota(jnp.int32, rates.shape, 1)

    def pick(i):
        return jnp.sum(jnp.where(lane_b == i, rates, 0.0), axis=1, keepdims=True)

    for i in range(4, 8):
        copies[i].wait()
    row_scale = lax.rsqrt(pick(63) / width + EPSILON)
    repeat = 128 // rb
    group = 4
    for h in range(heads):
        at = slice(h * head, (h + 1) * head)
        beta_raw = pick(tp * heads + h) * row_scale
        decay_raw = pick(32 + tp * heads + h) * row_scale
        beta = 1.0 / (1.0 + jnp.exp(-beta_raw))
        softplus = jnp.maximum(decay_raw, 0.0) + jnp.log1p(jnp.exp(-jnp.abs(decay_raw)))
        decay = jnp.exp(-rate[0:1, h : h + 1] * softplus)
        query = silu(query_sum[:, at] * row_scale)
        query = query * lax.rsqrt(jnp.sum(query * query, axis=1, keepdims=True) + EPSILON)
        query = query * head ** (-0.5)
        key = silu(key_sum[:, at] * row_scale)
        key = key * lax.rsqrt(jnp.sum(key * key, axis=1, keepdims=True) + EPSILON)
        key_tr = jnp.concatenate([key] * repeat, axis=0).T
        query_tr = jnp.concatenate([query] * repeat, axis=0).T
        for g in range(rb // group):
            key_t[g, h] = pltpu.roll(key_tr, (128 - g * group) % 128, 1) if g else key_tr
            query_t[g, h] = pltpu.roll(query_tr, (128 - g * group) % 128, 1) if g else query_tr
        shape = (rb, head)
        rows_s[0, h] = jnp.broadcast_to(decay, shape)
        rows_s[1, h] = jnp.broadcast_to(beta, shape)
        rows_s[2, h] = jnp.broadcast_to(
            jnp.sum(key * query, axis=1, keepdims=True), shape
        )

    def read_group(g):
        for i in range(group):
            b = g * group + i
            for h in range(heads):
                state = st[b, h]
                rows_s[3, h, pl.ds(b, 1), :] = jnp.sum(
                    state * key_t[g, h, :, i : i + 1], axis=0, keepdims=True
                )
                rows_s[4, h, pl.ds(b, 1), :] = jnp.sum(
                    state * query_t[g, h, :, i : i + 1], axis=0, keepdims=True
                )

    loop(0, rb // group, read_group)

    value_sum = for_value.second_sum(value_sum)
    gate_sum = for_gate.second_sum(gate_sum)
    for h in range(heads):
        at = slice(h * head, (h + 1) * head)
        decay = rows_s[0, h]
        value = silu(value_sum[:, at] * row_scale)
        change = rows_s[1, h] * (value - decay * rows_s[3, h])
        read = decay * rows_s[4, h] + rows_s[2, h] * change
        rows_s[3, h] = change
        scale = lax.rsqrt(jnp.sum(read * read, axis=1, keepdims=True) / head + EPSILON)
        gate = silu(gate_sum[:, at] * row_scale)
        mine[:, at] = (read * scale * out_gain[...] * gate).astype(BF16)

    per_half = nkv // nc
    home = kv // per_half
    my_rows = block(lax.rem(kv, per_half), rb)
    slot = merged.at[my_rows, block(c, proj)]

    def d_bytes(n):
        return send_b.at[pl.ds(0, n * rb), pl.ds(0, proj)]

    def hops(d):
        dz, dy = d // ny, d % ny
        return min(dz, nz - dz) + min(dy, ny - dy)

    def kv_peer(d):
        return lax.rem(z + d // ny, nz) * ny + lax.rem(y + d % ny, ny)

    for d in sorted(range(1, nkv), key=lambda d: -hops(d)):
        dev = {**kv_dev(kv_peer(d)), "tp_1": home}
        remote(mine, slot, d_send, d_recv, dev).start()

    @pl.when(home != c)
    def _():
        remote(mine, slot, d_send, d_recv, {"tp_1": home}).start()

    @pl.when(home == c)
    def _():
        merged[my_rows, block(c, proj)] = mine[...]

    def write_group(g):
        for i in range(group):
            b = g * group + i
            for h in range(heads):
                st[b, h] = (
                    rows_s[0, h, pl.ds(b, 1), :] * st[b, h]
                    + key_t[g, h, :, i : i + 1] * rows_s[3, h, pl.ds(b, 1), :]
                )

    loop(0, rb // group, write_group)
    state_out = pltpu.make_async_copy(st, new_state_ref, local_sem.at[12])
    state_out.start()
    all_sent(a_all, a_send, a_recv)
    for reduction in (for_query, for_key, for_value, for_gate):
        reduction.sent()

    @pl.when(home == c)
    def _():
        all_received(d_bytes(nkv - 1), d_send, d_recv)

    @pl.when(home != c)
    def _():
        all_received(d_bytes(nkv), d_send, d_recv)

    swaps[0].wait_recv()

    def ex_copy(half, dev):
        blk = recv_ex.at[x, pl.ds(half * rc, rc), :]
        return remote(blk, blk, ex_send.at[half], ex_recv.at[half], dev)

    def ex_all(half):
        return recv_ex.at[pl.ds(0, nx - 1), pl.ds(half * rc, rc), :]

    for half in range(2):
        at = slice(half * rc, (half + 1) * rc)
        part = jnp.dot(merged[at, :], w_out[...], preferred_element_type=F32)
        recv_ex[x, at] = part.astype(BF16)
        for d in ring(nx):
            ex_copy(half, {"tp_0": lax.rem(x + d, nx)}).start()

    def residual(half):
        all_received(ex_all(half), ex_send.at[half], ex_recv.at[half])
        at = slice(half * rc, (half + 1) * rc)
        branch = recv_ex[0, at].astype(F32)
        for i in range(1, nx):
            branch = branch + recv_ex[i, at].astype(F32)
        tok = col_n[pl.ds(pl.multiple_of(c * rh + half * rc, rc), rc), :]
        res[kv, at] = (tok.astype(F32) + branch).astype(BF16)

    rows_a, rows_b = pl.ds(0, rc), pl.ds(rc, rc)

    def fa_copy(k, dev):
        blk = res.at[k, rows_a, :]
        return remote(blk, blk, fa_send, fa_recv.at[k], dev)

    def fb_copy(k, dev):
        blk = res.at[k, rows_b, :]
        return remote(blk, blk, fb_send, fb_recv.at[k], dev)

    def y_dev(d):
        return {"kv_1": lax.rem(y + d, ny)}

    def z_dev(d):
        return {"kv_0": lax.rem(z + d, nz)}

    residual(0)
    for d in ring(ny):
        fa_copy(kv, y_dev(d)).start()
    for d in ring(nz):
        fa_copy(kv, z_dev(d)).start()
    residual(1)
    for d in ring(nz):
        fb_copy(kv, z_dev(d)).start()
    for d in ring(ny):
        fb_copy(kv, y_dev(d)).start()

    res_t[...] = res[kv].astype(F32).T.astype(BF16)
    r_copy = remote(
        res_t.at[block(x * nc + other, dt), :], recv_r, r_send, r_recv, partner
    )
    r_copy.start()

    def up(*blocks):
        total, acc = total_sq[...], acc_up[...]
        for j in blocks:
            k = lax.rem(z + nz - j // ny, nz) * ny + lax.rem(y + ny - lax.rem(j, ny), ny)
            at = block(k, dk)
            blk = res[k].astype(F32)
            sq = blk * blk
            for i in range(dk // 128):
                total = total + sq[:, i * 128 : (i + 1) * 128]
            acc = acc + jnp.dot(
                (blk * mlp_gain[:, at]).astype(BF16), w_up[at, :], preferred_element_type=F32
            )
        total_sq[...], acc_up[...] = total, acc

    acc_up[...] = jnp.zeros_like(acc_up)
    total_sq[...] = jnp.zeros_like(total_sq)
    for swap in swaps[1:]:
        swap.wait_recv()
    up(0)

    @pl.when(home == c)
    def _():
        all_sent(d_bytes(nkv - 1), d_send, d_recv)

    @pl.when(home != c)
    def _():
        all_sent(d_bytes(nkv), d_send, d_recv)

    for half in range(2):
        all_sent(ex_all(half), ex_send.at[half], ex_recv.at[half])

    for i in range(1, max(ny, nz)):
        if i < ny:
            k = z * ny + lax.rem(y + ny - i, ny)
            fa_copy(k, partner).wait_recv()
            for d in ring(nz):
                fa_copy(k, z_dev(d)).start()
        if i < nz:
            k = lax.rem(z + nz - i, nz) * ny + y
            fb_copy(k, partner).wait_recv()
            for d in ring(ny):
                fb_copy(k, y_dev(d)).start()

    n_late = max((nz - 1) * ny, (ny - 1) * nz)

    def late(i):
        zd, yd = 1 + lax.rem(i, nz - 1), i // (nz - 1)
        k = lax.rem(z + nz - zd, nz) * ny + lax.rem(y + ny - yd, ny)
        fa_copy(k, partner).wait_recv()
        yd, zd = 1 + lax.rem(i, ny - 1), i // (ny - 1)
        k = lax.rem(z + nz - zd, nz) * ny + lax.rem(y + ny - yd, ny)
        fb_copy(k, partner).wait_recv()

    lag = 0
    for j in range(1, nkv):
        zd, yd = j // ny, j % ny
        ready = max(yd * (nz - 1) + zd - 1 if zd else 0, zd * (ny - 1) + yd - 1 if yd else 0)
        lag = max(lag, ready - (j - 1))

    loop(0, lag, late)

    def late_and_up(i):
        late(i)
        up(i - lag + 1)

    loop(lag, n_late, late_and_up)

    up(*range(n_late - lag + 1, nkv))

    scale = lax.rsqrt(jnp.sum(total_sq[...], axis=1, keepdims=True) / width + EPSILON)
    relu = jnp.maximum(acc_up[...] * scale, 0.0)
    hid[...] = (relu * relu).astype(BF16)

    hw = dk // 2
    part_a, part_b = pl.ds(0, hw), pl.ds(hw, hw)

    def h1a_copy(dz, k):
        return remote(
            send_h.at[k, :, part_a],
            recv_h1a.at[lax.rem(k, ny), dz - 1],
            h1a_send,
            h1a_recv.at[lax.rem(k, ny)],
            {"kv_0": k // ny},
        )

    def h1b_copy(dy, k):
        return remote(
            send_h.at[k, :, part_b],
            recv_h1b.at[k // ny, dy - 1],
            h1b_send,
            h1b_recv.at[k // ny],
            {"kv_1": lax.rem(k, ny)},
        )

    def down(dz, dy):
        zk, yk = lax.rem(z + dz, nz), lax.rem(y + dy, ny)
        k = zk * ny + yk
        out = jnp.dot(hid[...], w_down[:, block(k, dk)], preferred_element_type=F32)
        send_h[k] = out.astype(BF16)
        if dz:
            h1a_copy(dz, k).start()
        if dy:
            h1b_copy(dy, k).start()

    z_order, y_order = [*ring(nz), 0], [*ring(ny), 0]
    for s in range(max(nz, ny)):
        shell = [(i, s) for i in range(s, nz)] + [(s, i) for i in range(s + 1, ny)]
        for i, j in shell:
            if i < nz and j < ny:
                down(z_order[i], y_order[j])
    all_sent(res.at[pl.ds(0, nkv - 1), rows_a, :], fa_send, fa_recv.at[0])
    all_sent(res.at[pl.ds(0, nkv - 1), rows_b, :], fb_send, fb_recv.at[0])
    for swap in swaps:
        swap.wait_send()
    r_copy.wait_send()

    def h1a_sum(yk):
        acc = send_h[z * ny + yk, :, 0:hw].astype(F32)
        all_received(recv_h1a.at[yk], h1a_send, h1a_recv.at[yk])
        for i in range(nz - 1):
            acc = acc + recv_h1a[yk, i].astype(F32)
        return acc

    def h1b_sum(zk):
        acc = send_h[zk * ny + y, :, hw : 2 * hw].astype(F32)
        all_received(recv_h1b.at[zk], h1b_send, h1b_recv.at[zk])
        for i in range(ny - 1):
            acc = acc + recv_h1b[zk, i].astype(F32)
        return acc

    pieces = ntp // 2

    def deliver(d, upper):
        if upper:
            total, line, buf = h1b_sum(lax.rem(z + d, nz)), z, send_xb.at[d]
            dev = {"kv_0": lax.rem(z + d, nz)}
        else:
            total, line, buf = h1a_sum(lax.rem(y + d, ny)), y, send_xa.at[d]
            dev = {"kv_1": lax.rem(y + d, ny)}
        buf[...] = total.T.astype(BF16)
        for piece in range(pieces):
            t = piece + pieces if upper else piece
            at = pl.ds(piece * dt, dt)

            def send(at=at, t=t):
                to = {**dev, "tp_0": t // nc, "tp_1": t % nc}
                remote(buf.at[at], recv_x.at[line, tp], x_send, x_recv, to).start()

            if d:
                send()
            else:

                @pl.when(tp != t)
                def _():
                    send()

                @pl.when(tp == t)
                def _():
                    recv_x[line, tp] = buf[at]

    for i in range(max(ny, nz)):
        if i < ny:
            deliver([*ring(ny), 0][i], False)
        if i < nz:
            deliver([*ring(nz), 0][i], True)

    def finish(lines):
        all_received(bytes_x.at[pl.ds(0, lines * ntp - 1)], x_send, x_recv)
        for core, residual in ((c, res_t[block(tp, dt), :]), (other, recv_r[...])):
            total = residual.astype(F32)
            for i in range(lines):
                for xx in range(nx):
                    total = total + recv_x[i, xx * nc + core].astype(F32)
            mixed_ref[:, block(core, rh)] = total.astype(BF16)

    r_copy.wait_recv()

    @pl.when(tp < pieces)
    def _():
        finish(ny)

    @pl.when(tp >= pieces)
    def _():
        finish(nz)

    all_sent(bytes_x.at[pl.ds(0, (ny + nz) * pieces - 1)], x_send, x_recv)
    all_sent(recv_h1a, h1a_send, h1a_recv.at[0])
    all_sent(recv_h1b, h1b_send, h1b_recv.at[0])
    state_out.wait()


STORES = 8


def store_kernel(mixed_ref, state_ref, mixed_out, state_out, sem):
    n = state_ref.shape[0] // STORES
    copies = [pltpu.make_async_copy(mixed_ref, mixed_out, sem.at[0])]
    for i in range(STORES):
        at = pl.ds(i * n, n)
        copies.append(pltpu.make_async_copy(state_ref.at[at], state_out.at[at], sem.at[1 + i]))
    for copy in copies:
        copy.start()
    for copy in copies:
        copy.wait()


def local(
    sizes,
    tokens,
    mix_gain,
    w_query,
    w_key,
    w_value,
    w_gate,
    w_beta,
    w_decay,
    decay_rate,
    out_gain,
    state,
    w_out,
    mlp_gain,
    w_up,
    w_down,
):
    nz, ny, nx, nc = sizes
    nkv, ntp = nz * ny, nx * nc
    rows, dt = tokens.shape
    dk = dt * ntp
    rb, heads, head, _ = state.shape
    proj = heads * head
    sent = 4 * proj + 128
    reductions = ((proj + 128, True), (proj, False), (proj, True), (proj, False))
    first = [(ny, nz) if by_z else (nz, ny) for _, by_z in reductions]
    widths = [w for w, _ in reductions]
    n_heads = w_beta.shape[1]
    ff = w_up.shape[1]
    rh = rows // nc
    rc = rh // 2
    vmem, dma = pltpu.VMEM, pltpu.SemaphoreType.DMA
    scratch = [
        vmem((dk, rows), BF16),
        vmem((4, dk, proj), BF16),
        vmem((128, dk), BF16),
        vmem((n_heads, dk), BF16),
        vmem((n_heads, dk), BF16),
        vmem((1, dk), F32),
        vmem((1, head), F32),
        vmem((1, dk * nkv), F32),
        vmem((1, heads), F32),
        vmem((nc * proj, dk), BF16),
        vmem((w_up.shape[0], 2 * ff), BF16),
        vmem((2 * ff, w_down.shape[1]), BF16),
        vmem(state.shape, F32),
        vmem((rows, dk), BF16),
        vmem((rows, sent), BF16),
        [vmem((n2, n1 - 1, rb, w), BF16) for (n2, n1), w in zip(first, widths)],
        [vmem((n2 - 1, rb, w), BF16) for (n2, n1), w in zip(first, widths)],
        [vmem((n2 - 1, rb, w), BF16) for (n2, n1), w in zip(first, widths)],
        vmem((rb // 4, heads, head, 128), F32),
        vmem((rb // 4, heads, head, 128), F32),
        vmem((5, heads, rb, head), F32),
        vmem((rb, proj), BF16),
        vmem((rh, nc * proj), BF16),
        vmem((nx, rh, dk), BF16),
        vmem((nkv, rh, dk), BF16),
        vmem((dk, rh), BF16),
        vmem((dt, rh), BF16),
        vmem((rh, 2 * ff), BF16),
        vmem((rh, 2 * ff), F32),
        vmem((rh, 128), F32),
        vmem((nkv, rh, dk), BF16),
        vmem((ny, nz - 1, rh, dk // 2), BF16),
        vmem((nz, ny - 1, rh, dk // 2), BF16),
        vmem((ny, dk // 2, rh), BF16),
        vmem((nz, dk // 2, rh), BF16),
        vmem((max(ny, nz), ntp, dt, rh), BF16),
        vmem((max(ny, nz) * ntp, dt, rh), BF16),
        dma((13,)),
        dma(()),
        dma(()),
        dma((4,)),
        dma((4, max(ny, nz))),
        dma((4,)),
        dma((4,)),
        dma(()),
        dma(()),
        dma((2,)),
        dma((2,)),
        dma(()),
        dma(()),
        dma((nkv,)),
        dma((nkv,)),
        dma(()),
        dma(()),
        dma((3,)),
        dma((3,)),
        dma(()),
        dma(()),
        dma((ny,)),
        dma((nz,)),
        dma(()),
        dma(()),
    ]
    in_hbm = pl.BlockSpec(memory_space=pl.ANY)
    in_vmem = pl.BlockSpec(memory_space=pltpu.VMEM)
    mixed_t, new_state = pl.pallas_call(
        functools.partial(layer_kernel, sizes),
        out_shape=(
            pltpu.VMEM((dt, rows), BF16),
            pltpu.VMEM(state.shape, F32),
        ),
        in_specs=[in_hbm] * 15,
        out_specs=(in_vmem, in_hbm),
        scratch_shapes=scratch,
        compiler_params=pltpu.CompilerParams(
            collective_id=0, has_side_effects=True, vmem_limit_bytes=63_500_000
        ),
        name="layer",
    )(
        tokens.T,
        mix_gain[None, :],
        w_query,
        w_key,
        w_value,
        w_gate,
        w_beta.T,
        w_decay.T,
        decay_rate[None, :],
        out_gain[None, :],
        state,
        w_out,
        mlp_gain[None, :],
        w_up,
        w_down,
    )
    mixed_t, new_state = pl.pallas_call(
        store_kernel,
        out_shape=(
            jax.ShapeDtypeStruct((dt, rows), BF16),
            jax.ShapeDtypeStruct(state.shape, F32),
        ),
        in_specs=[in_hbm] * 2,
        out_specs=(in_hbm, in_hbm),
        scratch_shapes=[dma((1 + STORES,))],
        compiler_params=pltpu.CompilerParams(vmem_limit_bytes=1_000_000),
        name="store",
    )(mixed_t, new_state)
    return mixed_t.T, new_state


def solution(mesh):
    n = dict(mesh.shape)
    sizes = (n["kv"] // 4, 4, n["tp"] // 2, 2) if n["kv"] >= 8 else (2, n["kv"] // 2, n["tp"] // 2, 2)
    torus = Mesh(mesh.devices.reshape(sizes), KV_TP)
    in_specs = (
        P(None, KV_TP),
        P(KV),
        P(KV, TP),
        P(KV, TP),
        P(KV, TP),
        P(KV, TP),
        P(KV, None),
        P(KV, None),
        P(TP),
        P(),
        P(KV, TP, None, None),
        P(TP, KV),
        P(),
        P(None, KV_TP),
        P(KV_TP, None),
    )
    out_specs = (P(None, KV_TP), P(KV, TP, None, None))
    return jax.shard_map(
        functools.partial(local, sizes),
        mesh=torus,
        in_specs=in_specs,
        out_specs=out_specs,
        check_vma=False,
    )
```

```python
import functools

import jax
import jax.numpy as jnp
from jax import lax
from jax.experimental import pallas as pl
from jax.experimental.pallas import tpu as pltpu
from jax.sharding import Mesh
from jax.sharding import PartitionSpec as P

EPSILON = 1e-06
MESH = pl.DeviceIdType.MESH
KV_TP = ("kv_0", "kv_1", "tp_0", "tp_1")
KV = ("kv_0", "kv_1")
TP = ("tp_0", "tp_1")
F32 = jnp.float32
BF16 = jnp.bfloat16


def silu(v):
    return v / (1.0 + jnp.exp(-v))


def layer_kernel(
    sizes,
    tok_ref,
    mix_gain_ref,
    wq_ref,
    wk_ref,
    wv_ref,
    wg_ref,
    wbeta_ref,
    wdecay_ref,
    rate_ref,
    out_gain_ref,
    state_ref,
    wout_ref,
    mlp_gain_ref,
    wup_ref,
    wdown_ref,
    mixed_ref,
    new_state_ref,
    col_t,
    w_proj,
    w_rates,
    perm,
    w_beta,
    w_decay,
    mix_gain,
    out_gain,
    mlp_gain,
    rate,
    w_out,
    w_up,
    w_down,
    st,
    col_n,
    send_b,
    recv_b1,
    send_b2,
    recv_b2,
    key_t,
    query_t,
    rows_s,
    mine,
    merged,
    recv_ex,
    res,
    res_t,
    recv_r,
    hid,
    acc_up,
    total_sq,
    send_h,
    recv_h1a,
    recv_h1b,
    send_xa,
    send_xb,
    recv_x,
    bytes_x,
    local_sem,
    a_send,
    a_recv,
    b1_send,
    b1_recv,
    b2_send,
    b2_recv,
    d_send,
    d_recv,
    ex_send,
    ex_recv,
    fa_send,
    fb_send,
    fa_recv,
    fb_recv,
    r_send,
    r_recv,
    swap_send,
    swap_recv,
    h1a_send,
    h1b_send,
    h1a_recv,
    h1b_recv,
    x_send,
    x_recv,
):
    nz, ny, nx, nc = sizes
    nkv, ntp = nz * ny, nx * nc
    z, y = lax.axis_index("kv_0"), lax.axis_index("kv_1")
    x, c = lax.axis_index("tp_0"), lax.axis_index("tp_1")
    kv, tp = z * ny + y, x * nc + c
    partner = {"tp_1": nc - 1 - c}

    dt, rows = tok_ref.shape
    ff = wup_ref.shape[1]
    dk = dt * ntp
    width = dk * nkv
    rb, heads, head = st.shape[0], st.shape[1], st.shape[2]
    proj = heads * head
    rh = rows // nc
    rc = rh // 2
    other = nc - 1 - c

    def kv_dev(k):
        return {"kv_0": k // ny, "kv_1": lax.rem(k, ny)}

    def tp_dev(t):
        return {"tp_0": t // nc, "tp_1": lax.rem(t, nc)}

    def remote(src, dst, send_sem, recv_sem, dev):
        return pltpu.make_async_remote_copy(
            src_ref=src,
            dst_ref=dst,
            send_sem=send_sem,
            recv_sem=recv_sem,
            device_id=dev,
            device_id_type=MESH,
        )

    def all_received(ref, send_sem, recv_sem):
        remote(ref, ref, send_sem, recv_sem, partner).wait_recv()

    def all_sent(ref, send_sem, recv_sem):
        remote(ref, ref, send_sem, recv_sem, partner).wait_send()

    def loop(lo, hi, body):
        def wrapped(i, carry):
            body(i)
            return carry

        lax.fori_loop(lo, hi, wrapped, 0)

    def ring(n):
        return sorted(range(1, n), key=lambda d: (-min(d, n - d), d))

    def block(i, n):
        return pl.ds(pl.multiple_of(i * n, n), n)

    barrier = pltpu.get_barrier_semaphore()

    def greet(dev):
        pl.semaphore_signal(barrier, inc=1, device_id=dev, device_id_type=MESH)

    for dx in range(nx):
        for dc in range(nc):
            if dx or dc:
                greet({"tp_0": lax.rem(x + dx, nx), "tp_1": lax.rem(c + dc, nc)})
    for d in range(1, ny):
        greet({"kv_1": lax.rem(y + d, ny)})
    for d in range(1, nz):
        greet({"kv_0": lax.rem(z + d, nz)})

    own_tok = col_t.at[block(tp, dt), :]
    first = (
        (tok_ref, own_tok),
        (wbeta_ref, w_beta),
        (wdecay_ref, w_decay),
        (mix_gain_ref, mix_gain),
        (rate_ref, rate),
        (out_gain_ref, out_gain),
        (mlp_gain_ref, mlp_gain),
        (state_ref, st),
        (wout_ref, w_out.at[block(c, proj), :]),
        (wup_ref, w_up.at[:, pl.ds(0, ff)]),
        (wdown_ref, w_down.at[pl.ds(0, ff), :]),
    )
    copies = [
        pltpu.make_async_copy(src, dst, local_sem.at[i]) for i, (src, dst) in enumerate(first)
    ]
    for copy in copies[:4]:
        copy.start()
    for i, w in enumerate((wq_ref, wk_ref, wv_ref, wg_ref)):
        pltpu.make_async_copy(w, w_proj.at[i], local_sem.at[11]).start()
    for copy in copies[4:]:
        copy.start()

    n_heads = wbeta_ref.shape[0]
    copies[1].wait()
    copies[2].wait()
    w_rates[...] = jnp.zeros_like(w_rates)
    w_rates[0:n_heads, :] = w_beta[...]
    w_rates[32 : 32 + n_heads, :] = w_decay[...]

    width_x = nx * dt
    column = lax.broadcasted_iota(jnp.int32, (dk, dk), 1)
    source = (lax.rem(column, width_x) // dt * nc + column // width_x) * dt + lax.rem(column, dt)
    row = lax.broadcasted_iota(jnp.int32, (dk, dk), 0)
    perm[...] = jnp.where(row == source, 1.0, 0.0).astype(BF16)

    copies[0].wait()
    copies[3].wait()
    pl.semaphore_wait(barrier, ntp - 1 + ny - 1 + nz - 1)

    def tp_peers():
        near = [(0, 1)] if nc == 2 else []
        return [(dx, dc) for dx in ring(nx) for dc in range(nc)] + near

    def tp_peer(dx, dc):
        return lax.rem(x + dx, nx) * nc + lax.rem(c + dc, nc)

    for dx, dc in tp_peers():
        remote(own_tok, own_tok, a_send, a_recv, tp_dev(tp_peer(dx, dc))).start()

    a_all = col_t.at[pl.ds(0, (ntp - 1) * dt), :]
    all_received(a_all, a_send, a_recv)

    cols = col_t[...].astype(F32).T
    col_n[...] = cols.astype(BF16)
    normed = (cols * mix_gain[...]).astype(BF16)
    squares = jnp.sum(cols * cols, axis=1, keepdims=True)

    pltpu.make_async_copy(w_proj, w_proj, local_sem.at[11]).wait()

    def project(i):
        return jnp.dot(normed, w_proj[i], preferred_element_type=F32).astype(BF16)

    class Reduction:
        def __init__(self, i, column, columns, z_first):
            self.i, self.z_first = i, z_first
            self.n1, self.n2 = (nz, ny) if z_first else (ny, nz)
            self.at = pl.ds(column, columns)
            self.recv1, self.send2, self.recv2 = recv_b1[i], send_b2[i], recv_b2[i]

        def place(self, first, second):
            dz, dy = (first, second) if self.z_first else (second, first)
            return lax.rem(z + dz, nz), lax.rem(y + dy, ny)

        def rows(self, first, second):
            zk, yk = self.place(first, second)
            return send_b.at[block(zk * ny + yk, rb), self.at]

        def start(self):
            for second in [*ring(self.n2), 0]:
                for first in ring(self.n1):
                    zk, yk = self.place(first, second)
                    line, dev = (yk, {"kv_0": zk}) if self.z_first else (zk, {"kv_1": yk})
                    remote(
                        self.rows(first, second),
                        self.recv1.at[line, first - 1],
                        b1_send.at[self.i],
                        b1_recv.at[self.i, line],
                        dev,
                    ).start()

        def first_sum(self, second):
            zk, yk = self.place(0, second)
            line = yk if self.z_first else zk
            acc = self.rows(0, second)[...].astype(F32)
            all_received(self.recv1.at[line], b1_send.at[self.i], b1_recv.at[self.i, line])
            for k in range(self.n1 - 1):
                acc = acc + self.recv1[line, k].astype(F32)
            return acc

        def pass_on(self, second):
            zk, yk = self.place(0, second)
            dev = {"kv_1": yk} if self.z_first else {"kv_0": zk}
            blk = self.send2.at[second - 1]
            blk[...] = self.first_sum(second).astype(BF16)
            remote(
                blk, self.recv2.at[second - 1], b2_send.at[self.i], b2_recv.at[self.i], dev
            ).start()

        def second_sum(self, acc):
            all_received(self.recv2, b2_send.at[self.i], b2_recv.at[self.i])
            for k in range(self.n2 - 1):
                acc = acc + self.recv2[k].astype(F32)
            return acc

        def sent(self):
            all_sent(self.recv1, b1_send.at[self.i], b1_recv.at[self.i, 0])
            all_sent(self.recv2, b2_send.at[self.i], b2_recv.at[self.i])

    q_end, k_end = proj + 128, 2 * proj + 128
    for_query = Reduction(0, 0, q_end, True)
    for_key = Reduction(1, q_end, proj, False)
    for_value = Reduction(2, k_end, proj, True)
    for_gate = Reduction(3, k_end + proj, proj, False)

    send_b[:, q_end:k_end] = project(1)
    for_key.start()
    contract_last = (((1,), (1,)), ((), ()))
    rates_part = lax.dot_general(
        normed, w_rates[...], contract_last, preferred_element_type=F32
    )
    lane = lax.broadcasted_iota(jnp.int32, rates_part.shape, 1)
    rates_part = jnp.where(lane == 63, squares, rates_part)
    high = rates_part.astype(BF16).astype(F32)
    low = pltpu.roll(rates_part - high, 64, 1)
    send_b[:, proj:q_end] = jnp.where(lane < 64, high, low).astype(BF16)
    send_b[:, :proj] = project(0)
    for_query.start()
    send_b[:, k_end : k_end + proj] = project(2)
    for_value.start()
    send_b[:, k_end + proj :] = project(3)
    for_gate.start()

    copies[10].wait()

    def reorder(k):
        at = (pl.ds(0, ff), block(k, dk))
        w_down[at] = jnp.dot(w_down[at], perm[...], preferred_element_type=F32).astype(BF16)

    loop(0, nkv, reorder)

    def pass_on_both(by_z, by_y):
        for i in range(max(ny, nz) - 1):
            if i < nz - 1:
                by_y.pass_on(ring(nz)[i])
            if i < ny - 1:
                by_z.pass_on(ring(ny)[i])
        return by_z.first_sum(0), by_y.first_sum(0)

    query_sum, key_sum = pass_on_both(for_query, for_key)

    value_sum, gate_sum = pass_on_both(for_value, for_gate)

    key_sum = for_key.second_sum(key_sum)
    query_sum = for_query.second_sum(query_sum)

    swaps = [
        remote(
            w_out.at[block(c, proj), :],
            w_out.at[block(c, proj), :],
            swap_send.at[0],
            swap_recv.at[0],
            partner,
        ),
        remote(
            w_up.at[:, pl.ds(0, ff)],
            w_up.at[:, pl.ds(ff, ff)],
            swap_send.at[1],
            swap_recv.at[1],
            partner,
        ),
        remote(
            w_down.at[pl.ds(0, ff), :],
            w_down.at[pl.ds(ff, ff), :],
            swap_send.at[2],
            swap_recv.at[2],
            partner,
        ),
    ]
    copies[8].wait()
    copies[9].wait()
    for swap in swaps:
        swap.start()

    rates = query_sum[:, proj:]
    rates = rates + pltpu.roll(rates, 64, 1)
    lane_b = lax.broadcasted_iota(jnp.int32, rates.shape, 1)

    def pick(i):
        return jnp.sum(jnp.where(lane_b == i, rates, 0.0), axis=1, keepdims=True)

    for i in range(4, 8):
        copies[i].wait()
    row_scale = lax.rsqrt(pick(63) / width + EPSILON)
    repeat = 128 // rb
    group = 8
    for h in range(heads):
        at = slice(h * head, (h + 1) * head)
        beta_raw = pick(tp * heads + h) * row_scale
        decay_raw = pick(32 + tp * heads + h) * row_scale
        beta = 1.0 / (1.0 + jnp.exp(-beta_raw))
        softplus = jnp.maximum(decay_raw, 0.0) + jnp.log1p(jnp.exp(-jnp.abs(decay_raw)))
        decay = jnp.exp(-rate[0:1, h : h + 1] * softplus)
        query = silu(query_sum[:, at] * row_scale)
        query = query * lax.rsqrt(jnp.sum(query * query, axis=1, keepdims=True) + EPSILON)
        query = query * head ** (-0.5)
        key = silu(key_sum[:, at] * row_scale)
        key = key * lax.rsqrt(jnp.sum(key * key, axis=1, keepdims=True) + EPSILON)
        key_tr = jnp.concatenate([key] * repeat, axis=0).T
        query_tr = jnp.concatenate([query] * repeat, axis=0).T
        for g in range(rb // group):
            key_t[g, h] = pltpu.roll(key_tr, (128 - g * group) % 128, 1) if g else key_tr
            query_t[g, h] = pltpu.roll(query_tr, (128 - g * group) % 128, 1) if g else query_tr
        shape = (rb, head)
        rows_s[0, h] = jnp.broadcast_to(decay, shape)
        rows_s[1, h] = jnp.broadcast_to(beta, shape)
        rows_s[2, h] = jnp.broadcast_to(
            jnp.sum(key * query, axis=1, keepdims=True), shape
        )

    def read_group(g):
        for i in range(group):
            b = g * group + i
            for h in range(heads):
                state = st[b, h]
                rows_s[3, h, pl.ds(b, 1), :] = jnp.sum(
                    state * key_t[g, h, :, i : i + 1], axis=0, keepdims=True
                )
                rows_s[4, h, pl.ds(b, 1), :] = jnp.sum(
                    state * query_t[g, h, :, i : i + 1], axis=0, keepdims=True
                )

    loop(0, rb // group, read_group)

    value_sum = for_value.second_sum(value_sum)
    gate_sum = for_gate.second_sum(gate_sum)
    for h in range(heads):
        at = slice(h * head, (h + 1) * head)
        decay = rows_s[0, h]
        value = silu(value_sum[:, at] * row_scale)
        change = rows_s[1, h] * (value - decay * rows_s[3, h])
        read = decay * rows_s[4, h] + rows_s[2, h] * change
        rows_s[3, h] = change
        scale = lax.rsqrt(jnp.sum(read * read, axis=1, keepdims=True) / head + EPSILON)
        gate = silu(gate_sum[:, at] * row_scale)
        mine[:, at] = (read * scale * out_gain[...] * gate).astype(BF16)

    per_half = nkv // nc
    keeper = kv // per_half
    my_rows = block(lax.rem(kv, per_half), rb)
    slot = merged.at[my_rows, block(c, proj)]

    def d_bytes(n):
        return send_b.at[pl.ds(0, n * rb), pl.ds(0, proj)]

    def hops(d):
        dz, dy = d // ny, d % ny
        return min(dz, nz - dz) + min(dy, ny - dy)

    def kv_peer(d):
        return lax.rem(z + d // ny, nz) * ny + lax.rem(y + d % ny, ny)

    for d in sorted(range(1, nkv), key=lambda d: -hops(d)):
        dev = {**kv_dev(kv_peer(d)), "tp_1": keeper}
        remote(mine, slot, d_send, d_recv, dev).start()

    @pl.when(keeper != c)
    def _():
        remote(mine, slot, d_send, d_recv, {"tp_1": keeper}).start()

    @pl.when(keeper == c)
    def _():
        merged[my_rows, block(c, proj)] = mine[...]

    def write_group(g):
        for i in range(group):
            b = g * group + i
            for h in range(heads):
                st[b, h] = (
                    rows_s[0, h, pl.ds(b, 1), :] * st[b, h]
                    + key_t[g, h, :, i : i + 1] * rows_s[3, h, pl.ds(b, 1), :]
                )

    loop(0, rb // group, write_group)
    state_out = pltpu.make_async_copy(st, new_state_ref, local_sem.at[12])
    state_out.start()
    all_sent(a_all, a_send, a_recv)
    for reduction in (for_query, for_key, for_value, for_gate):
        reduction.sent()

    @pl.when(keeper == c)
    def _():
        all_received(d_bytes(nkv - 1), d_send, d_recv)

    @pl.when(keeper != c)
    def _():
        all_received(d_bytes(nkv), d_send, d_recv)

    swaps[0].wait_recv()

    def ex_copy(half, dev):
        blk = recv_ex.at[x, pl.ds(half * rc, rc), :]
        return remote(blk, blk, ex_send.at[half], ex_recv.at[half], dev)

    def ex_all(half):
        return recv_ex.at[pl.ds(0, nx - 1), pl.ds(half * rc, rc), :]

    for half in range(2):
        at = slice(half * rc, (half + 1) * rc)
        part = jnp.dot(merged[at, :], w_out[...], preferred_element_type=F32)
        recv_ex[x, at] = part.astype(BF16)
        for d in ring(nx):
            ex_copy(half, {"tp_0": lax.rem(x + d, nx)}).start()

    def residual(half):
        all_received(ex_all(half), ex_send.at[half], ex_recv.at[half])
        at = slice(half * rc, (half + 1) * rc)
        branch = recv_ex[0, at].astype(F32)
        for i in range(1, nx):
            branch = branch + recv_ex[i, at].astype(F32)
        tok = col_n[pl.ds(pl.multiple_of(c * rh + half * rc, rc), rc), :]
        res[kv, at] = (tok.astype(F32) + branch).astype(BF16)

    rows_a, rows_b = pl.ds(0, rc), pl.ds(rc, rc)

    y_arrival, z_arrival = [0, *ring(ny)[::-1]], [0, *ring(nz)[::-1]]
    y_last, z_last = y_arrival[-1], z_arrival[-1]

    def fa_copy(k, sem, dev):
        blk = res.at[k, rows_a, :]
        return remote(blk, blk, fa_send, fa_recv.at[sem], dev)

    def fb_copy(k, sem, dev):
        blk = res.at[k, rows_b, :]
        return remote(blk, blk, fb_send, fb_recv.at[sem], dev)

    def near_a(d):
        return d - 1

    def near_b(d):
        return d - 1

    def late_a(dy, dz):
        return ny - 1 + (ny - 1 + dz if dy == y_last else y_arrival.index(dy))

    def late_b(dz, dy):
        return nz - 1 + (nz - 1 + dy if dz == z_last else z_arrival.index(dz))

    def home(dz, dy):
        return lax.rem(z + nz - dz, nz) * ny + lax.rem(y + ny - dy, ny)

    def y_dev(d):
        return {"kv_1": lax.rem(y + d, ny)}

    def z_dev(d):
        return {"kv_0": lax.rem(z + d, nz)}

    residual(0)
    for d in ring(ny):
        fa_copy(kv, near_a(d), y_dev(d)).start()
    for d in ring(nz):
        fa_copy(kv, late_a(0, d), z_dev(d)).start()
    residual(1)
    for d in ring(nz):
        fb_copy(kv, near_b(d), z_dev(d)).start()
    for d in ring(ny):
        fb_copy(kv, late_b(0, d), y_dev(d)).start()

    res_t[...] = res[kv].astype(F32).T.astype(BF16)
    r_copy = remote(
        res_t.at[block(x * nc + other, dt), :], recv_r, r_send, r_recv, partner
    )
    r_copy.start()

    def up(*blocks):
        total, acc = total_sq[...], acc_up[...]
        for dz, dy in blocks:
            k = home(dz, dy)
            at = block(k, dk)
            blk = res[k].astype(F32)
            sq = blk * blk
            for i in range(dk // 128):
                total = total + sq[:, i * 128 : (i + 1) * 128]
            acc = acc + jnp.dot(
                (blk * mlp_gain[:, at]).astype(BF16), w_up[at, :], preferred_element_type=F32
            )
        total_sq[...], acc_up[...] = total, acc

    acc_up[...] = jnp.zeros_like(acc_up)
    total_sq[...] = jnp.zeros_like(total_sq)
    for swap in swaps[1:]:
        swap.wait_recv()
    up((0, 0))

    @pl.when(keeper == c)
    def _():
        all_sent(d_bytes(nkv - 1), d_send, d_recv)

    @pl.when(keeper != c)
    def _():
        all_sent(d_bytes(nkv), d_send, d_recv)

    for half in range(2):
        all_sent(ex_all(half), ex_send.at[half], ex_recv.at[half])

    for i in range(1, max(ny, nz)):
        if i < ny:
            dy = y_arrival[i]
            fa_copy(home(0, dy), near_a(dy), partner).wait_recv()
            for d in ring(nz):
                fa_copy(home(0, dy), late_a(dy, d), z_dev(d)).start()
        if i < nz:
            dz = z_arrival[i]
            fb_copy(home(dz, 0), near_b(dz), partner).wait_recv()
            for d in ring(ny):
                fb_copy(home(dz, 0), late_b(dz, d), y_dev(d)).start()

    got_a = {(0, dy) for dy in range(ny)}
    got_b = {(dz, 0) for dz in range(nz)}
    done = {(0, 0)}

    def up_ready():
        ready = sorted((got_a & got_b) - done)
        done.update(ready)
        for i in range(0, len(ready), 2):
            up(*ready[i : i + 2])

    for i in range(max(ny, nz)):
        if i < ny - 1:
            dy = y_arrival[i]
            all_received(
                res.at[pl.ds(0, nz - 1), rows_a, :], fa_send, fa_recv.at[late_a(dy, 1)]
            )
            got_a |= {(dz, dy) for dz in range(1, nz)}
        if i < nz - 1:
            dz = z_arrival[i]
            all_received(
                res.at[pl.ds(0, ny - 1), rows_b, :], fb_send, fb_recv.at[late_b(dz, 1)]
            )
            got_b |= {(dz, dy) for dy in range(1, ny)}
        up_ready()
    for i in range(1, max(ny, nz)):
        if i < nz:
            dz = z_arrival[i]
            fa_copy(home(dz, y_last), late_a(y_last, dz), partner).wait_recv()
            got_a.add((dz, y_last))
        if i < ny:
            dy = y_arrival[i]
            fb_copy(home(z_last, dy), late_b(z_last, dy), partner).wait_recv()
            got_b.add((z_last, dy))
        up_ready()

    scale = lax.rsqrt(jnp.sum(total_sq[...], axis=1, keepdims=True) / width + EPSILON)
    relu = jnp.maximum(acc_up[...] * scale, 0.0)
    hid[...] = (relu * relu).astype(BF16)

    hw = dk // 2
    part_a, part_b = pl.ds(0, hw), pl.ds(hw, hw)

    def h1a_copy(dz, k):
        return remote(
            send_h.at[k, :, part_a],
            recv_h1a.at[lax.rem(k, ny), dz - 1],
            h1a_send,
            h1a_recv.at[lax.rem(k, ny)],
            {"kv_0": k // ny},
        )

    def h1b_copy(dy, k):
        return remote(
            send_h.at[k, :, part_b],
            recv_h1b.at[k // ny, dy - 1],
            h1b_send,
            h1b_recv.at[k // ny],
            {"kv_1": lax.rem(k, ny)},
        )

    def down(dz, dy):
        zk, yk = lax.rem(z + dz, nz), lax.rem(y + dy, ny)
        k = zk * ny + yk
        out = jnp.dot(hid[...], w_down[:, block(k, dk)], preferred_element_type=F32)
        send_h[k] = out.astype(BF16)
        if dz:
            h1a_copy(dz, k).start()
        if dy:
            h1b_copy(dy, k).start()

    z_order, y_order = [*ring(nz), 0], [*ring(ny), 0]
    for s in range(max(nz, ny)):
        shell = [(i, s) for i in range(s, nz)] + [(s, i) for i in range(s + 1, ny)]
        for i, j in shell:
            if i < nz and j < ny:
                down(z_order[i], y_order[j])
    all_sent(res.at[pl.ds(0, nkv - 1), rows_a, :], fa_send, fa_recv.at[0])
    all_sent(res.at[pl.ds(0, nkv - 1), rows_b, :], fb_send, fb_recv.at[0])
    for swap in swaps:
        swap.wait_send()
    r_copy.wait_send()

    def h1a_sum(yk):
        acc = send_h[z * ny + yk, :, 0:hw].astype(F32)
        all_received(recv_h1a.at[yk], h1a_send, h1a_recv.at[yk])
        for i in range(nz - 1):
            acc = acc + recv_h1a[yk, i].astype(F32)
        return acc

    def h1b_sum(zk):
        acc = send_h[zk * ny + y, :, hw : 2 * hw].astype(F32)
        all_received(recv_h1b.at[zk], h1b_send, h1b_recv.at[zk])
        for i in range(ny - 1):
            acc = acc + recv_h1b[zk, i].astype(F32)
        return acc

    def deliver(d, core):
        if core:
            total, line, buf = h1b_sum(lax.rem(z + d, nz)), z, send_xb.at[d]
            dev = {"kv_0": lax.rem(z + d, nz), "tp_1": core}
        else:
            total, line, buf = h1a_sum(lax.rem(y + d, ny)), y, send_xa.at[d]
            dev = {"kv_1": lax.rem(y + d, ny), "tp_1": core}
        buf[...] = total.T.astype(BF16)
        for dx in [*ring(nx), 0]:
            to_x = lax.rem(x + dx, nx)
            at = block(to_x, dt)

            def send(at=at, to_x=to_x):
                to = {**dev, "tp_0": to_x}
                remote(buf.at[at], recv_x.at[line, tp], x_send, x_recv, to).start()

            if d or dx:
                send()
            else:

                @pl.when(c != core)
                def _():
                    send()

                @pl.when(c == core)
                def _():
                    recv_x[line, tp] = buf[at]

    for i in range(max(ny, nz)):
        if i < ny:
            deliver([*ring(ny), 0][i], 0)
        if i < nz:
            deliver([*ring(nz), 0][i], 1)

    def finish(lines):
        all_received(bytes_x.at[pl.ds(0, lines * ntp - 1)], x_send, x_recv)
        for core, residual in ((c, res_t[block(tp, dt), :]), (other, recv_r[...])):
            total = residual.astype(F32)
            for i in range(lines):
                for xx in range(nx):
                    total = total + recv_x[i, xx * nc + core].astype(F32)
            mixed_ref[:, block(core, rh)] = total.astype(BF16)

    r_copy.wait_recv()

    @pl.when(c == 0)
    def _():
        finish(ny)

    @pl.when(c == 1)
    def _():
        finish(nz)

    all_sent(bytes_x.at[pl.ds(0, (ny + nz) * nx - 1)], x_send, x_recv)
    all_sent(recv_h1a, h1a_send, h1a_recv.at[0])
    all_sent(recv_h1b, h1b_send, h1b_recv.at[0])
    state_out.wait()


STORES = 8


def store_kernel(mixed_ref, state_ref, mixed_out, state_out, sem):
    n = state_ref.shape[0] // STORES
    copies = [pltpu.make_async_copy(mixed_ref, mixed_out, sem.at[0])]
    for i in range(STORES):
        at = pl.ds(i * n, n)
        copies.append(pltpu.make_async_copy(state_ref.at[at], state_out.at[at], sem.at[1 + i]))
    for copy in copies:
        copy.start()
    for copy in copies:
        copy.wait()


def local(
    sizes,
    tokens,
    mix_gain,
    w_query,
    w_key,
    w_value,
    w_gate,
    w_beta,
    w_decay,
    decay_rate,
    out_gain,
    state,
    w_out,
    mlp_gain,
    w_up,
    w_down,
):
    nz, ny, nx, nc = sizes
    nkv, ntp = nz * ny, nx * nc
    rows, dt = tokens.shape
    dk = dt * ntp
    rb, heads, head, _ = state.shape
    proj = heads * head
    sent = 4 * proj + 128
    reductions = ((proj + 128, True), (proj, False), (proj, True), (proj, False))
    first = [(ny, nz) if by_z else (nz, ny) for _, by_z in reductions]
    widths = [w for w, _ in reductions]
    n_heads = w_beta.shape[1]
    ff = w_up.shape[1]
    rh = rows // nc
    rc = rh // 2
    vmem, dma = pltpu.VMEM, pltpu.SemaphoreType.DMA
    scratch = [
        vmem((dk, rows), BF16),
        vmem((4, dk, proj), BF16),
        vmem((128, dk), BF16),
        vmem((dk, dk), BF16),
        vmem((n_heads, dk), BF16),
        vmem((n_heads, dk), BF16),
        vmem((1, dk), F32),
        vmem((1, head), F32),
        vmem((1, dk * nkv), F32),
        vmem((1, heads), F32),
        vmem((nc * proj, dk), BF16),
        vmem((w_up.shape[0], 2 * ff), BF16),
        vmem((2 * ff, w_down.shape[1]), BF16),
        vmem(state.shape, F32),
        vmem((rows, dk), BF16),
        vmem((rows, sent), BF16),
        [vmem((n2, n1 - 1, rb, w), BF16) for (n2, n1), w in zip(first, widths)],
        [vmem((n2 - 1, rb, w), BF16) for (n2, n1), w in zip(first, widths)],
        [vmem((n2 - 1, rb, w), BF16) for (n2, n1), w in zip(first, widths)],
        vmem((rb // 8, heads, head, 128), F32),
        vmem((rb // 8, heads, head, 128), F32),
        vmem((5, heads, rb, head), F32),
        vmem((rb, proj), BF16),
        vmem((rh, nc * proj), BF16),
        vmem((nx, rh, dk), BF16),
        vmem((nkv, rh, dk), BF16),
        vmem((dk, rh), BF16),
        vmem((dt, rh), BF16),
        vmem((rh, 2 * ff), BF16),
        vmem((rh, 2 * ff), F32),
        vmem((rh, 128), F32),
        vmem((nkv, rh, dk), BF16),
        vmem((ny, nz - 1, rh, dk // 2), BF16),
        vmem((nz, ny - 1, rh, dk // 2), BF16),
        vmem((ny, dk // 2, rh), BF16),
        vmem((nz, dk // 2, rh), BF16),
        vmem((max(ny, nz), ntp, dt, rh), BF16),
        vmem((max(ny, nz) * ntp, dt, rh), BF16),
        dma((13,)),
        dma(()),
        dma(()),
        dma((4,)),
        dma((4, max(ny, nz))),
        dma((4,)),
        dma((4,)),
        dma(()),
        dma(()),
        dma((2,)),
        dma((2,)),
        dma(()),
        dma(()),
        dma((2 * (ny - 1) + nz,)),
        dma((2 * (nz - 1) + ny,)),
        dma(()),
        dma(()),
        dma((3,)),
        dma((3,)),
        dma(()),
        dma(()),
        dma((ny,)),
        dma((nz,)),
        dma(()),
        dma(()),
    ]
    in_hbm = pl.BlockSpec(memory_space=pl.ANY)
    in_vmem = pl.BlockSpec(memory_space=pltpu.VMEM)
    mixed_t, new_state = pl.pallas_call(
        functools.partial(layer_kernel, sizes),
        out_shape=(
            pltpu.VMEM((dt, rows), BF16),
            pltpu.VMEM(state.shape, F32),
        ),
        in_specs=[in_hbm] * 15,
        out_specs=(in_vmem, in_hbm),
        scratch_shapes=scratch,
        compiler_params=pltpu.CompilerParams(
            collective_id=0, has_side_effects=True, vmem_limit_bytes=63_500_000
        ),
        name="layer",
    )(
        tokens.T,
        mix_gain[None, :],
        w_query,
        w_key,
        w_value,
        w_gate,
        w_beta.T,
        w_decay.T,
        decay_rate[None, :],
        out_gain[None, :],
        state,
        w_out,
        mlp_gain[None, :],
        w_up,
        w_down,
    )
    mixed_t, new_state = pl.pallas_call(
        store_kernel,
        out_shape=(
            jax.ShapeDtypeStruct((dt, rows), BF16),
            jax.ShapeDtypeStruct(state.shape, F32),
        ),
        in_specs=[in_hbm] * 2,
        out_specs=(in_hbm, in_hbm),
        scratch_shapes=[dma((1 + STORES,))],
        compiler_params=pltpu.CompilerParams(vmem_limit_bytes=1_000_000),
        name="store",
    )(mixed_t, new_state)
    return mixed_t.T, new_state


def solution(mesh):
    n = dict(mesh.shape)
    sizes = (n["kv"] // 4, 4, n["tp"] // 2, 2) if n["kv"] >= 8 else (2, n["kv"] // 2, n["tp"] // 2, 2)
    torus = Mesh(mesh.devices.reshape(sizes), KV_TP)
    in_specs = (
        P(None, KV_TP),
        P(KV),
        P(KV, TP),
        P(KV, TP),
        P(KV, TP),
        P(KV, TP),
        P(KV, None),
        P(KV, None),
        P(TP),
        P(),
        P(KV, TP, None, None),
        P(TP, KV),
        P(),
        P(None, KV_TP),
        P(KV_TP, None),
    )
    out_specs = (P(None, KV_TP), P(KV, TP, None, None))
    return jax.shard_map(
        functools.partial(local, sizes),
        mesh=torus,
        in_specs=in_specs,
        out_specs=out_specs,
        check_vma=False,
    )
```

```python
import functools

import jax
import jax.numpy as jnp
from jax import lax
from jax.experimental import pallas as pl
from jax.experimental.pallas import tpu as pltpu
from jax.sharding import Mesh
from jax.sharding import PartitionSpec as P

EPSILON = 1e-06
MESH = pl.DeviceIdType.MESH
KV_TP = ("kv_0", "kv_1", "tp_0", "tp_1")
KV = ("kv_0", "kv_1")
TP = ("tp_0", "tp_1")
F32 = jnp.float32
BF16 = jnp.bfloat16


def silu(v):
    return v / (1.0 + jnp.exp(-v))


def layer_kernel(
    sizes,
    tok_ref,
    mix_gain_ref,
    wq_ref,
    wk_ref,
    wv_ref,
    wg_ref,
    wbeta_ref,
    wdecay_ref,
    rate_ref,
    out_gain_ref,
    state_ref,
    wout_ref,
    mlp_gain_ref,
    wup_ref,
    wdown_ref,
    mixed_ref,
    new_state_ref,
    col_t,
    w_proj,
    w_rates,
    perm,
    w_beta,
    w_decay,
    mix_gain,
    out_gain,
    mlp_gain,
    rate,
    w_out,
    w_up,
    w_down,
    st,
    col_n,
    send_b,
    recv_b1,
    send_b2,
    recv_b2,
    key_t,
    key_s,
    lhs_s,
    st_terms,
    rows_s,
    mine,
    merged,
    recv_ex,
    res,
    res_t,
    recv_r,
    hid,
    acc_up,
    total_sq,
    send_h,
    recv_h1a,
    recv_h1b,
    send_xa,
    send_xb,
    recv_x,
    bytes_x,
    local_sem,
    a_send,
    a_recv,
    b1_send,
    b1_recv,
    b2_send,
    b2_recv,
    d_send,
    d_recv,
    ex_send,
    ex_recv,
    fa_send,
    fb_send,
    fa_recv,
    fb_recv,
    r_send,
    r_recv,
    swap_send,
    swap_recv,
    h1a_send,
    h1b_send,
    h1a_recv,
    h1b_recv,
    x_send,
    x_recv,
):
    nz, ny, nx, nc = sizes
    nkv, ntp = nz * ny, nx * nc
    z, y = lax.axis_index("kv_0"), lax.axis_index("kv_1")
    x, c = lax.axis_index("tp_0"), lax.axis_index("tp_1")
    kv, tp = z * ny + y, x * nc + c
    partner = {"tp_1": nc - 1 - c}

    dt, rows = tok_ref.shape
    ff = wup_ref.shape[1]
    dk = dt * ntp
    width = dk * nkv
    rb, heads, head = st.shape[0], st.shape[1], st.shape[2]
    proj = heads * head
    rh = rows // nc
    rc = rh // 2
    other = nc - 1 - c

    def kv_dev(k):
        return {"kv_0": k // ny, "kv_1": lax.rem(k, ny)}

    def tp_dev(t):
        return {"tp_0": t // nc, "tp_1": lax.rem(t, nc)}

    def remote(src, dst, send_sem, recv_sem, dev):
        return pltpu.make_async_remote_copy(
            src_ref=src,
            dst_ref=dst,
            send_sem=send_sem,
            recv_sem=recv_sem,
            device_id=dev,
            device_id_type=MESH,
        )

    def all_received(ref, send_sem, recv_sem):
        remote(ref, ref, send_sem, recv_sem, partner).wait_recv()

    def all_sent(ref, send_sem, recv_sem):
        remote(ref, ref, send_sem, recv_sem, partner).wait_send()

    def loop(lo, hi, body):
        def wrapped(i, carry):
            body(i)
            return carry

        lax.fori_loop(lo, hi, wrapped, 0)

    def ring(n):
        return sorted(range(1, n), key=lambda d: (-min(d, n - d), d))

    def block(i, n):
        return pl.ds(pl.multiple_of(i * n, n), n)

    barrier = pltpu.get_barrier_semaphore()

    def greet(dev):
        pl.semaphore_signal(barrier, inc=1, device_id=dev, device_id_type=MESH)

    for dx in range(nx):
        for dc in range(nc):
            if dx or dc:
                greet({"tp_0": lax.rem(x + dx, nx), "tp_1": lax.rem(c + dc, nc)})
    for d in range(1, ny):
        greet({"kv_1": lax.rem(y + d, ny)})
    for d in range(1, nz):
        greet({"kv_0": lax.rem(z + d, nz)})

    own_tok = col_t.at[block(tp, dt), :]
    first = (
        (tok_ref, own_tok),
        (wbeta_ref, w_beta),
        (wdecay_ref, w_decay),
        (mix_gain_ref, mix_gain),
        (rate_ref, rate),
        (out_gain_ref, out_gain),
        (mlp_gain_ref, mlp_gain),
        (state_ref, st),
        (wout_ref, w_out.at[block(c, proj), :]),
        (wup_ref, w_up.at[:, pl.ds(0, ff)]),
        (wdown_ref, w_down.at[pl.ds(0, ff), :]),
    )
    copies = [
        pltpu.make_async_copy(src, dst, local_sem.at[i]) for i, (src, dst) in enumerate(first)
    ]
    for copy in copies[:4]:
        copy.start()
    for i, w in enumerate((wq_ref, wk_ref, wv_ref, wg_ref)):
        pltpu.make_async_copy(w, w_proj.at[i], local_sem.at[11]).start()
    for copy in copies[4:]:
        copy.start()

    n_heads = wbeta_ref.shape[0]
    copies[1].wait()
    copies[2].wait()
    w_rates[...] = jnp.zeros_like(w_rates)
    w_rates[0:n_heads, :] = w_beta[...]
    w_rates[32 : 32 + n_heads, :] = w_decay[...]

    width_x = nx * dt
    column = lax.broadcasted_iota(jnp.int32, (dk, dk), 1)
    source = (lax.rem(column, width_x) // dt * nc + column // width_x) * dt + lax.rem(column, dt)
    row = lax.broadcasted_iota(jnp.int32, (dk, dk), 0)
    perm[...] = jnp.where(row == source, 1.0, 0.0).astype(BF16)

    copies[0].wait()
    copies[3].wait()
    pl.semaphore_wait(barrier, ntp - 1 + ny - 1 + nz - 1)

    def tp_peers():
        near = [(0, 1)] if nc == 2 else []
        return [(dx, dc) for dx in ring(nx) for dc in range(nc)] + near

    def tp_peer(dx, dc):
        return lax.rem(x + dx, nx) * nc + lax.rem(c + dc, nc)

    for dx, dc in tp_peers():
        remote(own_tok, own_tok, a_send, a_recv, tp_dev(tp_peer(dx, dc))).start()

    a_all = col_t.at[pl.ds(0, (ntp - 1) * dt), :]
    all_received(a_all, a_send, a_recv)

    cols = col_t[...].astype(F32).T
    col_n[...] = cols.astype(BF16)
    normed = (cols * mix_gain[...]).astype(BF16)
    squares = jnp.sum(cols * cols, axis=1, keepdims=True)

    pltpu.make_async_copy(w_proj, w_proj, local_sem.at[11]).wait()

    def project(i):
        return jnp.dot(normed, w_proj[i], preferred_element_type=F32).astype(BF16)

    class Reduction:
        def __init__(self, i, column, columns, z_first):
            self.i, self.z_first = i, z_first
            self.n1, self.n2 = (nz, ny) if z_first else (ny, nz)
            self.at = pl.ds(column, columns)
            self.recv1, self.send2, self.recv2 = recv_b1[i], send_b2[i], recv_b2[i]

        def place(self, first, second):
            dz, dy = (first, second) if self.z_first else (second, first)
            return lax.rem(z + dz, nz), lax.rem(y + dy, ny)

        def rows(self, first, second):
            zk, yk = self.place(first, second)
            return send_b.at[block(zk * ny + yk, rb), self.at]

        def start(self):
            for second in [*ring(self.n2), 0]:
                for first in ring(self.n1):
                    zk, yk = self.place(first, second)
                    line, dev = (yk, {"kv_0": zk}) if self.z_first else (zk, {"kv_1": yk})
                    remote(
                        self.rows(first, second),
                        self.recv1.at[line, first - 1],
                        b1_send.at[self.i],
                        b1_recv.at[self.i, line],
                        dev,
                    ).start()

        def first_sum(self, second):
            zk, yk = self.place(0, second)
            line = yk if self.z_first else zk
            acc = self.rows(0, second)[...].astype(F32)
            all_received(self.recv1.at[line], b1_send.at[self.i], b1_recv.at[self.i, line])
            for k in range(self.n1 - 1):
                acc = acc + self.recv1[line, k].astype(F32)
            return acc

        def pass_on(self, second):
            zk, yk = self.place(0, second)
            dev = {"kv_1": yk} if self.z_first else {"kv_0": zk}
            blk = self.send2.at[second - 1]
            blk[...] = self.first_sum(second).astype(BF16)
            remote(
                blk, self.recv2.at[second - 1], b2_send.at[self.i], b2_recv.at[self.i], dev
            ).start()

        def second_sum(self, acc):
            all_received(self.recv2, b2_send.at[self.i], b2_recv.at[self.i])
            for k in range(self.n2 - 1):
                acc = acc + self.recv2[k].astype(F32)
            return acc

        def sent(self):
            all_sent(self.recv1, b1_send.at[self.i], b1_recv.at[self.i, 0])
            all_sent(self.recv2, b2_send.at[self.i], b2_recv.at[self.i])

    q_end, k_end = proj + 128, 2 * proj + 128
    for_query = Reduction(0, 0, q_end, True)
    for_key = Reduction(1, q_end, proj, False)
    for_value = Reduction(2, k_end, proj, True)
    for_gate = Reduction(3, k_end + proj, proj, False)

    send_b[:, q_end:k_end] = project(1)
    for_key.start()
    contract_last = (((1,), (1,)), ((), ()))
    rates_part = lax.dot_general(
        normed, w_rates[...], contract_last, preferred_element_type=F32
    )
    lane = lax.broadcasted_iota(jnp.int32, rates_part.shape, 1)
    rates_part = jnp.where(lane == 63, squares, rates_part)
    high = rates_part.astype(BF16).astype(F32)
    low = pltpu.roll(rates_part - high, 64, 1)
    send_b[:, proj:q_end] = jnp.where(lane < 64, high, low).astype(BF16)
    send_b[:, :proj] = project(0)
    for_query.start()
    send_b[:, k_end : k_end + proj] = project(2)
    for_value.start()
    send_b[:, k_end + proj :] = project(3)
    for_gate.start()

    copies[10].wait()

    def reorder(k):
        at = (pl.ds(0, ff), block(k, dk))
        w_down[at] = jnp.dot(w_down[at], perm[...], preferred_element_type=F32).astype(BF16)

    loop(0, nkv, reorder)

    copies[7].wait()

    def split(x):
        high = x.astype(BF16)
        return high, (x - high.astype(F32)).astype(BF16)

    def split_state(g):
        for h in range(heads):
            for i in range(2):
                high, low = split(st[2 * g + i, h])
                at = slice(i * head, (i + 1) * head)
                st_terms[g, h, :head, at] = high
                st_terms[g, h, head:, at] = low

    loop(0, rb // 2, split_state)

    def pass_on_both(by_z, by_y):
        for i in range(max(ny, nz) - 1):
            if i < nz - 1:
                by_y.pass_on(ring(nz)[i])
            if i < ny - 1:
                by_z.pass_on(ring(ny)[i])
        return by_z.first_sum(0), by_y.first_sum(0)

    query_sum, key_sum = pass_on_both(for_query, for_key)

    value_sum, gate_sum = pass_on_both(for_value, for_gate)

    key_sum = for_key.second_sum(key_sum)
    query_sum = for_query.second_sum(query_sum)

    swaps = [
        remote(
            w_out.at[block(c, proj), :],
            w_out.at[block(c, proj), :],
            swap_send.at[0],
            swap_recv.at[0],
            partner,
        ),
        remote(
            w_up.at[:, pl.ds(0, ff)],
            w_up.at[:, pl.ds(ff, ff)],
            swap_send.at[1],
            swap_recv.at[1],
            partner,
        ),
        remote(
            w_down.at[pl.ds(0, ff), :],
            w_down.at[pl.ds(ff, ff), :],
            swap_send.at[2],
            swap_recv.at[2],
            partner,
        ),
    ]
    copies[8].wait()
    copies[9].wait()
    for swap in swaps:
        swap.start()

    rates = query_sum[:, proj:]
    rates = rates + pltpu.roll(rates, 64, 1)
    lane_b = lax.broadcasted_iota(jnp.int32, rates.shape, 1)

    def pick(i):
        return jnp.sum(jnp.where(lane_b == i, rates, 0.0), axis=1, keepdims=True)

    for i in range(4, 7):
        copies[i].wait()
    row_scale = lax.rsqrt(pick(63) / width + EPSILON)
    for h in range(heads):
        at = slice(h * head, (h + 1) * head)
        beta_raw = pick(tp * heads + h) * row_scale
        decay_raw = pick(32 + tp * heads + h) * row_scale
        beta = 1.0 / (1.0 + jnp.exp(-beta_raw))
        softplus = jnp.maximum(decay_raw, 0.0) + jnp.log1p(jnp.exp(-jnp.abs(decay_raw)))
        decay = jnp.exp(-rate[0:1, h : h + 1] * softplus)
        query = silu(query_sum[:, at] * row_scale)
        query = query * lax.rsqrt(jnp.sum(query * query, axis=1, keepdims=True) + EPSILON)
        query = query * head ** (-0.5)
        key = silu(key_sum[:, at] * row_scale)
        key = key * lax.rsqrt(jnp.sum(key * key, axis=1, keepdims=True) + EPSILON)
        key_s[h] = key
        terms = jnp.concatenate([*split(key), *split(query)], axis=0)
        lhs_s[h] = jnp.concatenate([terms, terms], axis=1)
        shape = (rb, head)
        rows_s[0, h] = jnp.broadcast_to(decay, shape)
        rows_s[1, h] = jnp.broadcast_to(beta, shape)
        rows_s[2, h] = jnp.broadcast_to(
            jnp.sum(key * query, axis=1, keepdims=True), shape
        )

    row = lax.broadcasted_iota(jnp.int32, (rb, head), 0)

    def read_pair(g, sums):
        out = []
        for h in range(heads):
            got = jnp.dot(lhs_s[h], st_terms[g, h], preferred_element_type=F32)
            for k in range(2):
                both = got[2 * k * rb : (2 * k + 1) * rb] + got[(2 * k + 1) * rb : (2 * k + 2) * rb]
                acc = sums[2 * h + k]
                for i in range(2):
                    acc = jnp.where(row == 2 * g + i, both[:, i * head : (i + 1) * head], acc)
                out.append(acc)
        return out

    def read_pairs(g, sums):
        for i in range(2):
            sums = read_pair(2 * g + i, sums)
        return sums

    zero = jnp.zeros((rb, head), F32)
    read_sums = lax.fori_loop(0, rb // 4, read_pairs, [zero] * (2 * heads))

    value_sum = for_value.second_sum(value_sum)
    gate_sum = for_gate.second_sum(gate_sum)
    for h in range(heads):
        at = slice(h * head, (h + 1) * head)
        decay = rows_s[0, h]
        value = silu(value_sum[:, at] * row_scale)
        change = rows_s[1, h] * (value - decay * read_sums[2 * h])
        read = decay * read_sums[2 * h + 1] + rows_s[2, h] * change
        rows_s[3, h] = change
        scale = lax.rsqrt(jnp.sum(read * read, axis=1, keepdims=True) / head + EPSILON)
        gate = silu(gate_sum[:, at] * row_scale)
        mine[:, at] = (read * scale * out_gain[...] * gate).astype(BF16)

    per_half = nkv // nc
    keeper = kv // per_half
    my_rows = block(lax.rem(kv, per_half), rb)
    slot = merged.at[my_rows, block(c, proj)]

    def d_bytes(n):
        return send_b.at[pl.ds(0, n * rb), pl.ds(0, proj)]

    def hops(d):
        dz, dy = d // ny, d % ny
        return min(dz, nz - dz) + min(dy, ny - dy)

    def kv_peer(d):
        return lax.rem(z + d // ny, nz) * ny + lax.rem(y + d % ny, ny)

    for d in sorted(range(1, nkv), key=lambda d: -hops(d)):
        dev = {**kv_dev(kv_peer(d)), "tp_1": keeper}
        remote(mine, slot, d_send, d_recv, dev).start()

    @pl.when(keeper != c)
    def _():
        remote(mine, slot, d_send, d_recv, {"tp_1": keeper}).start()

    @pl.when(keeper == c)
    def _():
        merged[my_rows, block(c, proj)] = mine[...]

    group, repeat = 8, 128 // rb
    for h in range(heads):
        key_tr = jnp.concatenate([key_s[h]] * repeat, axis=0).T
        for g in range(rb // group):
            key_t[g, h] = pltpu.roll(key_tr, (128 - g * group) % 128, 1) if g else key_tr

    def write_group(g):
        for i in range(group):
            b = g * group + i
            for h in range(heads):
                st[b, h] = (
                    rows_s[0, h, pl.ds(b, 1), :] * st[b, h]
                    + key_t[g, h, :, i : i + 1] * rows_s[3, h, pl.ds(b, 1), :]
                )

    loop(0, rb // group, write_group)
    state_out = pltpu.make_async_copy(st, new_state_ref, local_sem.at[12])
    state_out.start()
    all_sent(a_all, a_send, a_recv)
    for reduction in (for_query, for_key, for_value, for_gate):
        reduction.sent()

    @pl.when(keeper == c)
    def _():
        all_received(d_bytes(nkv - 1), d_send, d_recv)

    @pl.when(keeper != c)
    def _():
        all_received(d_bytes(nkv), d_send, d_recv)

    swaps[0].wait_recv()

    def ex_copy(half, dev):
        blk = recv_ex.at[x, pl.ds(half * rc, rc), :]
        return remote(blk, blk, ex_send.at[half], ex_recv.at[half], dev)

    def ex_all(half):
        return recv_ex.at[pl.ds(0, nx - 1), pl.ds(half * rc, rc), :]

    for half in range(2):
        at = slice(half * rc, (half + 1) * rc)
        part = jnp.dot(merged[at, :], w_out[...], preferred_element_type=F32)
        recv_ex[x, at] = part.astype(BF16)
        for d in ring(nx):
            ex_copy(half, {"tp_0": lax.rem(x + d, nx)}).start()

    def residual(half):
        all_received(ex_all(half), ex_send.at[half], ex_recv.at[half])
        at = slice(half * rc, (half + 1) * rc)
        branch = recv_ex[0, at].astype(F32)
        for i in range(1, nx):
            branch = branch + recv_ex[i, at].astype(F32)
        tok = col_n[pl.ds(pl.multiple_of(c * rh + half * rc, rc), rc), :]
        res[kv, at] = (tok.astype(F32) + branch).astype(BF16)

    rows_a, rows_b = pl.ds(0, rc), pl.ds(rc, rc)

    y_arrival, z_arrival = [0, *ring(ny)[::-1]], [0, *ring(nz)[::-1]]
    y_last, z_last = y_arrival[-1], z_arrival[-1]

    rq = rc // 2

    def part_of(base, part):
        return pl.ds(base, rc) if part is None else pl.ds(base + part * rq, rq)

    def fa_copy(k, sem, dev, part=None):
        blk = res.at[k, part_of(0, part), :]
        return remote(blk, blk, fa_send, fa_recv.at[sem], dev)

    def fb_copy(k, sem, dev, part=None):
        blk = res.at[k, part_of(rc, part), :]
        return remote(blk, blk, fb_send, fb_recv.at[sem], dev)

    def near_a(d, part):
        return part * (ny - 1) + d - 1

    def near_b(d, part):
        return part * (nz - 1) + d - 1

    def late_a(dy, dz):
        return 2 * (ny - 1) + (ny - 1 + dz if dy == y_last else y_arrival.index(dy))

    def late_b(dz, dy):
        return 2 * (nz - 1) + (nz - 1 + dy if dz == z_last else z_arrival.index(dz))

    def home(dz, dy):
        return lax.rem(z + nz - dz, nz) * ny + lax.rem(y + ny - dy, ny)

    def y_dev(d):
        return {"kv_1": lax.rem(y + d, ny)}

    def z_dev(d):
        return {"kv_0": lax.rem(z + d, nz)}

    residual(0)
    for part in range(2):
        for d in ring(ny):
            fa_copy(kv, near_a(d, part), y_dev(d), part).start()
    for d in ring(nz):
        fa_copy(kv, late_a(0, d), z_dev(d)).start()
    residual(1)
    for part in range(2):
        for d in ring(nz):
            fb_copy(kv, near_b(d, part), z_dev(d), part).start()
    for d in ring(ny):
        fb_copy(kv, late_b(0, d), y_dev(d)).start()

    res_t[...] = res[kv].astype(F32).T.astype(BF16)
    r_copy = remote(
        res_t.at[block(x * nc + other, dt), :], recv_r, r_send, r_recv, partner
    )
    r_copy.start()

    def up(*blocks):
        total, acc = total_sq[...], acc_up[...]
        for dz, dy in blocks:
            k = home(dz, dy)
            at = block(k, dk)
            blk = res[k].astype(F32)
            sq = blk * blk
            for i in range(dk // 128):
                total = total + sq[:, i * 128 : (i + 1) * 128]
            acc = acc + jnp.dot(
                (blk * mlp_gain[:, at]).astype(BF16), w_up[at, :], preferred_element_type=F32
            )
        total_sq[...], acc_up[...] = total, acc

    acc_up[...] = jnp.zeros_like(acc_up)
    total_sq[...] = jnp.zeros_like(total_sq)
    for swap in swaps[1:]:
        swap.wait_recv()
    up((0, 0))

    @pl.when(keeper == c)
    def _():
        all_sent(d_bytes(nkv - 1), d_send, d_recv)

    @pl.when(keeper != c)
    def _():
        all_sent(d_bytes(nkv), d_send, d_recv)

    for half in range(2):
        all_sent(ex_all(half), ex_send.at[half], ex_recv.at[half])

    for part in range(2):
        for i in range(1, max(ny, nz)):
            if i < ny:
                dy = y_arrival[i]
                fa_copy(home(0, dy), near_a(dy, part), partner, part).wait_recv()
                for d in ring(nz):
                    fa_copy(home(0, dy), late_a(dy, d), z_dev(d), part).start()
            if i < nz:
                dz = z_arrival[i]
                fb_copy(home(dz, 0), near_b(dz, part), partner, part).wait_recv()
                for d in ring(ny):
                    fb_copy(home(dz, 0), late_b(dz, d), y_dev(d), part).start()

    got_a = {(0, dy) for dy in range(ny)}
    got_b = {(dz, 0) for dz in range(nz)}
    done = {(0, 0)}

    def up_ready():
        ready = sorted((got_a & got_b) - done)
        done.update(ready)
        for i in range(0, len(ready), 2):
            up(*ready[i : i + 2])

    for i in range(max(ny, nz)):
        if i < ny - 1:
            dy = y_arrival[i]
            all_received(
                res.at[pl.ds(0, nz - 1), rows_a, :], fa_send, fa_recv.at[late_a(dy, 1)]
            )
            got_a |= {(dz, dy) for dz in range(1, nz)}
        if i < nz - 1:
            dz = z_arrival[i]
            all_received(
                res.at[pl.ds(0, ny - 1), rows_b, :], fb_send, fb_recv.at[late_b(dz, 1)]
            )
            got_b |= {(dz, dy) for dy in range(1, ny)}
        up_ready()
    for i in range(1, max(ny, nz)):
        if i < nz:
            dz = z_arrival[i]
            fa_copy(home(dz, y_last), late_a(y_last, dz), partner).wait_recv()
            got_a.add((dz, y_last))
        if i < ny:
            dy = y_arrival[i]
            fb_copy(home(z_last, dy), late_b(z_last, dy), partner).wait_recv()
            got_b.add((z_last, dy))
        up_ready()

    scale = lax.rsqrt(jnp.sum(total_sq[...], axis=1, keepdims=True) / width + EPSILON)
    relu = jnp.maximum(acc_up[...] * scale, 0.0)
    hid[...] = (relu * relu).astype(BF16)

    hw = dk // 2
    part_a, part_b = pl.ds(0, hw), pl.ds(hw, hw)

    def h1a_copy(dz, k):
        return remote(
            send_h.at[k, :, part_a],
            recv_h1a.at[lax.rem(k, ny), dz - 1],
            h1a_send,
            h1a_recv.at[lax.rem(k, ny)],
            {"kv_0": k // ny},
        )

    def h1b_copy(dy, k):
        return remote(
            send_h.at[k, :, part_b],
            recv_h1b.at[k // ny, dy - 1],
            h1b_send,
            h1b_recv.at[k // ny],
            {"kv_1": lax.rem(k, ny)},
        )

    def down(dz, dy):
        zk, yk = lax.rem(z + dz, nz), lax.rem(y + dy, ny)
        k = zk * ny + yk
        out = jnp.dot(hid[...], w_down[:, block(k, dk)], preferred_element_type=F32)
        send_h[k] = out.astype(BF16)
        if dz:
            h1a_copy(dz, k).start()
        if dy:
            h1b_copy(dy, k).start()

    z_order, y_order = [*ring(nz), 0], [*ring(ny), 0]
    for s in range(max(nz, ny)):
        shell = [(i, s) for i in range(s, nz)] + [(s, i) for i in range(s + 1, ny)]
        for i, j in shell:
            if i < nz and j < ny:
                down(z_order[i], y_order[j])
    all_sent(res.at[pl.ds(0, nkv - 1), rows_a, :], fa_send, fa_recv.at[0])
    all_sent(res.at[pl.ds(0, nkv - 1), rows_b, :], fb_send, fb_recv.at[0])
    for swap in swaps:
        swap.wait_send()
    r_copy.wait_send()

    def h1a_sum(yk):
        acc = send_h[z * ny + yk, :, 0:hw].astype(F32)
        all_received(recv_h1a.at[yk], h1a_send, h1a_recv.at[yk])
        for i in range(nz - 1):
            acc = acc + recv_h1a[yk, i].astype(F32)
        return acc

    def h1b_sum(zk):
        acc = send_h[zk * ny + y, :, hw : 2 * hw].astype(F32)
        all_received(recv_h1b.at[zk], h1b_send, h1b_recv.at[zk])
        for i in range(ny - 1):
            acc = acc + recv_h1b[zk, i].astype(F32)
        return acc

    def deliver(d, core):
        if core:
            total, line, buf = h1b_sum(lax.rem(z + d, nz)), z, send_xb.at[d]
            dev = {"kv_0": lax.rem(z + d, nz), "tp_1": core}
        else:
            total, line, buf = h1a_sum(lax.rem(y + d, ny)), y, send_xa.at[d]
            dev = {"kv_1": lax.rem(y + d, ny), "tp_1": core}
        buf[...] = total.T.astype(BF16)
        for dx in [*ring(nx), 0]:
            to_x = lax.rem(x + dx, nx)
            at = block(to_x, dt)

            def send(at=at, to_x=to_x):
                to = {**dev, "tp_0": to_x}
                remote(buf.at[at], recv_x.at[line, tp], x_send, x_recv, to).start()

            if d or dx:
                send()
            else:

                @pl.when(c != core)
                def _():
                    send()

                @pl.when(c == core)
                def _():
                    recv_x[line, tp] = buf[at]

    for i in range(max(ny, nz)):
        if i < ny:
            deliver([*ring(ny), 0][i], 0)
        if i < nz:
            deliver([*ring(nz), 0][i], 1)

    def finish(lines):
        all_received(bytes_x.at[pl.ds(0, lines * ntp - 1)], x_send, x_recv)
        for core, residual in ((c, res_t[block(tp, dt), :]), (other, recv_r[...])):
            total = residual.astype(F32)
            for i in range(lines):
                for xx in range(nx):
                    total = total + recv_x[i, xx * nc + core].astype(F32)
            mixed_ref[:, block(core, rh)] = total.astype(BF16)

    r_copy.wait_recv()

    @pl.when(c == 0)
    def _():
        finish(ny)

    @pl.when(c == 1)
    def _():
        finish(nz)

    all_sent(bytes_x.at[pl.ds(0, (ny + nz) * nx - 1)], x_send, x_recv)
    all_sent(recv_h1a, h1a_send, h1a_recv.at[0])
    all_sent(recv_h1b, h1b_send, h1b_recv.at[0])
    state_out.wait()


STORES = 4


def store_kernel(mixed_ref, state_ref, mixed_out, state_out, sem):
    n = state_ref.shape[0] // STORES
    copies = [pltpu.make_async_copy(mixed_ref, mixed_out, sem.at[0])]
    for i in range(STORES):
        at = pl.ds(i * n, n)
        copies.append(pltpu.make_async_copy(state_ref.at[at], state_out.at[at], sem.at[1 + i]))
    for copy in copies:
        copy.start()
    for copy in copies:
        copy.wait()


def local(
    sizes,
    tokens,
    mix_gain,
    w_query,
    w_key,
    w_value,
    w_gate,
    w_beta,
    w_decay,
    decay_rate,
    out_gain,
    state,
    w_out,
    mlp_gain,
    w_up,
    w_down,
):
    nz, ny, nx, nc = sizes
    nkv, ntp = nz * ny, nx * nc
    rows, dt = tokens.shape
    dk = dt * ntp
    rb, heads, head, _ = state.shape
    proj = heads * head
    sent = 4 * proj + 128
    reductions = ((proj + 128, True), (proj, False), (proj, True), (proj, False))
    first = [(ny, nz) if by_z else (nz, ny) for _, by_z in reductions]
    widths = [w for w, _ in reductions]
    n_heads = w_beta.shape[1]
    ff = w_up.shape[1]
    rh = rows // nc
    rc = rh // 2
    vmem, dma = pltpu.VMEM, pltpu.SemaphoreType.DMA
    scratch = [
        vmem((dk, rows), BF16),
        vmem((4, dk, proj), BF16),
        vmem((128, dk), BF16),
        vmem((dk, dk), BF16),
        vmem((n_heads, dk), BF16),
        vmem((n_heads, dk), BF16),
        vmem((1, dk), F32),
        vmem((1, head), F32),
        vmem((1, dk * nkv), F32),
        vmem((1, heads), F32),
        vmem((nc * proj, dk), BF16),
        vmem((w_up.shape[0], 2 * ff), BF16),
        vmem((2 * ff, w_down.shape[1]), BF16),
        vmem(state.shape, F32),
        vmem((rows, dk), BF16),
        vmem((rows, sent), BF16),
        [vmem((n2, n1 - 1, rb, w), BF16) for (n2, n1), w in zip(first, widths)],
        [vmem((n2 - 1, rb, w), BF16) for (n2, n1), w in zip(first, widths)],
        [vmem((n2 - 1, rb, w), BF16) for (n2, n1), w in zip(first, widths)],
        vmem((rb // 8, heads, head, 128), F32),
        vmem((heads, rb, head), F32),
        vmem((heads, 4 * rb, 2 * head), BF16),
        vmem((rb // 2, heads, 2 * head, 2 * head), BF16),
        vmem((4, heads, rb, head), F32),
        vmem((rb, proj), BF16),
        vmem((rh, nc * proj), BF16),
        vmem((nx, rh, dk), BF16),
        vmem((nkv, rh, dk), BF16),
        vmem((dk, rh), BF16),
        vmem((dt, rh), BF16),
        vmem((rh, 2 * ff), BF16),
        vmem((rh, 2 * ff), F32),
        vmem((rh, 128), F32),
        vmem((nkv, rh, dk), BF16),
        vmem((ny, nz - 1, rh, dk // 2), BF16),
        vmem((nz, ny - 1, rh, dk // 2), BF16),
        vmem((ny, dk // 2, rh), BF16),
        vmem((nz, dk // 2, rh), BF16),
        vmem((max(ny, nz), ntp, dt, rh), BF16),
        vmem((max(ny, nz) * ntp, dt, rh), BF16),
        dma((13,)),
        dma(()),
        dma(()),
        dma((4,)),
        dma((4, max(ny, nz))),
        dma((4,)),
        dma((4,)),
        dma(()),
        dma(()),
        dma((2,)),
        dma((2,)),
        dma(()),
        dma(()),
        dma((3 * (ny - 1) + nz,)),
        dma((3 * (nz - 1) + ny,)),
        dma(()),
        dma(()),
        dma((3,)),
        dma((3,)),
        dma(()),
        dma(()),
        dma((ny,)),
        dma((nz,)),
        dma(()),
        dma(()),
    ]
    in_hbm = pl.BlockSpec(memory_space=pl.ANY)
    in_vmem = pl.BlockSpec(memory_space=pltpu.VMEM)
    mixed_t, new_state = pl.pallas_call(
        functools.partial(layer_kernel, sizes),
        out_shape=(
            pltpu.VMEM((dt, rows), BF16),
            pltpu.VMEM(state.shape, F32),
        ),
        in_specs=[in_hbm] * 15,
        out_specs=(in_vmem, in_hbm),
        scratch_shapes=scratch,
        compiler_params=pltpu.CompilerParams(
            collective_id=0, has_side_effects=True, vmem_limit_bytes=63_500_000
        ),
        name="layer",
    )(
        tokens.T,
        mix_gain[None, :],
        w_query,
        w_key,
        w_value,
        w_gate,
        w_beta.T,
        w_decay.T,
        decay_rate[None, :],
        out_gain[None, :],
        state,
        w_out,
        mlp_gain[None, :],
        w_up,
        w_down,
    )
    mixed_t, new_state = pl.pallas_call(
        store_kernel,
        out_shape=(
            jax.ShapeDtypeStruct((dt, rows), BF16),
            jax.ShapeDtypeStruct(state.shape, F32),
        ),
        in_specs=[in_hbm] * 2,
        out_specs=(in_hbm, in_hbm),
        scratch_shapes=[dma((1 + STORES,))],
        compiler_params=pltpu.CompilerParams(vmem_limit_bytes=1_000_000),
        name="store",
    )(mixed_t, new_state)
    return mixed_t.T, new_state


def solution(mesh):
    n = dict(mesh.shape)
    sizes = (n["kv"] // 4, 4, n["tp"] // 2, 2) if n["kv"] >= 8 else (2, n["kv"] // 2, n["tp"] // 2, 2)
    torus = Mesh(mesh.devices.reshape(sizes), KV_TP)
    in_specs = (
        P(None, KV_TP),
        P(KV),
        P(KV, TP),
        P(KV, TP),
        P(KV, TP),
        P(KV, TP),
        P(KV, None),
        P(KV, None),
        P(TP),
        P(),
        P(KV, TP, None, None),
        P(TP, KV),
        P(),
        P(None, KV_TP),
        P(KV_TP, None),
    )
    out_specs = (P(None, KV_TP), P(KV, TP, None, None))
    return jax.shard_map(
        functools.partial(local, sizes),
        mesh=torus,
        in_specs=in_specs,
        out_specs=out_specs,
        check_vma=False,
    )
```

```python
import functools

import jax
import jax.numpy as jnp
from jax import lax
from jax.experimental import pallas as pl
from jax.experimental.pallas import tpu as pltpu
from jax.sharding import Mesh
from jax.sharding import PartitionSpec as P

EPSILON = 1e-06
MESH = pl.DeviceIdType.MESH
KV_TP = ("kv_0", "kv_1", "tp_0", "tp_1")
KV = ("kv_0", "kv_1")
TP = ("tp_0", "tp_1")
F32 = jnp.float32
BF16 = jnp.bfloat16


def silu(v):
    return v / (1.0 + jnp.exp(-v))


def layer_kernel(
    sizes,
    tok_ref,
    mix_gain_ref,
    wq_ref,
    wk_ref,
    wv_ref,
    wg_ref,
    wbeta_ref,
    wdecay_ref,
    rate_ref,
    out_gain_ref,
    state_ref,
    wout_ref,
    mlp_gain_ref,
    wup_ref,
    wdown_ref,
    mixed_ref,
    new_state_ref,
    col_t,
    w_proj,
    w_rates,
    perm,
    w_beta,
    w_decay,
    mix_gain,
    out_gain,
    mlp_gain,
    rate,
    w_out,
    w_up,
    w_down,
    st,
    col_n,
    send_b,
    recv_b1,
    send_b2,
    recv_b2,
    key_t,
    key_s,
    lhs_s,
    st_terms,
    rows_s,
    mine,
    merged,
    recv_ex,
    res,
    res_t,
    recv_r,
    hid,
    acc_up,
    total_sq,
    send_h,
    recv_h1a,
    recv_h1b,
    send_xa,
    send_xb,
    recv_x,
    bytes_x,
    local_sem,
    a_send,
    a_recv,
    b1_send,
    b1_recv,
    b2_send,
    b2_recv,
    d_send,
    d_recv,
    ex_send,
    ex_recv,
    fa_send,
    fb_send,
    fa_recv,
    fb_recv,
    r_send,
    r_recv,
    swap_send,
    swap_recv,
    h1a_send,
    h1b_send,
    h1a_recv,
    h1b_recv,
    x_send,
    x_recv,
):
    nz, ny, nx, nc = sizes
    nkv, ntp = nz * ny, nx * nc
    z, y = lax.axis_index("kv_0"), lax.axis_index("kv_1")
    x, c = lax.axis_index("tp_0"), lax.axis_index("tp_1")
    kv, tp = z * ny + y, x * nc + c
    partner = {"tp_1": nc - 1 - c}

    dt, rows = tok_ref.shape
    ff = wup_ref.shape[1]
    dk = dt * ntp
    width = dk * nkv
    rb, heads, head = st.shape[0], st.shape[1], st.shape[2]
    proj = heads * head
    rh = rows // nc
    rc = rh // 2
    other = nc - 1 - c

    def kv_dev(k):
        return {"kv_0": k // ny, "kv_1": lax.rem(k, ny)}

    def tp_dev(t):
        return {"tp_0": t // nc, "tp_1": lax.rem(t, nc)}

    def remote(src, dst, send_sem, recv_sem, dev):
        return pltpu.make_async_remote_copy(
            src_ref=src,
            dst_ref=dst,
            send_sem=send_sem,
            recv_sem=recv_sem,
            device_id=dev,
            device_id_type=MESH,
        )

    def all_received(ref, send_sem, recv_sem):
        remote(ref, ref, send_sem, recv_sem, partner).wait_recv()

    def all_sent(ref, send_sem, recv_sem):
        remote(ref, ref, send_sem, recv_sem, partner).wait_send()

    def loop(lo, hi, body):
        def wrapped(i, carry):
            body(i)
            return carry

        lax.fori_loop(lo, hi, wrapped, 0)

    def ring(n):
        return sorted(range(1, n), key=lambda d: (-min(d, n - d), d))

    def block(i, n):
        return pl.ds(pl.multiple_of(i * n, n), n)

    barrier = pltpu.get_barrier_semaphore()

    def greet(dev):
        pl.semaphore_signal(barrier, inc=1, device_id=dev, device_id_type=MESH)

    for dx in range(nx):
        for dc in range(nc):
            if dx or dc:
                greet({"tp_0": lax.rem(x + dx, nx), "tp_1": lax.rem(c + dc, nc)})
    for d in range(1, ny):
        greet({"kv_1": lax.rem(y + d, ny)})
    for d in range(1, nz):
        greet({"kv_0": lax.rem(z + d, nz)})

    own_tok = col_t.at[block(tp, dt), :]
    first = (
        (tok_ref, own_tok),
        (wbeta_ref, w_beta),
        (wdecay_ref, w_decay),
        (mix_gain_ref, mix_gain),
        (rate_ref, rate),
        (out_gain_ref, out_gain),
        (mlp_gain_ref, mlp_gain),
        (state_ref, st),
        (wout_ref, w_out.at[block(c, proj), :]),
        (wup_ref, w_up.at[:, pl.ds(0, ff)]),
        (wdown_ref, w_down.at[pl.ds(0, ff), :]),
    )
    copies = [
        pltpu.make_async_copy(src, dst, local_sem.at[i]) for i, (src, dst) in enumerate(first)
    ]
    for copy in copies[:4]:
        copy.start()
    for i, w in enumerate((wq_ref, wk_ref, wv_ref, wg_ref)):
        pltpu.make_async_copy(w, w_proj.at[i], local_sem.at[11]).start()
    for copy in copies[4:]:
        copy.start()

    n_heads = wbeta_ref.shape[0]
    copies[1].wait()
    copies[2].wait()
    w_rates[...] = jnp.zeros_like(w_rates)
    w_rates[0:n_heads, :] = w_beta[...]
    w_rates[32 : 32 + n_heads, :] = w_decay[...]

    width_x = nx * dt
    column = lax.broadcasted_iota(jnp.int32, (dk, dk), 1)
    source = (lax.rem(column, width_x) // dt * nc + column // width_x) * dt + lax.rem(column, dt)
    row = lax.broadcasted_iota(jnp.int32, (dk, dk), 0)
    perm[...] = jnp.where(row == source, 1.0, 0.0).astype(BF16)

    copies[0].wait()
    copies[3].wait()
    pl.semaphore_wait(barrier, ntp - 1 + ny - 1 + nz - 1)

    def tp_peers():
        near = [(0, 1)] if nc == 2 else []
        return [(dx, dc) for dx in ring(nx) for dc in range(nc)] + near

    def tp_peer(dx, dc):
        return lax.rem(x + dx, nx) * nc + lax.rem(c + dc, nc)

    for dx, dc in tp_peers():
        remote(own_tok, own_tok, a_send, a_recv, tp_dev(tp_peer(dx, dc))).start()

    a_all = col_t.at[pl.ds(0, (ntp - 1) * dt), :]
    all_received(a_all, a_send, a_recv)

    cols = col_t[...].astype(F32).T
    col_n[...] = cols.astype(BF16)
    normed = (cols * mix_gain[...]).astype(BF16)
    squares = jnp.sum(cols * cols, axis=1, keepdims=True)

    pltpu.make_async_copy(w_proj, w_proj, local_sem.at[11]).wait()

    def project(i):
        return jnp.dot(normed, w_proj[i], preferred_element_type=F32).astype(BF16)

    class Reduction:
        def __init__(self, i, column, columns, z_first):
            self.i, self.z_first = i, z_first
            self.n1, self.n2 = (nz, ny) if z_first else (ny, nz)
            self.at = pl.ds(column, columns)
            self.recv1, self.send2, self.recv2 = recv_b1[i], send_b2[i], recv_b2[i]

        def place(self, first, second):
            dz, dy = (first, second) if self.z_first else (second, first)
            return lax.rem(z + dz, nz), lax.rem(y + dy, ny)

        def rows(self, first, second):
            zk, yk = self.place(first, second)
            return send_b.at[block(zk * ny + yk, rb), self.at]

        def start(self):
            for second in [*ring(self.n2), 0]:
                for first in ring(self.n1):
                    zk, yk = self.place(first, second)
                    line, dev = (yk, {"kv_0": zk}) if self.z_first else (zk, {"kv_1": yk})
                    remote(
                        self.rows(first, second),
                        self.recv1.at[line, first - 1],
                        b1_send.at[self.i],
                        b1_recv.at[self.i, line],
                        dev,
                    ).start()

        def first_sum(self, second):
            zk, yk = self.place(0, second)
            line = yk if self.z_first else zk
            acc = self.rows(0, second)[...].astype(F32)
            all_received(self.recv1.at[line], b1_send.at[self.i], b1_recv.at[self.i, line])
            for k in range(self.n1 - 1):
                acc = acc + self.recv1[line, k].astype(F32)
            return acc

        def pass_on(self, second):
            zk, yk = self.place(0, second)
            dev = {"kv_1": yk} if self.z_first else {"kv_0": zk}
            blk = self.send2.at[second - 1]
            blk[...] = self.first_sum(second).astype(BF16)
            remote(
                blk, self.recv2.at[second - 1], b2_send.at[self.i], b2_recv.at[self.i], dev
            ).start()

        def second_sum(self, acc):
            all_received(self.recv2, b2_send.at[self.i], b2_recv.at[self.i])
            for k in range(self.n2 - 1):
                acc = acc + self.recv2[k].astype(F32)
            return acc

        def sent(self):
            all_sent(self.recv1, b1_send.at[self.i], b1_recv.at[self.i, 0])
            all_sent(self.recv2, b2_send.at[self.i], b2_recv.at[self.i])

    q_end, k_end = proj + 128, 2 * proj + 128
    for_query = Reduction(0, 0, q_end, True)
    for_key = Reduction(1, q_end, proj, False)
    for_value = Reduction(2, k_end, proj, True)
    for_gate = Reduction(3, k_end + proj, proj, False)

    send_b[:, q_end:k_end] = project(1)
    for_key.start()
    contract_last = (((1,), (1,)), ((), ()))
    rates_part = lax.dot_general(
        normed, w_rates[...], contract_last, preferred_element_type=F32
    )
    lane = lax.broadcasted_iota(jnp.int32, rates_part.shape, 1)
    rates_part = jnp.where(lane == 63, squares, rates_part)
    high = rates_part.astype(BF16).astype(F32)
    low = pltpu.roll(rates_part - high, 64, 1)
    send_b[:, proj:q_end] = jnp.where(lane < 64, high, low).astype(BF16)
    send_b[:, :proj] = project(0)
    for_query.start()
    send_b[:, k_end : k_end + proj] = project(2)
    for_value.start()
    send_b[:, k_end + proj :] = project(3)
    for_gate.start()

    copies[10].wait()

    def reorder(k):
        at = (pl.ds(0, ff), block(k, dk))
        w_down[at] = jnp.dot(w_down[at], perm[...], preferred_element_type=F32).astype(BF16)

    loop(0, nkv, reorder)

    copies[7].wait()

    def split(x):
        high = x.astype(BF16)
        return high, (x - high.astype(F32)).astype(BF16)

    def split_state(g):
        for h in range(heads):
            for i in range(2):
                high, low = split(st[2 * g + i, h])
                at = slice(i * head, (i + 1) * head)
                st_terms[g, h, :head, at] = high
                st_terms[g, h, head:, at] = low

    loop(0, rb // 2, split_state)

    def pass_on_both(by_z, by_y):
        for i in range(max(ny, nz) - 1):
            if i < nz - 1:
                by_y.pass_on(ring(nz)[i])
            if i < ny - 1:
                by_z.pass_on(ring(ny)[i])
        return by_z.first_sum(0), by_y.first_sum(0)

    query_sum, key_sum = pass_on_both(for_query, for_key)

    value_sum, gate_sum = pass_on_both(for_value, for_gate)

    key_sum = for_key.second_sum(key_sum)
    query_sum = for_query.second_sum(query_sum)

    swaps = [
        remote(
            w_out.at[block(c, proj), :],
            w_out.at[block(c, proj), :],
            swap_send.at[0],
            swap_recv.at[0],
            partner,
        ),
        remote(
            w_up.at[:, pl.ds(0, ff)],
            w_up.at[:, pl.ds(ff, ff)],
            swap_send.at[1],
            swap_recv.at[1],
            partner,
        ),
        remote(
            w_down.at[pl.ds(0, ff), :],
            w_down.at[pl.ds(ff, ff), :],
            swap_send.at[2],
            swap_recv.at[2],
            partner,
        ),
    ]
    copies[8].wait()
    copies[9].wait()
    for swap in swaps:
        swap.start()

    rates = query_sum[:, proj:]
    rates = rates + pltpu.roll(rates, 64, 1)
    lane_b = lax.broadcasted_iota(jnp.int32, rates.shape, 1)

    def pick(i):
        return jnp.sum(jnp.where(lane_b == i, rates, 0.0), axis=1, keepdims=True)

    for i in range(4, 7):
        copies[i].wait()
    row_scale = lax.rsqrt(pick(63) / width + EPSILON)
    for h in range(heads):
        at = slice(h * head, (h + 1) * head)
        beta_raw = pick(tp * heads + h) * row_scale
        decay_raw = pick(32 + tp * heads + h) * row_scale
        beta = 1.0 / (1.0 + jnp.exp(-beta_raw))
        softplus = jnp.maximum(decay_raw, 0.0) + jnp.log1p(jnp.exp(-jnp.abs(decay_raw)))
        decay = jnp.exp(-rate[0:1, h : h + 1] * softplus)
        query = silu(query_sum[:, at] * row_scale)
        query = query * lax.rsqrt(jnp.sum(query * query, axis=1, keepdims=True) + EPSILON)
        query = query * head ** (-0.5)
        key = silu(key_sum[:, at] * row_scale)
        key = key * lax.rsqrt(jnp.sum(key * key, axis=1, keepdims=True) + EPSILON)
        key_s[h] = key
        terms = jnp.concatenate([*split(key), *split(query)], axis=0)
        lhs_s[h] = jnp.concatenate([terms, terms], axis=1)
        shape = (rb, head)
        rows_s[0, h] = jnp.broadcast_to(decay, shape)
        rows_s[1, h] = jnp.broadcast_to(beta, shape)
        rows_s[2, h] = jnp.broadcast_to(
            jnp.sum(key * query, axis=1, keepdims=True), shape
        )

    row = lax.broadcasted_iota(jnp.int32, (rb, head), 0)

    def read_pair(g, sums):
        out = []
        for h in range(heads):
            got = jnp.dot(lhs_s[h], st_terms[g, h], preferred_element_type=F32)
            for k in range(2):
                both = got[2 * k * rb : (2 * k + 1) * rb] + got[(2 * k + 1) * rb : (2 * k + 2) * rb]
                acc = sums[2 * h + k]
                for i in range(2):
                    acc = jnp.where(row == 2 * g + i, both[:, i * head : (i + 1) * head], acc)
                out.append(acc)
        return out

    def read_pairs(g, sums):
        for i in range(2):
            sums = read_pair(2 * g + i, sums)
        return sums

    zero = jnp.zeros((rb, head), F32)
    read_sums = lax.fori_loop(0, rb // 4, read_pairs, [zero] * (2 * heads))

    value_sum = for_value.second_sum(value_sum)
    gate_sum = for_gate.second_sum(gate_sum)
    for h in range(heads):
        at = slice(h * head, (h + 1) * head)
        decay = rows_s[0, h]
        value = silu(value_sum[:, at] * row_scale)
        change = rows_s[1, h] * (value - decay * read_sums[2 * h])
        read = decay * read_sums[2 * h + 1] + rows_s[2, h] * change
        rows_s[3, h] = change
        scale = lax.rsqrt(jnp.sum(read * read, axis=1, keepdims=True) / head + EPSILON)
        gate = silu(gate_sum[:, at] * row_scale)
        mine[:, at] = (read * scale * out_gain[...] * gate).astype(BF16)

    per_half = nkv // nc
    keeper = kv // per_half
    my_rows = block(lax.rem(kv, per_half), rb)
    slot = merged.at[my_rows, block(c, proj)]

    def d_bytes(n):
        return send_b.at[pl.ds(0, n * rb), pl.ds(0, proj)]

    def hops(d):
        dz, dy = d // ny, d % ny
        return min(dz, nz - dz) + min(dy, ny - dy)

    def kv_peer(d):
        return lax.rem(z + d // ny, nz) * ny + lax.rem(y + d % ny, ny)

    for d in sorted(range(1, nkv), key=lambda d: -hops(d)):
        dev = {**kv_dev(kv_peer(d)), "tp_1": keeper}
        remote(mine, slot, d_send, d_recv, dev).start()

    @pl.when(keeper != c)
    def _():
        remote(mine, slot, d_send, d_recv, {"tp_1": keeper}).start()

    @pl.when(keeper == c)
    def _():
        merged[my_rows, block(c, proj)] = mine[...]

    group, repeat = 8, 128 // rb
    for h in range(heads):
        key_tr = jnp.concatenate([key_s[h]] * repeat, axis=0).T
        for g in range(rb // group):
            key_t[g, h] = pltpu.roll(key_tr, (128 - g * group) % 128, 1) if g else key_tr

    def write_group(g):
        for i in range(group):
            b = g * group + i
            for h in range(heads):
                st[b, h] = (
                    rows_s[0, h, pl.ds(b, 1), :] * st[b, h]
                    + key_t[g, h, :, i : i + 1] * rows_s[3, h, pl.ds(b, 1), :]
                )

    loop(0, rb // group, write_group)
    state_out = pltpu.make_async_copy(st, new_state_ref, local_sem.at[12])
    state_out.start()
    all_sent(a_all, a_send, a_recv)
    for reduction in (for_query, for_key, for_value, for_gate):
        reduction.sent()

    @pl.when(keeper == c)
    def _():
        all_received(d_bytes(nkv - 1), d_send, d_recv)

    @pl.when(keeper != c)
    def _():
        all_received(d_bytes(nkv), d_send, d_recv)

    swaps[0].wait_recv()

    rq = rc // 2

    def ex_rows(order, part):
        return pl.ds(order * rc + part * rq, rq)

    def ex_start(order, part):
        blk = recv_ex.at[x, ex_rows(order, part), :]
        i = 2 * order + part
        for d in ring(nx):
            to = {"tp_0": lax.rem(x + d, nx)}
            remote(blk, blk, ex_send.at[i], ex_recv.at[i], to).start()

    def ex_all(order, part):
        return recv_ex.at[pl.ds(0, nx - 1), ex_rows(order, part), :]

    for order in range(2):
        at = slice(order * rc, (order + 1) * rc)
        part = jnp.dot(merged[at, :], w_out[...], preferred_element_type=F32)
        recv_ex[x, at] = part.astype(BF16)
        ex_start(order, 0)
    for order in range(2):
        ex_start(order, 1)

    def residual(order, part):
        i = 2 * order + part
        all_received(ex_all(order, part), ex_send.at[i], ex_recv.at[i])
        at = ex_rows(order, part)
        branch = recv_ex[0, at].astype(F32)
        for i in range(1, nx):
            branch = branch + recv_ex[i, at].astype(F32)
        start = c * rh + order * rc + part * rq
        tok = col_n[pl.ds(pl.multiple_of(start, rq), rq), :]
        res[kv, at] = (tok.astype(F32) + branch).astype(BF16)

    rows_a, rows_b = pl.ds(0, rc), pl.ds(rc, rc)

    y_arrival, z_arrival = [0, *ring(ny)[::-1]], [0, *ring(nz)[::-1]]
    y_last, z_last = y_arrival[-1], z_arrival[-1]

    def part_of(base, part):
        return pl.ds(base, rc) if part is None else pl.ds(base + part * rq, rq)

    def fa_copy(k, sem, dev, part=None):
        blk = res.at[k, part_of(0, part), :]
        return remote(blk, blk, fa_send, fa_recv.at[sem], dev)

    def fb_copy(k, sem, dev, part=None):
        blk = res.at[k, part_of(rc, part), :]
        return remote(blk, blk, fb_send, fb_recv.at[sem], dev)

    def near_a(d, part):
        return part * (ny - 1) + d - 1

    def near_b(d, part):
        return part * (nz - 1) + d - 1

    def late_a(dy, dz):
        return 2 * (ny - 1) + (ny - 1 + dz if dy == y_last else y_arrival.index(dy))

    def late_b(dz, dy):
        return 2 * (nz - 1) + (nz - 1 + dy if dz == z_last else z_arrival.index(dz))

    def home(dz, dy):
        return lax.rem(z + nz - dz, nz) * ny + lax.rem(y + ny - dy, ny)

    def y_dev(d):
        return {"kv_1": lax.rem(y + d, ny)}

    def z_dev(d):
        return {"kv_0": lax.rem(z + d, nz)}

    for part in range(2):
        residual(0, part)
        for d in ring(ny):
            fa_copy(kv, near_a(d, part), y_dev(d), part).start()
        residual(1, part)
        for d in ring(nz):
            fb_copy(kv, near_b(d, part), z_dev(d), part).start()
    for d in ring(nz):
        fa_copy(kv, late_a(0, d), z_dev(d)).start()
    for d in ring(ny):
        fb_copy(kv, late_b(0, d), y_dev(d)).start()

    res_t[...] = res[kv].astype(F32).T.astype(BF16)
    r_copy = remote(
        res_t.at[block(x * nc + other, dt), :], recv_r, r_send, r_recv, partner
    )
    r_copy.start()

    def up(*blocks):
        total, acc = total_sq[...], acc_up[...]
        for dz, dy in blocks:
            k = home(dz, dy)
            at = block(k, dk)
            blk = res[k].astype(F32)
            sq = blk * blk
            for i in range(dk // 128):
                total = total + sq[:, i * 128 : (i + 1) * 128]
            acc = acc + jnp.dot(
                (blk * mlp_gain[:, at]).astype(BF16), w_up[at, :], preferred_element_type=F32
            )
        total_sq[...], acc_up[...] = total, acc

    acc_up[...] = jnp.zeros_like(acc_up)
    total_sq[...] = jnp.zeros_like(total_sq)
    for swap in swaps[1:]:
        swap.wait_recv()
    up((0, 0))

    @pl.when(keeper == c)
    def _():
        all_sent(d_bytes(nkv - 1), d_send, d_recv)

    @pl.when(keeper != c)
    def _():
        all_sent(d_bytes(nkv), d_send, d_recv)

    for i in range(4):
        all_sent(ex_all(i // 2, i % 2), ex_send.at[i], ex_recv.at[i])

    for part in range(2):
        for i in range(1, max(ny, nz)):
            if i < ny:
                dy = y_arrival[i]
                fa_copy(home(0, dy), near_a(dy, part), partner, part).wait_recv()
                for d in ring(nz):
                    fa_copy(home(0, dy), late_a(dy, d), z_dev(d), part).start()
            if i < nz:
                dz = z_arrival[i]
                fb_copy(home(dz, 0), near_b(dz, part), partner, part).wait_recv()
                for d in ring(ny):
                    fb_copy(home(dz, 0), late_b(dz, d), y_dev(d), part).start()

    got_a = {(0, dy) for dy in range(ny)}
    got_b = {(dz, 0) for dz in range(nz)}
    done = {(0, 0)}

    def up_ready():
        ready = sorted((got_a & got_b) - done)
        done.update(ready)
        for i in range(0, len(ready), 2):
            up(*ready[i : i + 2])

    for i in range(max(ny, nz)):
        if i < ny - 1:
            dy = y_arrival[i]
            all_received(
                res.at[pl.ds(0, nz - 1), rows_a, :], fa_send, fa_recv.at[late_a(dy, 1)]
            )
            got_a |= {(dz, dy) for dz in range(1, nz)}
        if i < nz - 1:
            dz = z_arrival[i]
            all_received(
                res.at[pl.ds(0, ny - 1), rows_b, :], fb_send, fb_recv.at[late_b(dz, 1)]
            )
            got_b |= {(dz, dy) for dy in range(1, ny)}
        up_ready()
    for i in range(1, max(ny, nz)):
        if i < nz:
            dz = z_arrival[i]
            fa_copy(home(dz, y_last), late_a(y_last, dz), partner).wait_recv()
            got_a.add((dz, y_last))
        if i < ny:
            dy = y_arrival[i]
            fb_copy(home(z_last, dy), late_b(z_last, dy), partner).wait_recv()
            got_b.add((z_last, dy))
        up_ready()

    scale = lax.rsqrt(jnp.sum(total_sq[...], axis=1, keepdims=True) / width + EPSILON)
    relu = jnp.maximum(acc_up[...] * scale, 0.0)
    hid[...] = (relu * relu).astype(BF16)

    hw = dk // 2
    part_a, part_b = pl.ds(0, hw), pl.ds(hw, hw)

    def h1a_copy(dz, k):
        return remote(
            send_h.at[k, :, part_a],
            recv_h1a.at[lax.rem(k, ny), dz - 1],
            h1a_send,
            h1a_recv.at[lax.rem(k, ny)],
            {"kv_0": k // ny},
        )

    def h1b_copy(dy, k):
        return remote(
            send_h.at[k, :, part_b],
            recv_h1b.at[k // ny, dy - 1],
            h1b_send,
            h1b_recv.at[k // ny],
            {"kv_1": lax.rem(k, ny)},
        )

    def down(dz, dy):
        zk, yk = lax.rem(z + dz, nz), lax.rem(y + dy, ny)
        k = zk * ny + yk
        out = jnp.dot(hid[...], w_down[:, block(k, dk)], preferred_element_type=F32)
        send_h[k] = out.astype(BF16)
        if dz:
            h1a_copy(dz, k).start()
        if dy:
            h1b_copy(dy, k).start()

    z_order, y_order = [*ring(nz), 0], [*ring(ny), 0]
    for s in range(max(nz, ny)):
        shell = [(i, s) for i in range(s, nz)] + [(s, i) for i in range(s + 1, ny)]
        for i, j in shell:
            if i < nz and j < ny:
                down(z_order[i], y_order[j])
    all_sent(res.at[pl.ds(0, nkv - 1), rows_a, :], fa_send, fa_recv.at[0])
    all_sent(res.at[pl.ds(0, nkv - 1), rows_b, :], fb_send, fb_recv.at[0])
    for swap in swaps:
        swap.wait_send()
    r_copy.wait_send()

    def h1a_sum(yk):
        acc = send_h[z * ny + yk, :, 0:hw].astype(F32)
        all_received(recv_h1a.at[yk], h1a_send, h1a_recv.at[yk])
        for i in range(nz - 1):
            acc = acc + recv_h1a[yk, i].astype(F32)
        return acc

    def h1b_sum(zk):
        acc = send_h[zk * ny + y, :, hw : 2 * hw].astype(F32)
        all_received(recv_h1b.at[zk], h1b_send, h1b_recv.at[zk])
        for i in range(ny - 1):
            acc = acc + recv_h1b[zk, i].astype(F32)
        return acc

    def deliver(d, core):
        if core:
            total, line, buf = h1b_sum(lax.rem(z + d, nz)), z, send_xb.at[d]
            dev = {"kv_0": lax.rem(z + d, nz), "tp_1": core}
        else:
            total, line, buf = h1a_sum(lax.rem(y + d, ny)), y, send_xa.at[d]
            dev = {"kv_1": lax.rem(y + d, ny), "tp_1": core}
        buf[...] = total.T.astype(BF16)
        for dx in [*ring(nx), 0]:
            to_x = lax.rem(x + dx, nx)
            at = block(to_x, dt)

            def send(at=at, to_x=to_x):
                to = {**dev, "tp_0": to_x}
                remote(buf.at[at], recv_x.at[line, tp], x_send, x_recv, to).start()

            if d or dx:
                send()
            else:

                @pl.when(c != core)
                def _():
                    send()

                @pl.when(c == core)
                def _():
                    recv_x[line, tp] = buf[at]

    for i in range(max(ny, nz)):
        if i < ny:
            deliver([*ring(ny), 0][i], 0)
        if i < nz:
            deliver([*ring(nz), 0][i], 1)

    def finish(lines):
        all_received(bytes_x.at[pl.ds(0, lines * ntp - 1)], x_send, x_recv)
        for core, residual in ((c, res_t[block(tp, dt), :]), (other, recv_r[...])):
            total = residual.astype(F32)
            for i in range(lines):
                for xx in range(nx):
                    total = total + recv_x[i, xx * nc + core].astype(F32)
            mixed_ref[:, block(core, rh)] = total.astype(BF16)

    r_copy.wait_recv()

    @pl.when(c == 0)
    def _():
        finish(ny)

    @pl.when(c == 1)
    def _():
        finish(nz)

    all_sent(bytes_x.at[pl.ds(0, (ny + nz) * nx - 1)], x_send, x_recv)
    all_sent(recv_h1a, h1a_send, h1a_recv.at[0])
    all_sent(recv_h1b, h1b_send, h1b_recv.at[0])
    state_out.wait()


STORES = 4


def store_kernel(mixed_ref, state_ref, mixed_out, state_out, sem):
    n = state_ref.shape[0] // STORES
    copies = [pltpu.make_async_copy(mixed_ref, mixed_out, sem.at[0])]
    for i in range(STORES):
        at = pl.ds(i * n, n)
        copies.append(pltpu.make_async_copy(state_ref.at[at], state_out.at[at], sem.at[1 + i]))
    for copy in copies:
        copy.start()
    for copy in copies:
        copy.wait()


def local(
    sizes,
    tokens,
    mix_gain,
    w_query,
    w_key,
    w_value,
    w_gate,
    w_beta,
    w_decay,
    decay_rate,
    out_gain,
    state,
    w_out,
    mlp_gain,
    w_up,
    w_down,
):
    nz, ny, nx, nc = sizes
    nkv, ntp = nz * ny, nx * nc
    rows, dt = tokens.shape
    dk = dt * ntp
    rb, heads, head, _ = state.shape
    proj = heads * head
    sent = 4 * proj + 128
    reductions = ((proj + 128, True), (proj, False), (proj, True), (proj, False))
    first = [(ny, nz) if by_z else (nz, ny) for _, by_z in reductions]
    widths = [w for w, _ in reductions]
    n_heads = w_beta.shape[1]
    ff = w_up.shape[1]
    rh = rows // nc
    rc = rh // 2
    vmem, dma = pltpu.VMEM, pltpu.SemaphoreType.DMA
    scratch = [
        vmem((dk, rows), BF16),
        vmem((4, dk, proj), BF16),
        vmem((128, dk), BF16),
        vmem((dk, dk), BF16),
        vmem((n_heads, dk), BF16),
        vmem((n_heads, dk), BF16),
        vmem((1, dk), F32),
        vmem((1, head), F32),
        vmem((1, dk * nkv), F32),
        vmem((1, heads), F32),
        vmem((nc * proj, dk), BF16),
        vmem((w_up.shape[0], 2 * ff), BF16),
        vmem((2 * ff, w_down.shape[1]), BF16),
        vmem(state.shape, F32),
        vmem((rows, dk), BF16),
        vmem((rows, sent), BF16),
        [vmem((n2, n1 - 1, rb, w), BF16) for (n2, n1), w in zip(first, widths)],
        [vmem((n2 - 1, rb, w), BF16) for (n2, n1), w in zip(first, widths)],
        [vmem((n2 - 1, rb, w), BF16) for (n2, n1), w in zip(first, widths)],
        vmem((rb // 8, heads, head, 128), F32),
        vmem((heads, rb, head), F32),
        vmem((heads, 4 * rb, 2 * head), BF16),
        vmem((rb // 2, heads, 2 * head, 2 * head), BF16),
        vmem((4, heads, rb, head), F32),
        vmem((rb, proj), BF16),
        vmem((rh, nc * proj), BF16),
        vmem((nx, rh, dk), BF16),
        vmem((nkv, rh, dk), BF16),
        vmem((dk, rh), BF16),
        vmem((dt, rh), BF16),
        vmem((rh, 2 * ff), BF16),
        vmem((rh, 2 * ff), F32),
        vmem((rh, 128), F32),
        vmem((nkv, rh, dk), BF16),
        vmem((ny, nz - 1, rh, dk // 2), BF16),
        vmem((nz, ny - 1, rh, dk // 2), BF16),
        vmem((ny, dk // 2, rh), BF16),
        vmem((nz, dk // 2, rh), BF16),
        vmem((max(ny, nz), ntp, dt, rh), BF16),
        vmem((max(ny, nz) * ntp, dt, rh), BF16),
        dma((13,)),
        dma(()),
        dma(()),
        dma((4,)),
        dma((4, max(ny, nz))),
        dma((4,)),
        dma((4,)),
        dma(()),
        dma(()),
        dma((4,)),
        dma((4,)),
        dma(()),
        dma(()),
        dma((3 * (ny - 1) + nz,)),
        dma((3 * (nz - 1) + ny,)),
        dma(()),
        dma(()),
        dma((3,)),
        dma((3,)),
        dma(()),
        dma(()),
        dma((ny,)),
        dma((nz,)),
        dma(()),
        dma(()),
    ]
    in_hbm = pl.BlockSpec(memory_space=pl.ANY)
    in_vmem = pl.BlockSpec(memory_space=pltpu.VMEM)
    mixed_t, new_state = pl.pallas_call(
        functools.partial(layer_kernel, sizes),
        out_shape=(
            pltpu.VMEM((dt, rows), BF16),
            pltpu.VMEM(state.shape, F32),
        ),
        in_specs=[in_hbm] * 15,
        out_specs=(in_vmem, in_hbm),
        scratch_shapes=scratch,
        compiler_params=pltpu.CompilerParams(
            collective_id=0, has_side_effects=True, vmem_limit_bytes=63_500_000
        ),
        name="layer",
    )(
        tokens.T,
        mix_gain[None, :],
        w_query,
        w_key,
        w_value,
        w_gate,
        w_beta.T,
        w_decay.T,
        decay_rate[None, :],
        out_gain[None, :],
        state,
        w_out,
        mlp_gain[None, :],
        w_up,
        w_down,
    )
    mixed_t, new_state = pl.pallas_call(
        store_kernel,
        out_shape=(
            jax.ShapeDtypeStruct((dt, rows), BF16),
            jax.ShapeDtypeStruct(state.shape, F32),
        ),
        in_specs=[in_hbm] * 2,
        out_specs=(in_hbm, in_hbm),
        scratch_shapes=[dma((1 + STORES,))],
        compiler_params=pltpu.CompilerParams(vmem_limit_bytes=1_000_000),
        name="store",
    )(mixed_t, new_state)
    return mixed_t.T, new_state


def solution(mesh):
    n = dict(mesh.shape)
    sizes = (n["kv"] // 4, 4, n["tp"] // 2, 2) if n["kv"] >= 8 else (2, n["kv"] // 2, n["tp"] // 2, 2)
    torus = Mesh(mesh.devices.reshape(sizes), KV_TP)
    in_specs = (
        P(None, KV_TP),
        P(KV),
        P(KV, TP),
        P(KV, TP),
        P(KV, TP),
        P(KV, TP),
        P(KV, None),
        P(KV, None),
        P(TP),
        P(),
        P(KV, TP, None, None),
        P(TP, KV),
        P(),
        P(None, KV_TP),
        P(KV_TP, None),
    )
    out_specs = (P(None, KV_TP), P(KV, TP, None, None))
    return jax.shard_map(
        functools.partial(local, sizes),
        mesh=torus,
        in_specs=in_specs,
        out_specs=out_specs,
        check_vma=False,
    )
```

```python
import functools

import jax
import jax.numpy as jnp
from jax import lax
from jax.experimental import pallas as pl
from jax.experimental.pallas import tpu as pltpu
from jax.sharding import Mesh
from jax.sharding import PartitionSpec as P

EPSILON = 1e-06
MESH = pl.DeviceIdType.MESH
KV_TP = ("kv_0", "kv_1", "tp_0", "tp_1")
KV = ("kv_0", "kv_1")
TP = ("tp_0", "tp_1")
F32 = jnp.float32
BF16 = jnp.bfloat16


def silu(v):
    return v / (1.0 + jnp.exp(-v))


def layer_kernel(
    sizes,
    tok_ref,
    mix_gain_ref,
    wq_ref,
    wk_ref,
    wv_ref,
    wg_ref,
    wbeta_ref,
    wdecay_ref,
    rate_ref,
    out_gain_ref,
    state_ref,
    wout_ref,
    mlp_gain_ref,
    wup_ref,
    wdown_ref,
    mixed_ref,
    new_state_ref,
    col_t,
    w_proj,
    w_rates,
    perm,
    w_beta,
    w_decay,
    mix_gain,
    out_gain,
    mlp_gain,
    rate,
    w_out,
    w_up,
    w_down,
    st,
    col_n,
    send_b,
    recv_b1,
    send_b2,
    recv_b2,
    key_t,
    key_s,
    lhs_s,
    st_terms,
    rows_s,
    mine,
    merged,
    recv_ex,
    res,
    res_t,
    recv_r,
    hid,
    acc_up,
    total_sq,
    send_h,
    recv_h1a,
    recv_h1b,
    send_xa,
    send_xb,
    recv_x,
    bytes_x,
    local_sem,
    a_send,
    a_recv,
    b1_send,
    b1_recv,
    b2_send,
    b2_recv,
    d_send,
    d_recv,
    ex_send,
    ex_recv,
    fa_send,
    fb_send,
    fa_recv,
    fb_recv,
    r_send,
    r_recv,
    swap_send,
    swap_recv,
    h1a_send,
    h1b_send,
    h1a_recv,
    h1b_recv,
    x_send,
    x_recv,
):
    nz, ny, nx, nc = sizes
    nkv, ntp = nz * ny, nx * nc
    z, y = lax.axis_index("kv_0"), lax.axis_index("kv_1")
    x, c = lax.axis_index("tp_0"), lax.axis_index("tp_1")
    kv, tp = z * ny + y, x * nc + c
    partner = {"tp_1": nc - 1 - c}

    dt, rows = tok_ref.shape
    ff = wup_ref.shape[1]
    dk = dt * ntp
    width = dk * nkv
    rb, heads, head = st.shape[0], st.shape[1], st.shape[2]
    proj = heads * head
    rh = rows // nc
    rc = rh // 2
    other = nc - 1 - c

    def kv_dev(k):
        return {"kv_0": k // ny, "kv_1": lax.rem(k, ny)}

    def tp_dev(t):
        return {"tp_0": t // nc, "tp_1": lax.rem(t, nc)}

    def remote(src, dst, send_sem, recv_sem, dev):
        return pltpu.make_async_remote_copy(
            src_ref=src,
            dst_ref=dst,
            send_sem=send_sem,
            recv_sem=recv_sem,
            device_id=dev,
            device_id_type=MESH,
        )

    def all_received(ref, send_sem, recv_sem):
        remote(ref, ref, send_sem, recv_sem, partner).wait_recv()

    def all_sent(ref, send_sem, recv_sem):
        remote(ref, ref, send_sem, recv_sem, partner).wait_send()

    def loop(lo, hi, body):
        def wrapped(i, carry):
            body(i)
            return carry

        lax.fori_loop(lo, hi, wrapped, 0)

    def ring(n):
        return sorted(range(1, n), key=lambda d: (-min(d, n - d), d))

    def block(i, n):
        return pl.ds(pl.multiple_of(i * n, n), n)

    barrier = pltpu.get_barrier_semaphore()

    def greet(dev):
        pl.semaphore_signal(barrier, inc=1, device_id=dev, device_id_type=MESH)

    for dx in [*ring(nx), 0]:
        for dc in range(nc):
            if dx or dc:
                greet({"tp_0": lax.rem(x + dx, nx), "tp_1": lax.rem(c + dc, nc)})
    for d in range(1, ny):
        greet({"kv_1": lax.rem(y + d, ny)})
    for d in range(1, nz):
        greet({"kv_0": lax.rem(z + d, nz)})

    own_tok = col_t.at[block(tp, dt), :]
    first = (
        (tok_ref, own_tok),
        (wbeta_ref, w_beta),
        (wdecay_ref, w_decay),
        (mix_gain_ref, mix_gain),
        (rate_ref, rate),
        (out_gain_ref, out_gain),
        (mlp_gain_ref, mlp_gain),
        (state_ref, st),
        (wout_ref, w_out.at[block(c, proj), :]),
        (wup_ref, w_up.at[:, pl.ds(0, ff)]),
        (wdown_ref, w_down.at[pl.ds(0, ff), :]),
    )
    copies = [
        pltpu.make_async_copy(src, dst, local_sem.at[i]) for i, (src, dst) in enumerate(first)
    ]
    for copy in copies[:4]:
        copy.start()
    for i, w in enumerate((wq_ref, wk_ref, wv_ref, wg_ref)):
        pltpu.make_async_copy(w, w_proj.at[i], local_sem.at[11]).start()
    for copy in copies[4:]:
        copy.start()

    n_heads = wbeta_ref.shape[0]
    copies[1].wait()
    copies[2].wait()
    w_rates[...] = jnp.zeros_like(w_rates)
    w_rates[0:n_heads, :] = w_beta[...]
    w_rates[32 : 32 + n_heads, :] = w_decay[...]

    width_x = nx * dt
    column = lax.broadcasted_iota(jnp.int32, (dk, dk), 1)
    source = (lax.rem(column, width_x) // dt * nc + column // width_x) * dt + lax.rem(column, dt)
    row = lax.broadcasted_iota(jnp.int32, (dk, dk), 0)
    perm[...] = jnp.where(row == source, 1.0, 0.0).astype(BF16)

    copies[0].wait()
    copies[3].wait()
    pl.semaphore_wait(barrier, ntp - 1 + ny - 1 + nz - 1)

    def tp_peers():
        near = [(0, 1)] if nc == 2 else []
        return [(dx, dc) for dx in ring(nx) for dc in range(nc)] + near

    def tp_peer(dx, dc):
        return lax.rem(x + dx, nx) * nc + lax.rem(c + dc, nc)

    for dx, dc in tp_peers():
        remote(own_tok, own_tok, a_send, a_recv, tp_dev(tp_peer(dx, dc))).start()

    a_all = col_t.at[pl.ds(0, (ntp - 1) * dt), :]
    all_received(a_all, a_send, a_recv)

    cols = col_t[...].astype(F32).T
    col_n[...] = cols.astype(BF16)
    normed = (cols * mix_gain[...]).astype(BF16)
    squares = jnp.sum(cols * cols, axis=1, keepdims=True)

    pltpu.make_async_copy(w_proj, w_proj, local_sem.at[11]).wait()

    def project(i):
        return jnp.dot(normed, w_proj[i], preferred_element_type=F32).astype(BF16)

    class Reduction:
        def __init__(self, i, column, columns, z_first):
            self.i, self.z_first = i, z_first
            self.n1, self.n2 = (nz, ny) if z_first else (ny, nz)
            self.at = pl.ds(column, columns)
            self.recv1, self.send2, self.recv2 = recv_b1[i], send_b2[i], recv_b2[i]

        def place(self, first, second):
            dz, dy = (first, second) if self.z_first else (second, first)
            return lax.rem(z + dz, nz), lax.rem(y + dy, ny)

        def rows(self, first, second):
            zk, yk = self.place(first, second)
            return send_b.at[block(zk * ny + yk, rb), self.at]

        def start(self):
            for second in [*ring(self.n2), 0]:
                for first in ring(self.n1):
                    zk, yk = self.place(first, second)
                    line, dev = (yk, {"kv_0": zk}) if self.z_first else (zk, {"kv_1": yk})
                    remote(
                        self.rows(first, second),
                        self.recv1.at[line, first - 1],
                        b1_send.at[self.i],
                        b1_recv.at[self.i, line],
                        dev,
                    ).start()

        def first_sum(self, second):
            zk, yk = self.place(0, second)
            line = yk if self.z_first else zk
            acc = self.rows(0, second)[...].astype(F32)
            all_received(self.recv1.at[line], b1_send.at[self.i], b1_recv.at[self.i, line])
            for k in range(self.n1 - 1):
                acc = acc + self.recv1[line, k].astype(F32)
            return acc

        def pass_on(self, second):
            zk, yk = self.place(0, second)
            dev = {"kv_1": yk} if self.z_first else {"kv_0": zk}
            blk = self.send2.at[second - 1]
            blk[...] = self.first_sum(second).astype(BF16)
            remote(
                blk, self.recv2.at[second - 1], b2_send.at[self.i], b2_recv.at[self.i], dev
            ).start()

        def second_sum(self, acc):
            all_received(self.recv2, b2_send.at[self.i], b2_recv.at[self.i])
            for k in range(self.n2 - 1):
                acc = acc + self.recv2[k].astype(F32)
            return acc

        def sent(self):
            all_sent(self.recv1, b1_send.at[self.i], b1_recv.at[self.i, 0])
            all_sent(self.recv2, b2_send.at[self.i], b2_recv.at[self.i])

    q_end, k_end = proj + 128, 2 * proj + 128
    for_query = Reduction(0, 0, q_end, True)
    for_key = Reduction(1, q_end, proj, False)
    for_value = Reduction(2, k_end, proj, True)
    for_gate = Reduction(3, k_end + proj, proj, False)

    contract_last = (((1,), (1,)), ((), ()))
    rates_part = lax.dot_general(
        normed, w_rates[...], contract_last, preferred_element_type=F32
    )
    lane = lax.broadcasted_iota(jnp.int32, rates_part.shape, 1)
    rates_part = jnp.where(lane == 63, squares, rates_part)
    high = rates_part.astype(BF16).astype(F32)
    low = pltpu.roll(rates_part - high, 64, 1)
    send_b[:, proj:q_end] = jnp.where(lane < 64, high, low).astype(BF16)
    send_b[:, :proj] = project(0)
    for_query.start()
    send_b[:, q_end:k_end] = project(1)
    for_key.start()
    send_b[:, k_end : k_end + proj] = project(2)
    for_value.start()
    send_b[:, k_end + proj :] = project(3)
    for_gate.start()

    copies[10].wait()

    def reorder(k):
        at = (pl.ds(0, ff), block(k, dk))
        w_down[at] = jnp.dot(w_down[at], perm[...], preferred_element_type=F32).astype(BF16)

    loop(0, nkv, reorder)

    copies[7].wait()

    def split(x):
        high = x.astype(BF16)
        return high, (x - high.astype(F32)).astype(BF16)

    def split_state(g):
        for h in range(heads):
            for i in range(2):
                high, low = split(st[2 * g + i, h])
                at = slice(i * head, (i + 1) * head)
                st_terms[g, h, :head, at] = high
                st_terms[g, h, head:, at] = low

    loop(0, rb // 2, split_state)

    def pass_on_both(by_z, by_y):
        for i in range(max(ny, nz) - 1):
            if i < nz - 1:
                by_y.pass_on(ring(nz)[i])
            if i < ny - 1:
                by_z.pass_on(ring(ny)[i])
        return by_z.first_sum(0), by_y.first_sum(0)

    query_sum, key_sum = pass_on_both(for_query, for_key)

    value_sum, gate_sum = pass_on_both(for_value, for_gate)

    key_sum = for_key.second_sum(key_sum)
    query_sum = for_query.second_sum(query_sum)

    swaps = [
        remote(
            w_out.at[block(c, proj), :],
            w_out.at[block(c, proj), :],
            swap_send.at[0],
            swap_recv.at[0],
            partner,
        ),
        remote(
            w_up.at[:, pl.ds(0, ff)],
            w_up.at[:, pl.ds(ff, ff)],
            swap_send.at[1],
            swap_recv.at[1],
            partner,
        ),
        remote(
            w_down.at[pl.ds(0, ff), :],
            w_down.at[pl.ds(ff, ff), :],
            swap_send.at[2],
            swap_recv.at[2],
            partner,
        ),
    ]
    copies[8].wait()
    copies[9].wait()
    for swap in swaps:
        swap.start()

    rates = query_sum[:, proj:]
    rates = rates + pltpu.roll(rates, 64, 1)
    lane_b = lax.broadcasted_iota(jnp.int32, rates.shape, 1)

    def pick(i):
        return jnp.sum(jnp.where(lane_b == i, rates, 0.0), axis=1, keepdims=True)

    for i in range(4, 7):
        copies[i].wait()
    row_scale = lax.rsqrt(pick(63) / width + EPSILON)
    for h in range(heads):
        at = slice(h * head, (h + 1) * head)
        beta_raw = pick(tp * heads + h) * row_scale
        decay_raw = pick(32 + tp * heads + h) * row_scale
        beta = 1.0 / (1.0 + jnp.exp(-beta_raw))
        softplus = jnp.maximum(decay_raw, 0.0) + jnp.log1p(jnp.exp(-jnp.abs(decay_raw)))
        decay = jnp.exp(-rate[0:1, h : h + 1] * softplus)
        query = silu(query_sum[:, at] * row_scale)
        query = query * lax.rsqrt(jnp.sum(query * query, axis=1, keepdims=True) + EPSILON)
        query = query * head ** (-0.5)
        key = silu(key_sum[:, at] * row_scale)
        key = key * lax.rsqrt(jnp.sum(key * key, axis=1, keepdims=True) + EPSILON)
        key_s[h] = key
        terms = jnp.concatenate([*split(key), *split(query)], axis=0)
        lhs_s[h] = jnp.concatenate([terms, terms], axis=1)
        shape = (rb, head)
        rows_s[0, h] = jnp.broadcast_to(decay, shape)
        rows_s[1, h] = jnp.broadcast_to(beta, shape)
        rows_s[2, h] = jnp.broadcast_to(
            jnp.sum(key * query, axis=1, keepdims=True), shape
        )

    row = lax.broadcasted_iota(jnp.int32, (rb, head), 0)

    def read_pair(g, sums):
        out = []
        for h in range(heads):
            got = jnp.dot(lhs_s[h], st_terms[g, h], preferred_element_type=F32)
            for k in range(2):
                both = got[2 * k * rb : (2 * k + 1) * rb] + got[(2 * k + 1) * rb : (2 * k + 2) * rb]
                acc = sums[2 * h + k]
                for i in range(2):
                    acc = jnp.where(row == 2 * g + i, both[:, i * head : (i + 1) * head], acc)
                out.append(acc)
        return out

    def read_pairs(g, sums):
        for i in range(2):
            sums = read_pair(2 * g + i, sums)
        return sums

    zero = jnp.zeros((rb, head), F32)
    read_sums = lax.fori_loop(0, rb // 4, read_pairs, [zero] * (2 * heads))

    value_sum = for_value.second_sum(value_sum)
    gate_sum = for_gate.second_sum(gate_sum)
    for h in range(heads):
        at = slice(h * head, (h + 1) * head)
        decay = rows_s[0, h]
        value = silu(value_sum[:, at] * row_scale)
        change = rows_s[1, h] * (value - decay * read_sums[2 * h])
        read = decay * read_sums[2 * h + 1] + rows_s[2, h] * change
        rows_s[3, h] = change
        scale = lax.rsqrt(jnp.sum(read * read, axis=1, keepdims=True) / head + EPSILON)
        gate = silu(gate_sum[:, at] * row_scale)
        mine[:, at] = (read * scale * out_gain[...] * gate).astype(BF16)

    per_half = nkv // nc
    keeper = kv // per_half
    my_rows = block(lax.rem(kv, per_half), rb)
    slot = merged.at[my_rows, block(c, proj)]

    def d_bytes(n):
        return send_b.at[pl.ds(0, n * rb), pl.ds(0, proj)]

    def hops(d):
        dz, dy = d // ny, d % ny
        return min(dz, nz - dz) + min(dy, ny - dy)

    def kv_peer(d):
        return lax.rem(z + d // ny, nz) * ny + lax.rem(y + d % ny, ny)

    for d in sorted(range(1, nkv), key=lambda d: -hops(d)):
        dev = {**kv_dev(kv_peer(d)), "tp_1": keeper}
        remote(mine, slot, d_send, d_recv, dev).start()

    @pl.when(keeper != c)
    def _():
        remote(mine, slot, d_send, d_recv, {"tp_1": keeper}).start()

    @pl.when(keeper == c)
    def _():
        merged[my_rows, block(c, proj)] = mine[...]

    group, repeat = 8, 128 // rb
    for h in range(heads):
        key_tr = jnp.concatenate([key_s[h]] * repeat, axis=0).T
        for g in range(rb // group):
            key_t[g, h] = pltpu.roll(key_tr, (128 - g * group) % 128, 1) if g else key_tr

    def write_group(g):
        for i in range(group):
            b = g * group + i
            for h in range(heads):
                st[b, h] = (
                    rows_s[0, h, pl.ds(b, 1), :] * st[b, h]
                    + key_t[g, h, :, i : i + 1] * rows_s[3, h, pl.ds(b, 1), :]
                )

    loop(0, rb // group, write_group)
    state_out = pltpu.make_async_copy(st, new_state_ref, local_sem.at[12])
    state_out.start()
    all_sent(a_all, a_send, a_recv)
    for reduction in (for_query, for_key, for_value, for_gate):
        reduction.sent()

    @pl.when(keeper == c)
    def _():
        all_received(d_bytes(nkv - 1), d_send, d_recv)

    @pl.when(keeper != c)
    def _():
        all_received(d_bytes(nkv), d_send, d_recv)

    swaps[0].wait_recv()

    rq = rc // 2

    def ex_rows(order, part):
        return pl.ds(order * rc + part * rq, rq)

    def ex_start(order, part):
        blk = recv_ex.at[x, ex_rows(order, part), :]
        i = 2 * order + part
        for d in ring(nx):
            to = {"tp_0": lax.rem(x + d, nx)}
            remote(blk, blk, ex_send.at[i], ex_recv.at[i], to).start()

    def ex_all(order, part):
        return recv_ex.at[pl.ds(0, nx - 1), ex_rows(order, part), :]

    for order in range(2):
        at = slice(order * rc, (order + 1) * rc)
        part = jnp.dot(merged[at, :], w_out[...], preferred_element_type=F32)
        recv_ex[x, at] = part.astype(BF16)
        ex_start(order, 0)
    for order in range(2):
        ex_start(order, 1)

    def residual(order, part):
        i = 2 * order + part
        all_received(ex_all(order, part), ex_send.at[i], ex_recv.at[i])
        at = ex_rows(order, part)
        branch = recv_ex[0, at].astype(F32)
        for i in range(1, nx):
            branch = branch + recv_ex[i, at].astype(F32)
        start = c * rh + order * rc + part * rq
        tok = col_n[pl.ds(pl.multiple_of(start, rq), rq), :]
        res[kv, at] = (tok.astype(F32) + branch).astype(BF16)

    rows_a, rows_b = pl.ds(0, rc), pl.ds(rc, rc)

    y_arrival, z_arrival = [0, *ring(ny)[::-1]], [0, *ring(nz)[::-1]]
    y_last, z_last = y_arrival[-1], z_arrival[-1]

    def part_of(base, part):
        return pl.ds(base, rc) if part is None else pl.ds(base + part * rq, rq)

    def fa_copy(k, sem, dev, part=None):
        blk = res.at[k, part_of(0, part), :]
        return remote(blk, blk, fa_send, fa_recv.at[sem], dev)

    def fb_copy(k, sem, dev, part=None):
        blk = res.at[k, part_of(rc, part), :]
        return remote(blk, blk, fb_send, fb_recv.at[sem], dev)

    def near_a(d, part):
        return part * (ny - 1) + d - 1

    def near_b(d, part):
        return part * (nz - 1) + d - 1

    def late_a(dy, dz):
        return 2 * (ny - 1) + (ny - 1 + dz if dy == y_last else y_arrival.index(dy))

    def late_b(dz, dy):
        return 2 * (nz - 1) + (nz - 1 + dy if dz == z_last else z_arrival.index(dz))

    def home(dz, dy):
        return lax.rem(z + nz - dz, nz) * ny + lax.rem(y + ny - dy, ny)

    def y_dev(d):
        return {"kv_1": lax.rem(y + d, ny)}

    def z_dev(d):
        return {"kv_0": lax.rem(z + d, nz)}

    for part in range(2):
        residual(0, part)
        for d in ring(ny):
            fa_copy(kv, near_a(d, part), y_dev(d), part).start()
        residual(1, part)
        for d in ring(nz):
            fb_copy(kv, near_b(d, part), z_dev(d), part).start()
    for d in ring(nz):
        fa_copy(kv, late_a(0, d), z_dev(d)).start()
    for d in ring(ny):
        fb_copy(kv, late_b(0, d), y_dev(d)).start()

    res_t[...] = res[kv].astype(F32).T.astype(BF16)
    r_copy = remote(
        res_t.at[block(x * nc + other, dt), :], recv_r, r_send, r_recv, partner
    )
    r_copy.start()

    def up(*blocks):
        total, acc = total_sq[...], acc_up[...]
        for dz, dy in blocks:
            k = home(dz, dy)
            at = block(k, dk)
            blk = res[k].astype(F32)
            sq = blk * blk
            for i in range(dk // 128):
                total = total + sq[:, i * 128 : (i + 1) * 128]
            acc = acc + jnp.dot(
                (blk * mlp_gain[:, at]).astype(BF16), w_up[at, :], preferred_element_type=F32
            )
        total_sq[...], acc_up[...] = total, acc

    acc_up[...] = jnp.zeros_like(acc_up)
    total_sq[...] = jnp.zeros_like(total_sq)
    for swap in swaps[1:]:
        swap.wait_recv()
    up((0, 0))

    @pl.when(keeper == c)
    def _():
        all_sent(d_bytes(nkv - 1), d_send, d_recv)

    @pl.when(keeper != c)
    def _():
        all_sent(d_bytes(nkv), d_send, d_recv)

    for i in range(4):
        all_sent(ex_all(i // 2, i % 2), ex_send.at[i], ex_recv.at[i])

    for part in range(2):
        for i in range(1, max(ny, nz)):
            if i < ny:
                dy = y_arrival[i]
                fa_copy(home(0, dy), near_a(dy, part), partner, part).wait_recv()
                for d in ring(nz):
                    fa_copy(home(0, dy), late_a(dy, d), z_dev(d), part).start()
            if i < nz:
                dz = z_arrival[i]
                fb_copy(home(dz, 0), near_b(dz, part), partner, part).wait_recv()
                for d in ring(ny):
                    fb_copy(home(dz, 0), late_b(dz, d), y_dev(d), part).start()

    got_a = {(0, dy) for dy in range(ny)}
    got_b = {(dz, 0) for dz in range(nz)}
    done = {(0, 0)}

    def up_ready():
        ready = sorted((got_a & got_b) - done)
        done.update(ready)
        for i in range(0, len(ready), 2):
            up(*ready[i : i + 2])

    for i in range(max(ny, nz)):
        if i < ny - 1:
            dy = y_arrival[i]
            all_received(
                res.at[pl.ds(0, nz - 1), rows_a, :], fa_send, fa_recv.at[late_a(dy, 1)]
            )
            got_a |= {(dz, dy) for dz in range(1, nz)}
        if i < nz - 1:
            dz = z_arrival[i]
            all_received(
                res.at[pl.ds(0, ny - 1), rows_b, :], fb_send, fb_recv.at[late_b(dz, 1)]
            )
            got_b |= {(dz, dy) for dy in range(1, ny)}
        up_ready()
    for i in range(1, max(ny, nz)):
        if i < nz:
            dz = z_arrival[i]
            fa_copy(home(dz, y_last), late_a(y_last, dz), partner).wait_recv()
            got_a.add((dz, y_last))
        if i < ny:
            dy = y_arrival[i]
            fb_copy(home(z_last, dy), late_b(z_last, dy), partner).wait_recv()
            got_b.add((z_last, dy))
        up_ready()

    scale = lax.rsqrt(jnp.sum(total_sq[...], axis=1, keepdims=True) / width + EPSILON)
    relu = jnp.maximum(acc_up[...] * scale, 0.0)
    hid[...] = (relu * relu).astype(BF16)

    hw = dk // 2
    part_a, part_b = pl.ds(0, hw), pl.ds(hw, hw)

    def h1a_copy(dz, k):
        return remote(
            send_h.at[k, :, part_a],
            recv_h1a.at[lax.rem(k, ny), dz - 1],
            h1a_send,
            h1a_recv.at[lax.rem(k, ny)],
            {"kv_0": k // ny},
        )

    def h1b_copy(dy, k):
        return remote(
            send_h.at[k, :, part_b],
            recv_h1b.at[k // ny, dy - 1],
            h1b_send,
            h1b_recv.at[k // ny],
            {"kv_1": lax.rem(k, ny)},
        )

    def down(dz, dy):
        zk, yk = lax.rem(z + dz, nz), lax.rem(y + dy, ny)
        k = zk * ny + yk
        out = jnp.dot(hid[...], w_down[:, block(k, dk)], preferred_element_type=F32)
        send_h[k] = out.astype(BF16)
        if dz:
            h1a_copy(dz, k).start()
        if dy:
            h1b_copy(dy, k).start()

    z_order, y_order = [*ring(nz), 0], [*ring(ny), 0]
    for s in range(max(nz, ny)):
        shell = [(i, s) for i in range(s, nz)] + [(s, i) for i in range(s + 1, ny)]
        for i, j in shell:
            if i < nz and j < ny:
                down(z_order[i], y_order[j])
    all_sent(res.at[pl.ds(0, nkv - 1), rows_a, :], fa_send, fa_recv.at[0])
    all_sent(res.at[pl.ds(0, nkv - 1), rows_b, :], fb_send, fb_recv.at[0])
    for swap in swaps:
        swap.wait_send()
    r_copy.wait_send()

    def h1a_sum(yk):
        acc = send_h[z * ny + yk, :, 0:hw].astype(F32)
        all_received(recv_h1a.at[yk], h1a_send, h1a_recv.at[yk])
        for i in range(nz - 1):
            acc = acc + recv_h1a[yk, i].astype(F32)
        return acc

    def h1b_sum(zk):
        acc = send_h[zk * ny + y, :, hw : 2 * hw].astype(F32)
        all_received(recv_h1b.at[zk], h1b_send, h1b_recv.at[zk])
        for i in range(ny - 1):
            acc = acc + recv_h1b[zk, i].astype(F32)
        return acc

    def deliver(d, core):
        if core:
            total, line, buf = h1b_sum(lax.rem(z + d, nz)), z, send_xb.at[d]
            dev = {"kv_0": lax.rem(z + d, nz), "tp_1": core}
        else:
            total, line, buf = h1a_sum(lax.rem(y + d, ny)), y, send_xa.at[d]
            dev = {"kv_1": lax.rem(y + d, ny), "tp_1": core}
        buf[...] = total.T.astype(BF16)
        for dx in [*ring(nx), 0]:
            to_x = lax.rem(x + dx, nx)
            at = block(to_x, dt)

            def send(at=at, to_x=to_x):
                to = {**dev, "tp_0": to_x}
                remote(buf.at[at], recv_x.at[line, tp], x_send, x_recv, to).start()

            if d or dx:
                send()
            else:

                @pl.when(c != core)
                def _():
                    send()

                @pl.when(c == core)
                def _():
                    recv_x[line, tp] = buf[at]

    for i in range(max(ny, nz)):
        if i < ny:
            deliver([*ring(ny), 0][i], 0)
        if i < nz:
            deliver([*ring(nz), 0][i], 1)

    def finish(lines):
        all_received(bytes_x.at[pl.ds(0, lines * ntp - 1)], x_send, x_recv)
        for core, residual in ((c, res_t[block(tp, dt), :]), (other, recv_r[...])):
            total = residual.astype(F32)
            for i in range(lines):
                for xx in range(nx):
                    total = total + recv_x[i, xx * nc + core].astype(F32)
            mixed_ref[:, block(core, rh)] = total.astype(BF16)

    r_copy.wait_recv()

    @pl.when(c == 0)
    def _():
        finish(ny)

    @pl.when(c == 1)
    def _():
        finish(nz)

    all_sent(bytes_x.at[pl.ds(0, (ny + nz) * nx - 1)], x_send, x_recv)
    all_sent(recv_h1a, h1a_send, h1a_recv.at[0])
    all_sent(recv_h1b, h1b_send, h1b_recv.at[0])
    state_out.wait()


STORES = 4


def store_kernel(mixed_ref, state_ref, mixed_out, state_out, sem):
    n = state_ref.shape[0] // STORES
    copies = [pltpu.make_async_copy(mixed_ref, mixed_out, sem.at[0])]
    for i in range(STORES):
        at = pl.ds(i * n, n)
        copies.append(pltpu.make_async_copy(state_ref.at[at], state_out.at[at], sem.at[1 + i]))
    for copy in copies:
        copy.start()
    for copy in copies:
        copy.wait()


def local(
    sizes,
    tokens,
    mix_gain,
    w_query,
    w_key,
    w_value,
    w_gate,
    w_beta,
    w_decay,
    decay_rate,
    out_gain,
    state,
    w_out,
    mlp_gain,
    w_up,
    w_down,
):
    nz, ny, nx, nc = sizes
    nkv, ntp = nz * ny, nx * nc
    rows, dt = tokens.shape
    dk = dt * ntp
    rb, heads, head, _ = state.shape
    proj = heads * head
    sent = 4 * proj + 128
    reductions = ((proj + 128, True), (proj, False), (proj, True), (proj, False))
    first = [(ny, nz) if by_z else (nz, ny) for _, by_z in reductions]
    widths = [w for w, _ in reductions]
    n_heads = w_beta.shape[1]
    ff = w_up.shape[1]
    rh = rows // nc
    rc = rh // 2
    vmem, dma = pltpu.VMEM, pltpu.SemaphoreType.DMA
    scratch = [
        vmem((dk, rows), BF16),
        vmem((4, dk, proj), BF16),
        vmem((128, dk), BF16),
        vmem((dk, dk), BF16),
        vmem((n_heads, dk), BF16),
        vmem((n_heads, dk), BF16),
        vmem((1, dk), F32),
        vmem((1, head), F32),
        vmem((1, dk * nkv), F32),
        vmem((1, heads), F32),
        vmem((nc * proj, dk), BF16),
        vmem((w_up.shape[0], 2 * ff), BF16),
        vmem((2 * ff, w_down.shape[1]), BF16),
        vmem(state.shape, F32),
        vmem((rows, dk), BF16),
        vmem((rows, sent), BF16),
        [vmem((n2, n1 - 1, rb, w), BF16) for (n2, n1), w in zip(first, widths)],
        [vmem((n2 - 1, rb, w), BF16) for (n2, n1), w in zip(first, widths)],
        [vmem((n2 - 1, rb, w), BF16) for (n2, n1), w in zip(first, widths)],
        vmem((rb // 8, heads, head, 128), F32),
        vmem((heads, rb, head), F32),
        vmem((heads, 4 * rb, 2 * head), BF16),
        vmem((rb // 2, heads, 2 * head, 2 * head), BF16),
        vmem((4, heads, rb, head), F32),
        vmem((rb, proj), BF16),
        vmem((rh, nc * proj), BF16),
        vmem((nx, rh, dk), BF16),
        vmem((nkv, rh, dk), BF16),
        vmem((dk, rh), BF16),
        vmem((dt, rh), BF16),
        vmem((rh, 2 * ff), BF16),
        vmem((rh, 2 * ff), F32),
        vmem((rh, 128), F32),
        vmem((nkv, rh, dk), BF16),
        vmem((ny, nz - 1, rh, dk // 2), BF16),
        vmem((nz, ny - 1, rh, dk // 2), BF16),
        vmem((ny, dk // 2, rh), BF16),
        vmem((nz, dk // 2, rh), BF16),
        vmem((max(ny, nz), ntp, dt, rh), BF16),
        vmem((max(ny, nz) * ntp, dt, rh), BF16),
        dma((13,)),
        dma(()),
        dma(()),
        dma((4,)),
        dma((4, max(ny, nz))),
        dma((4,)),
        dma((4,)),
        dma(()),
        dma(()),
        dma((4,)),
        dma((4,)),
        dma(()),
        dma(()),
        dma((3 * (ny - 1) + nz,)),
        dma((3 * (nz - 1) + ny,)),
        dma(()),
        dma(()),
        dma((3,)),
        dma((3,)),
        dma(()),
        dma(()),
        dma((ny,)),
        dma((nz,)),
        dma(()),
        dma(()),
    ]
    in_hbm = pl.BlockSpec(memory_space=pl.ANY)
    in_vmem = pl.BlockSpec(memory_space=pltpu.VMEM)
    mixed_t, new_state = pl.pallas_call(
        functools.partial(layer_kernel, sizes),
        out_shape=(
            pltpu.VMEM((dt, rows), BF16),
            pltpu.VMEM(state.shape, F32),
        ),
        in_specs=[in_hbm] * 15,
        out_specs=(in_vmem, in_hbm),
        scratch_shapes=scratch,
        compiler_params=pltpu.CompilerParams(
            collective_id=0, has_side_effects=True, vmem_limit_bytes=63_500_000
        ),
        name="layer",
    )(
        tokens.T,
        mix_gain[None, :],
        w_query,
        w_key,
        w_value,
        w_gate,
        w_beta.T,
        w_decay.T,
        decay_rate[None, :],
        out_gain[None, :],
        state,
        w_out,
        mlp_gain[None, :],
        w_up,
        w_down,
    )
    mixed_t, new_state = pl.pallas_call(
        store_kernel,
        out_shape=(
            jax.ShapeDtypeStruct((dt, rows), BF16),
            jax.ShapeDtypeStruct(state.shape, F32),
        ),
        in_specs=[in_hbm] * 2,
        out_specs=(in_hbm, in_hbm),
        scratch_shapes=[dma((1 + STORES,))],
        compiler_params=pltpu.CompilerParams(vmem_limit_bytes=1_000_000),
        name="store",
    )(mixed_t, new_state)
    return mixed_t.T, new_state


def solution(mesh):
    n = dict(mesh.shape)
    sizes = (n["kv"] // 4, 4, n["tp"] // 2, 2) if n["kv"] >= 8 else (2, n["kv"] // 2, n["tp"] // 2, 2)
    torus = Mesh(mesh.devices.reshape(sizes), KV_TP)
    in_specs = (
        P(None, KV_TP),
        P(KV),
        P(KV, TP),
        P(KV, TP),
        P(KV, TP),
        P(KV, TP),
        P(KV, None),
        P(KV, None),
        P(TP),
        P(),
        P(KV, TP, None, None),
        P(TP, KV),
        P(),
        P(None, KV_TP),
        P(KV_TP, None),
    )
    out_specs = (P(None, KV_TP), P(KV, TP, None, None))
    return jax.shard_map(
        functools.partial(local, sizes),
        mesh=torus,
        in_specs=in_specs,
        out_specs=out_specs,
        check_vma=False,
    )
```

```python
import functools

import jax
import jax.numpy as jnp
from jax import lax
from jax.experimental import pallas as pl
from jax.experimental.pallas import tpu as pltpu
from jax.sharding import Mesh
from jax.sharding import PartitionSpec as P

EPSILON = 1e-06
MESH = pl.DeviceIdType.MESH
KV_TP = ("kv_0", "kv_1", "tp_0", "tp_1")
KV = ("kv_0", "kv_1")
TP = ("tp_0", "tp_1")
F32 = jnp.float32
BF16 = jnp.bfloat16


def silu(v):
    return v / (1.0 + jnp.exp(-v))


def layer_kernel(
    sizes,
    tok_ref,
    mix_gain_ref,
    wq_ref,
    wk_ref,
    wv_ref,
    wg_ref,
    wbeta_ref,
    wdecay_ref,
    rate_ref,
    out_gain_ref,
    state_ref,
    wout_ref,
    mlp_gain_ref,
    wup_ref,
    wdown_ref,
    mixed_ref,
    new_state_ref,
    col_t,
    w_proj,
    w_rates,
    perm,
    w_beta,
    w_decay,
    mix_gain,
    out_gain,
    mlp_gain,
    rate,
    w_out,
    w_up,
    w_down,
    st,
    col_n,
    send_b,
    recv_b1,
    send_b2,
    recv_b2,
    key_t,
    key_s,
    lhs_s,
    st_terms,
    rows_s,
    mine,
    merged,
    recv_ex,
    res,
    res_t,
    recv_r,
    hid,
    acc_up,
    total_sq,
    send_h,
    recv_h1a,
    recv_h1b,
    send_xa,
    send_xb,
    recv_x,
    bytes_x,
    local_sem,
    a_send,
    a_recv,
    b1_send,
    b1_recv,
    b2_send,
    b2_recv,
    d_send,
    d_recv,
    ex_send,
    ex_recv,
    fa_send,
    fb_send,
    fa_recv,
    fb_recv,
    r_send,
    r_recv,
    swap_send,
    swap_recv,
    h1a_send,
    h1b_send,
    h1a_recv,
    h1b_recv,
    x_send,
    x_recv,
):
    nz, ny, nx, nc = sizes
    nkv, ntp = nz * ny, nx * nc
    z, y = lax.axis_index("kv_0"), lax.axis_index("kv_1")
    x, c = lax.axis_index("tp_0"), lax.axis_index("tp_1")
    kv, tp = z * ny + y, x * nc + c
    partner = {"tp_1": nc - 1 - c}

    dt, rows = tok_ref.shape
    ff = wup_ref.shape[1]
    dk = dt * ntp
    width = dk * nkv
    rb, heads, head = st.shape[0], st.shape[1], st.shape[2]
    proj = heads * head
    rh = rows // nc
    rc = rh // 2
    other = nc - 1 - c

    def kv_dev(k):
        return {"kv_0": k // ny, "kv_1": lax.rem(k, ny)}

    def tp_dev(t):
        return {"tp_0": t // nc, "tp_1": lax.rem(t, nc)}

    def remote(src, dst, send_sem, recv_sem, dev):
        return pltpu.make_async_remote_copy(
            src_ref=src,
            dst_ref=dst,
            send_sem=send_sem,
            recv_sem=recv_sem,
            device_id=dev,
            device_id_type=MESH,
        )

    def all_received(ref, send_sem, recv_sem):
        remote(ref, ref, send_sem, recv_sem, partner).wait_recv()

    def all_sent(ref, send_sem, recv_sem):
        remote(ref, ref, send_sem, recv_sem, partner).wait_send()

    def loop(lo, hi, body):
        def wrapped(i, carry):
            body(i)
            return carry

        lax.fori_loop(lo, hi, wrapped, 0)

    def ring(n):
        return sorted(range(1, n), key=lambda d: (-min(d, n - d), d))

    def block(i, n):
        return pl.ds(pl.multiple_of(i * n, n), n)

    barrier = pltpu.get_barrier_semaphore()

    def greet(dev):
        pl.semaphore_signal(barrier, inc=1, device_id=dev, device_id_type=MESH)

    for dx in [*ring(nx), 0]:
        for dc in range(nc):
            if dx or dc:
                greet({"tp_0": lax.rem(x + dx, nx), "tp_1": lax.rem(c + dc, nc)})
    for d in range(1, ny):
        greet({"kv_1": lax.rem(y + d, ny)})
    for d in range(1, nz):
        greet({"kv_0": lax.rem(z + d, nz)})

    own_tok = col_t.at[block(tp, dt), :]
    first = (
        (tok_ref, own_tok),
        (wbeta_ref, w_beta),
        (wdecay_ref, w_decay),
        (mix_gain_ref, mix_gain),
        (rate_ref, rate),
        (out_gain_ref, out_gain),
        (mlp_gain_ref, mlp_gain),
        (state_ref, st),
        (wout_ref, w_out.at[block(c, proj), :]),
        (wup_ref, w_up.at[:, pl.ds(0, ff)]),
        (wdown_ref, w_down.at[pl.ds(0, ff), :]),
    )
    copies = [
        pltpu.make_async_copy(src, dst, local_sem.at[i]) for i, (src, dst) in enumerate(first)
    ]
    for copy in copies[:4]:
        copy.start()
    for i, w in enumerate((wq_ref, wk_ref, wv_ref, wg_ref)):
        pltpu.make_async_copy(w, w_proj.at[i], local_sem.at[11]).start()
    for copy in copies[4:]:
        copy.start()

    n_heads = wbeta_ref.shape[0]
    copies[1].wait()
    copies[2].wait()
    w_rates[...] = jnp.zeros_like(w_rates)
    w_rates[0:n_heads, :] = w_beta[...]
    w_rates[32 : 32 + n_heads, :] = w_decay[...]

    width_x = nx * dt
    column = lax.broadcasted_iota(jnp.int32, (dk, dk), 1)
    source = (lax.rem(column, width_x) // dt * nc + column // width_x) * dt + lax.rem(column, dt)
    row = lax.broadcasted_iota(jnp.int32, (dk, dk), 0)
    perm[...] = jnp.where(row == source, 1.0, 0.0).astype(BF16)

    copies[0].wait()
    copies[3].wait()
    pl.semaphore_wait(barrier, ntp - 1 + ny - 1 + nz - 1)

    def tp_peers():
        near = [(0, 1)] if nc == 2 else []
        return [(dx, dc) for dx in ring(nx) for dc in range(nc)] + near

    def tp_peer(dx, dc):
        return lax.rem(x + dx, nx) * nc + lax.rem(c + dc, nc)

    for dx, dc in tp_peers():
        remote(own_tok, own_tok, a_send, a_recv, tp_dev(tp_peer(dx, dc))).start()

    a_all = col_t.at[pl.ds(0, (ntp - 1) * dt), :]
    all_received(a_all, a_send, a_recv)

    cols = col_t[...].astype(F32).T
    col_n[...] = cols.astype(BF16)
    normed = (cols * mix_gain[...]).astype(BF16)
    squares = jnp.sum(cols * cols, axis=1, keepdims=True)

    pltpu.make_async_copy(w_proj, w_proj, local_sem.at[11]).wait()

    def project(i):
        return jnp.dot(normed, w_proj[i], preferred_element_type=F32).astype(BF16)

    class Reduction:
        def __init__(self, i, column, columns, z_first):
            self.i, self.z_first = i, z_first
            self.n1, self.n2 = (nz, ny) if z_first else (ny, nz)
            self.at = pl.ds(column, columns)
            self.recv1, self.send2, self.recv2 = recv_b1[i], send_b2[i], recv_b2[i]

        def place(self, first, second):
            dz, dy = (first, second) if self.z_first else (second, first)
            return lax.rem(z + dz, nz), lax.rem(y + dy, ny)

        def rows(self, first, second):
            zk, yk = self.place(first, second)
            return send_b.at[block(zk * ny + yk, rb), self.at]

        def start(self):
            for second in [*ring(self.n2), 0]:
                for first in ring(self.n1):
                    zk, yk = self.place(first, second)
                    line, dev = (yk, {"kv_0": zk}) if self.z_first else (zk, {"kv_1": yk})
                    remote(
                        self.rows(first, second),
                        self.recv1.at[line, first - 1],
                        b1_send.at[self.i],
                        b1_recv.at[self.i, line],
                        dev,
                    ).start()

        def first_sum(self, second):
            zk, yk = self.place(0, second)
            line = yk if self.z_first else zk
            acc = self.rows(0, second)[...].astype(F32)
            all_received(self.recv1.at[line], b1_send.at[self.i], b1_recv.at[self.i, line])
            for k in range(self.n1 - 1):
                acc = acc + self.recv1[line, k].astype(F32)
            return acc

        def pass_on(self, second):
            zk, yk = self.place(0, second)
            dev = {"kv_1": yk} if self.z_first else {"kv_0": zk}
            blk = self.send2.at[second - 1]
            blk[...] = self.first_sum(second).astype(BF16)
            remote(
                blk, self.recv2.at[second - 1], b2_send.at[self.i], b2_recv.at[self.i], dev
            ).start()

        def second_sum(self, acc):
            all_received(self.recv2, b2_send.at[self.i], b2_recv.at[self.i])
            for k in range(self.n2 - 1):
                acc = acc + self.recv2[k].astype(F32)
            return acc

        def sent(self):
            all_sent(self.recv1, b1_send.at[self.i], b1_recv.at[self.i, 0])
            all_sent(self.recv2, b2_send.at[self.i], b2_recv.at[self.i])

    q_end, k_end = proj + 128, 2 * proj + 128
    for_query = Reduction(0, 0, q_end, True)
    for_key = Reduction(1, q_end, proj, False)
    for_value = Reduction(2, k_end, proj, True)
    for_gate = Reduction(3, k_end + proj, proj, False)

    contract_last = (((1,), (1,)), ((), ()))
    rates_part = lax.dot_general(
        normed, w_rates[...], contract_last, preferred_element_type=F32
    )
    lane = lax.broadcasted_iota(jnp.int32, rates_part.shape, 1)
    rates_part = jnp.where(lane == 63, squares, rates_part)
    high = rates_part.astype(BF16).astype(F32)
    low = pltpu.roll(rates_part - high, 64, 1)
    send_b[:, proj:q_end] = jnp.where(lane < 64, high, low).astype(BF16)
    send_b[:, :proj] = project(0)
    for_query.start()
    send_b[:, q_end:k_end] = project(1)
    for_key.start()
    send_b[:, k_end : k_end + proj] = project(2)
    for_value.start()
    send_b[:, k_end + proj :] = project(3)
    for_gate.start()

    copies[10].wait()

    def reorder(k):
        at = (pl.ds(0, ff), block(k, dk))
        w_down[at] = jnp.dot(w_down[at], perm[...], preferred_element_type=F32).astype(BF16)

    loop(0, nkv, reorder)

    copies[7].wait()

    def split(x):
        high = x.astype(BF16)
        return high, (x - high.astype(F32)).astype(BF16)

    def split_state(g):
        for h in range(heads):
            for i in range(2):
                high, low = split(st[2 * g + i, h])
                at = slice(i * head, (i + 1) * head)
                st_terms[g, h, :head, at] = high
                st_terms[g, h, head:, at] = low

    loop(0, rb // 2, split_state)

    def pass_on_both(by_z, by_y):
        for i in range(max(ny, nz) - 1):
            if i < nz - 1:
                by_y.pass_on(ring(nz)[i])
            if i < ny - 1:
                by_z.pass_on(ring(ny)[i])
        return by_z.first_sum(0), by_y.first_sum(0)

    query_sum, key_sum = pass_on_both(for_query, for_key)

    value_sum, gate_sum = pass_on_both(for_value, for_gate)

    key_sum = for_key.second_sum(key_sum)
    query_sum = for_query.second_sum(query_sum)

    swaps = [
        remote(
            w_out.at[block(c, proj), :],
            w_out.at[block(c, proj), :],
            swap_send.at[0],
            swap_recv.at[0],
            partner,
        ),
        remote(
            w_up.at[:, pl.ds(0, ff)],
            w_up.at[:, pl.ds(ff, ff)],
            swap_send.at[1],
            swap_recv.at[1],
            partner,
        ),
        remote(
            w_down.at[pl.ds(0, ff), :],
            w_down.at[pl.ds(ff, ff), :],
            swap_send.at[2],
            swap_recv.at[2],
            partner,
        ),
    ]
    copies[8].wait()
    copies[9].wait()
    for swap in swaps:
        swap.start()

    rates = query_sum[:, proj:]
    rates = rates + pltpu.roll(rates, 64, 1)
    lane_b = lax.broadcasted_iota(jnp.int32, rates.shape, 1)

    def pick(i):
        return jnp.sum(jnp.where(lane_b == i, rates, 0.0), axis=1, keepdims=True)

    for i in range(4, 7):
        copies[i].wait()
    row_scale = lax.rsqrt(pick(63) / width + EPSILON)
    for h in range(heads):
        at = slice(h * head, (h + 1) * head)
        beta_raw = pick(tp * heads + h) * row_scale
        decay_raw = pick(32 + tp * heads + h) * row_scale
        beta = 1.0 / (1.0 + jnp.exp(-beta_raw))
        softplus = jnp.maximum(decay_raw, 0.0) + jnp.log1p(jnp.exp(-jnp.abs(decay_raw)))
        decay = jnp.exp(-rate[0:1, h : h + 1] * softplus)
        query = silu(query_sum[:, at] * row_scale)
        query = query * lax.rsqrt(jnp.sum(query * query, axis=1, keepdims=True) + EPSILON)
        query = query * head ** (-0.5)
        key = silu(key_sum[:, at] * row_scale)
        key = key * lax.rsqrt(jnp.sum(key * key, axis=1, keepdims=True) + EPSILON)
        key_s[h] = key
        terms = jnp.concatenate([*split(key), *split(query)], axis=0)
        lhs_s[h] = jnp.concatenate([terms, terms], axis=1)
        shape = (rb, head)
        rows_s[0, h] = jnp.broadcast_to(decay, shape)
        rows_s[1, h] = jnp.broadcast_to(beta, shape)
        rows_s[2, h] = jnp.broadcast_to(
            jnp.sum(key * query, axis=1, keepdims=True), shape
        )

    row = lax.broadcasted_iota(jnp.int32, (rb, head), 0)

    def read_pair(g, sums):
        out = []
        for h in range(heads):
            got = jnp.dot(lhs_s[h], st_terms[g, h], preferred_element_type=F32)
            for k in range(2):
                both = got[2 * k * rb : (2 * k + 1) * rb] + got[(2 * k + 1) * rb : (2 * k + 2) * rb]
                acc = sums[2 * h + k]
                for i in range(2):
                    acc = jnp.where(row == 2 * g + i, both[:, i * head : (i + 1) * head], acc)
                out.append(acc)
        return out

    def read_pairs(g, sums):
        for i in range(2):
            sums = read_pair(2 * g + i, sums)
        return sums

    zero = jnp.zeros((rb, head), F32)
    read_sums = lax.fori_loop(0, rb // 4, read_pairs, [zero] * (2 * heads))

    value_sum = for_value.second_sum(value_sum)
    gate_sum = for_gate.second_sum(gate_sum)
    for h in range(heads):
        at = slice(h * head, (h + 1) * head)
        decay = rows_s[0, h]
        value = silu(value_sum[:, at] * row_scale)
        change = rows_s[1, h] * (value - decay * read_sums[2 * h])
        read = decay * read_sums[2 * h + 1] + rows_s[2, h] * change
        rows_s[3, h] = change
        scale = lax.rsqrt(jnp.sum(read * read, axis=1, keepdims=True) / head + EPSILON)
        gate = silu(gate_sum[:, at] * row_scale)
        mine[:, at] = (read * scale * out_gain[...] * gate).astype(BF16)

    per_half = nkv // nc
    keeper = kv // per_half
    my_rows = block(lax.rem(kv, per_half), rb)
    slot = merged.at[my_rows, block(c, proj)]

    def d_bytes(n):
        return send_b.at[pl.ds(0, n * rb), pl.ds(0, proj)]

    def hops(d):
        dz, dy = d // ny, d % ny
        return min(dz, nz - dz) + min(dy, ny - dy)

    def kv_peer(d):
        return lax.rem(z + d // ny, nz) * ny + lax.rem(y + d % ny, ny)

    for d in sorted(range(1, nkv), key=lambda d: -hops(d)):
        dev = {**kv_dev(kv_peer(d)), "tp_1": keeper}
        remote(mine, slot, d_send, d_recv, dev).start()

    @pl.when(keeper != c)
    def _():
        remote(mine, slot, d_send, d_recv, {"tp_1": keeper}).start()

    @pl.when(keeper == c)
    def _():
        merged[my_rows, block(c, proj)] = mine[...]

    group, repeat = 8, 128 // rb
    for h in range(heads):
        key_tr = jnp.concatenate([key_s[h]] * repeat, axis=0).T
        for g in range(rb // group):
            key_t[g, h] = pltpu.roll(key_tr, (128 - g * group) % 128, 1) if g else key_tr

    def write_group(g):
        for i in range(group):
            b = g * group + i
            for h in range(heads):
                st[b, h] = (
                    rows_s[0, h, pl.ds(b, 1), :] * st[b, h]
                    + key_t[g, h, :, i : i + 1] * rows_s[3, h, pl.ds(b, 1), :]
                )

    loop(0, rb // group, write_group)
    state_out = pltpu.make_async_copy(st, new_state_ref, local_sem.at[12])
    state_out.start()
    all_sent(a_all, a_send, a_recv)
    for reduction in (for_query, for_key, for_value, for_gate):
        reduction.sent()

    @pl.when(keeper == c)
    def _():
        all_received(d_bytes(nkv - 1), d_send, d_recv)

    @pl.when(keeper != c)
    def _():
        all_received(d_bytes(nkv), d_send, d_recv)

    swaps[0].wait_recv()

    rq = rc // 2

    def ex_rows(order, part):
        return pl.ds(order * rc + part * rq, rq)

    def ex_start(order, part):
        blk = recv_ex.at[x, ex_rows(order, part), :]
        i = 2 * order + part
        for d in ring(nx):
            to = {"tp_0": lax.rem(x + d, nx)}
            remote(blk, blk, ex_send.at[i], ex_recv.at[i], to).start()

    def ex_all(order, part):
        return recv_ex.at[pl.ds(0, nx - 1), ex_rows(order, part), :]

    for order in range(2):
        at = slice(order * rc, (order + 1) * rc)
        part = jnp.dot(merged[at, :], w_out[...], preferred_element_type=F32)
        recv_ex[x, at] = part.astype(BF16)
        ex_start(order, 0)
    for order in range(2):
        ex_start(order, 1)

    def residual(order, part):
        i = 2 * order + part
        all_received(ex_all(order, part), ex_send.at[i], ex_recv.at[i])
        at = ex_rows(order, part)
        branch = recv_ex[0, at].astype(F32)
        for i in range(1, nx):
            branch = branch + recv_ex[i, at].astype(F32)
        start = c * rh + order * rc + part * rq
        tok = col_n[pl.ds(pl.multiple_of(start, rq), rq), :]
        res[kv, at] = (tok.astype(F32) + branch).astype(BF16)

    rows_a, rows_b = pl.ds(0, rc), pl.ds(rc, rc)

    y_arrival, z_arrival = [0, *ring(ny)[::-1]], [0, *ring(nz)[::-1]]
    y_last, z_last = y_arrival[-1], z_arrival[-1]

    def part_of(base, part):
        return pl.ds(base, rc) if part is None else pl.ds(base + part * rq, rq)

    def fa_copy(k, sem, dev, part=None):
        blk = res.at[k, part_of(0, part), :]
        return remote(blk, blk, fa_send, fa_recv.at[sem], dev)

    def fb_copy(k, sem, dev, part=None):
        blk = res.at[k, part_of(rc, part), :]
        return remote(blk, blk, fb_send, fb_recv.at[sem], dev)

    def near_a(d, part):
        return part * (ny - 1) + d - 1

    def near_b(d, part):
        return part * (nz - 1) + d - 1

    def late_a(dy, dz):
        return 2 * (ny - 1) + (ny - 1 + dz if dy == y_last else y_arrival.index(dy))

    def late_b(dz, dy):
        return 2 * (nz - 1) + (nz - 1 + dy if dz == z_last else z_arrival.index(dz))

    def home(dz, dy):
        return lax.rem(z + nz - dz, nz) * ny + lax.rem(y + ny - dy, ny)

    def y_dev(d):
        return {"kv_1": lax.rem(y + d, ny)}

    def z_dev(d):
        return {"kv_0": lax.rem(z + d, nz)}

    for part in range(2):
        residual(0, part)
        for d in ring(ny):
            fa_copy(kv, near_a(d, part), y_dev(d), part).start()
        residual(1, part)
        for d in ring(nz):
            fb_copy(kv, near_b(d, part), z_dev(d), part).start()
        for d in ring(nz):
            fa_copy(kv, late_a(0, d), z_dev(d), part).start()
        for d in ring(ny):
            fb_copy(kv, late_b(0, d), y_dev(d), part).start()

    res_t[...] = res[kv].astype(F32).T.astype(BF16)
    r_copy = remote(
        res_t.at[block(x * nc + other, dt), :], recv_r, r_send, r_recv, partner
    )
    r_copy.start()

    def up(*blocks):
        total, acc = total_sq[...], acc_up[...]
        for dz, dy in blocks:
            k = home(dz, dy)
            at = block(k, dk)
            blk = res[k].astype(F32)
            sq = blk * blk
            for i in range(dk // 128):
                total = total + sq[:, i * 128 : (i + 1) * 128]
            acc = acc + jnp.dot(
                (blk * mlp_gain[:, at]).astype(BF16), w_up[at, :], preferred_element_type=F32
            )
        total_sq[...], acc_up[...] = total, acc

    acc_up[...] = jnp.zeros_like(acc_up)
    total_sq[...] = jnp.zeros_like(total_sq)
    for swap in swaps[1:]:
        swap.wait_recv()
    up((0, 0))

    @pl.when(keeper == c)
    def _():
        all_sent(d_bytes(nkv - 1), d_send, d_recv)

    @pl.when(keeper != c)
    def _():
        all_sent(d_bytes(nkv), d_send, d_recv)

    for i in range(4):
        all_sent(ex_all(i // 2, i % 2), ex_send.at[i], ex_recv.at[i])

    for part in range(2):
        for i in range(1, max(ny, nz)):
            if i < ny:
                dy = y_arrival[i]
                fa_copy(home(0, dy), near_a(dy, part), partner, part).wait_recv()
                for d in ring(nz):
                    fa_copy(home(0, dy), late_a(dy, d), z_dev(d), part).start()
            if i < nz:
                dz = z_arrival[i]
                fb_copy(home(dz, 0), near_b(dz, part), partner, part).wait_recv()
                for d in ring(ny):
                    fb_copy(home(dz, 0), late_b(dz, d), y_dev(d), part).start()

    got_a = {(0, dy) for dy in range(ny)}
    got_b = {(dz, 0) for dz in range(nz)}
    done = {(0, 0)}

    def up_ready():
        ready = sorted((got_a & got_b) - done)
        done.update(ready)
        for i in range(0, len(ready), 2):
            up(*ready[i : i + 2])

    for i in range(max(ny, nz)):
        if i < ny - 1:
            dy = y_arrival[i]
            all_received(
                res.at[pl.ds(0, nz - 1), rows_a, :], fa_send, fa_recv.at[late_a(dy, 1)]
            )
            got_a |= {(dz, dy) for dz in range(1, nz)}
        if i < nz - 1:
            dz = z_arrival[i]
            all_received(
                res.at[pl.ds(0, ny - 1), rows_b, :], fb_send, fb_recv.at[late_b(dz, 1)]
            )
            got_b |= {(dz, dy) for dy in range(1, ny)}
        up_ready()
    for i in range(1, max(ny, nz)):
        if i < nz:
            dz = z_arrival[i]
            fa_copy(home(dz, y_last), late_a(y_last, dz), partner).wait_recv()
            got_a.add((dz, y_last))
        if i < ny:
            dy = y_arrival[i]
            fb_copy(home(z_last, dy), late_b(z_last, dy), partner).wait_recv()
            got_b.add((z_last, dy))
        up_ready()

    scale = lax.rsqrt(jnp.sum(total_sq[...], axis=1, keepdims=True) / width + EPSILON)
    relu = jnp.maximum(acc_up[...] * scale, 0.0)
    hid[...] = (relu * relu).astype(BF16)

    hw = dk // 2
    part_a, part_b = pl.ds(0, hw), pl.ds(hw, hw)

    def h1a_copy(dz, k):
        return remote(
            send_h.at[k, :, part_a],
            recv_h1a.at[lax.rem(k, ny), dz - 1],
            h1a_send,
            h1a_recv.at[lax.rem(k, ny)],
            {"kv_0": k // ny},
        )

    def h1b_copy(dy, k):
        return remote(
            send_h.at[k, :, part_b],
            recv_h1b.at[k // ny, dy - 1],
            h1b_send,
            h1b_recv.at[k // ny],
            {"kv_1": lax.rem(k, ny)},
        )

    def down(dz, dy):
        zk, yk = lax.rem(z + dz, nz), lax.rem(y + dy, ny)
        k = zk * ny + yk
        out = jnp.dot(hid[...], w_down[:, block(k, dk)], preferred_element_type=F32)
        send_h[k] = out.astype(BF16)
        if dz:
            h1a_copy(dz, k).start()
        if dy:
            h1b_copy(dy, k).start()

    z_order, y_order = [*ring(nz), 0], [*ring(ny), 0]
    for s in range(max(nz, ny)):
        shell = [(i, s) for i in range(s, nz)] + [(s, i) for i in range(s + 1, ny)]
        for i, j in shell:
            if i < nz and j < ny:
                down(z_order[i], y_order[j])
    all_sent(res.at[pl.ds(0, nkv - 1), rows_a, :], fa_send, fa_recv.at[0])
    all_sent(res.at[pl.ds(0, nkv - 1), rows_b, :], fb_send, fb_recv.at[0])
    for swap in swaps:
        swap.wait_send()
    r_copy.wait_send()

    def h1a_sum(yk):
        acc = send_h[z * ny + yk, :, 0:hw].astype(F32)
        all_received(recv_h1a.at[yk], h1a_send, h1a_recv.at[yk])
        for i in range(nz - 1):
            acc = acc + recv_h1a[yk, i].astype(F32)
        return acc

    def h1b_sum(zk):
        acc = send_h[zk * ny + y, :, hw : 2 * hw].astype(F32)
        all_received(recv_h1b.at[zk], h1b_send, h1b_recv.at[zk])
        for i in range(ny - 1):
            acc = acc + recv_h1b[zk, i].astype(F32)
        return acc

    def deliver(d, core):
        if core:
            total, line, buf = h1b_sum(lax.rem(z + d, nz)), z, send_xb.at[d]
            dev = {"kv_0": lax.rem(z + d, nz), "tp_1": core}
        else:
            total, line, buf = h1a_sum(lax.rem(y + d, ny)), y, send_xa.at[d]
            dev = {"kv_1": lax.rem(y + d, ny), "tp_1": core}
        buf[...] = total.T.astype(BF16)
        for dx in [*ring(nx), 0]:
            to_x = lax.rem(x + dx, nx)
            at = block(to_x, dt)

            def send(at=at, to_x=to_x):
                to = {**dev, "tp_0": to_x}
                remote(buf.at[at], recv_x.at[line, tp], x_send, x_recv, to).start()

            if d or dx:
                send()
            else:

                @pl.when(c != core)
                def _():
                    send()

                @pl.when(c == core)
                def _():
                    recv_x[line, tp] = buf[at]

    for i in range(max(ny, nz)):
        if i < ny:
            deliver([*ring(ny), 0][i], 0)
        if i < nz:
            deliver([*ring(nz), 0][i], 1)

    def finish(lines):
        all_received(bytes_x.at[pl.ds(0, lines * ntp - 1)], x_send, x_recv)
        for core, residual in ((c, res_t[block(tp, dt), :]), (other, recv_r[...])):
            total = residual.astype(F32)
            for i in range(lines):
                for xx in range(nx):
                    total = total + recv_x[i, xx * nc + core].astype(F32)
            mixed_ref[:, block(core, rh)] = total.astype(BF16)

    r_copy.wait_recv()

    @pl.when(c == 0)
    def _():
        finish(ny)

    @pl.when(c == 1)
    def _():
        finish(nz)

    all_sent(bytes_x.at[pl.ds(0, (ny + nz) * nx - 1)], x_send, x_recv)
    all_sent(recv_h1a, h1a_send, h1a_recv.at[0])
    all_sent(recv_h1b, h1b_send, h1b_recv.at[0])
    state_out.wait()


STORES = 4


def store_kernel(mixed_ref, state_ref, mixed_out, state_out, sem):
    n = state_ref.shape[0] // STORES
    copies = [pltpu.make_async_copy(mixed_ref, mixed_out, sem.at[0])]
    for i in range(STORES):
        at = pl.ds(i * n, n)
        copies.append(pltpu.make_async_copy(state_ref.at[at], state_out.at[at], sem.at[1 + i]))
    for copy in copies:
        copy.start()
    for copy in copies:
        copy.wait()


def local(
    sizes,
    tokens,
    mix_gain,
    w_query,
    w_key,
    w_value,
    w_gate,
    w_beta,
    w_decay,
    decay_rate,
    out_gain,
    state,
    w_out,
    mlp_gain,
    w_up,
    w_down,
):
    nz, ny, nx, nc = sizes
    nkv, ntp = nz * ny, nx * nc
    rows, dt = tokens.shape
    dk = dt * ntp
    rb, heads, head, _ = state.shape
    proj = heads * head
    sent = 4 * proj + 128
    reductions = ((proj + 128, True), (proj, False), (proj, True), (proj, False))
    first = [(ny, nz) if by_z else (nz, ny) for _, by_z in reductions]
    widths = [w for w, _ in reductions]
    n_heads = w_beta.shape[1]
    ff = w_up.shape[1]
    rh = rows // nc
    rc = rh // 2
    vmem, dma = pltpu.VMEM, pltpu.SemaphoreType.DMA
    scratch = [
        vmem((dk, rows), BF16),
        vmem((4, dk, proj), BF16),
        vmem((128, dk), BF16),
        vmem((dk, dk), BF16),
        vmem((n_heads, dk), BF16),
        vmem((n_heads, dk), BF16),
        vmem((1, dk), F32),
        vmem((1, head), F32),
        vmem((1, dk * nkv), F32),
        vmem((1, heads), F32),
        vmem((nc * proj, dk), BF16),
        vmem((w_up.shape[0], 2 * ff), BF16),
        vmem((2 * ff, w_down.shape[1]), BF16),
        vmem(state.shape, F32),
        vmem((rows, dk), BF16),
        vmem((rows, sent), BF16),
        [vmem((n2, n1 - 1, rb, w), BF16) for (n2, n1), w in zip(first, widths)],
        [vmem((n2 - 1, rb, w), BF16) for (n2, n1), w in zip(first, widths)],
        [vmem((n2 - 1, rb, w), BF16) for (n2, n1), w in zip(first, widths)],
        vmem((rb // 8, heads, head, 128), F32),
        vmem((heads, rb, head), F32),
        vmem((heads, 4 * rb, 2 * head), BF16),
        vmem((rb // 2, heads, 2 * head, 2 * head), BF16),
        vmem((4, heads, rb, head), F32),
        vmem((rb, proj), BF16),
        vmem((rh, nc * proj), BF16),
        vmem((nx, rh, dk), BF16),
        vmem((nkv, rh, dk), BF16),
        vmem((dk, rh), BF16),
        vmem((dt, rh), BF16),
        vmem((rh, 2 * ff), BF16),
        vmem((rh, 2 * ff), F32),
        vmem((rh, 128), F32),
        vmem((nkv, rh, dk), BF16),
        vmem((ny, nz - 1, rh, dk // 2), BF16),
        vmem((nz, ny - 1, rh, dk // 2), BF16),
        vmem((ny, dk // 2, rh), BF16),
        vmem((nz, dk // 2, rh), BF16),
        vmem((max(ny, nz), ntp, dt, rh), BF16),
        vmem((max(ny, nz) * ntp, dt, rh), BF16),
        dma((13,)),
        dma(()),
        dma(()),
        dma((4,)),
        dma((4, max(ny, nz))),
        dma((4,)),
        dma((4,)),
        dma(()),
        dma(()),
        dma((4,)),
        dma((4,)),
        dma(()),
        dma(()),
        dma((3 * (ny - 1) + nz,)),
        dma((3 * (nz - 1) + ny,)),
        dma(()),
        dma(()),
        dma((3,)),
        dma((3,)),
        dma(()),
        dma(()),
        dma((ny,)),
        dma((nz,)),
        dma(()),
        dma(()),
    ]
    in_hbm = pl.BlockSpec(memory_space=pl.ANY)
    in_vmem = pl.BlockSpec(memory_space=pltpu.VMEM)
    mixed_t, new_state = pl.pallas_call(
        functools.partial(layer_kernel, sizes),
        out_shape=(
            pltpu.VMEM((dt, rows), BF16),
            pltpu.VMEM(state.shape, F32),
        ),
        in_specs=[in_hbm] * 15,
        out_specs=(in_vmem, in_hbm),
        scratch_shapes=scratch,
        compiler_params=pltpu.CompilerParams(
            collective_id=0, has_side_effects=True, vmem_limit_bytes=63_500_000
        ),
        name="layer",
    )(
        tokens.T,
        mix_gain[None, :],
        w_query,
        w_key,
        w_value,
        w_gate,
        w_beta.T,
        w_decay.T,
        decay_rate[None, :],
        out_gain[None, :],
        state,
        w_out,
        mlp_gain[None, :],
        w_up,
        w_down,
    )
    mixed_t, new_state = pl.pallas_call(
        store_kernel,
        out_shape=(
            jax.ShapeDtypeStruct((dt, rows), BF16),
            jax.ShapeDtypeStruct(state.shape, F32),
        ),
        in_specs=[in_hbm] * 2,
        out_specs=(in_hbm, in_hbm),
        scratch_shapes=[dma((1 + STORES,))],
        compiler_params=pltpu.CompilerParams(vmem_limit_bytes=1_000_000),
        name="store",
    )(mixed_t, new_state)
    return mixed_t.T, new_state


def solution(mesh):
    n = dict(mesh.shape)
    sizes = (n["kv"] // 4, 4, n["tp"] // 2, 2) if n["kv"] >= 8 else (2, n["kv"] // 2, n["tp"] // 2, 2)
    torus = Mesh(mesh.devices.reshape(sizes), KV_TP)
    in_specs = (
        P(None, KV_TP),
        P(KV),
        P(KV, TP),
        P(KV, TP),
        P(KV, TP),
        P(KV, TP),
        P(KV, None),
        P(KV, None),
        P(TP),
        P(),
        P(KV, TP, None, None),
        P(TP, KV),
        P(),
        P(None, KV_TP),
        P(KV_TP, None),
    )
    out_specs = (P(None, KV_TP), P(KV, TP, None, None))
    return jax.shard_map(
        functools.partial(local, sizes),
        mesh=torus,
        in_specs=in_specs,
        out_specs=out_specs,
        check_vma=False,
    )
```
